128 devices in a mesh: sp: 64 (over z, y, x), tp: 2 (over core).
Axes of the slice: x: 4, y: 4, z: 4, core: 2. Of those that a mesh axis runs over, the one named last changes fastest.
Arguments:
- queries: bfloat16 [16384, 512], P('sp', 'tp'), may hold values from -20 to 20
- key_rows: bfloat16 [16384, 512], P('sp', 'tp'), may hold values from -20 to 20
- value_rows: bfloat16 [16384, 512], P('sp', 'tp'), may hold values from -6 to 6
- residual: bfloat16 [16384, 2048], P(('sp', 'tp')), may hold values from -6 to 6
- out_weight: bfloat16 [512, 2048], replicated, may hold values from -0.75 to 0.75
- norm_gain: float32 [2048], replicated, may hold values from 0.1 to 1.9
- routes: int32 [16384, 8], P(('sp', 'tp')), may hold values from 0 to 63, all different within a row; in each aligned block of 128 rows (0 to 127, 128 to 255, ...) at most 20 rows name the same one
- route_weight: float32 [16384, 8], P(('sp', 'tp')), may hold values from 0.1 to 0.6
- expert_gate: bfloat16 [64, 2048, 512], P('sp', None, 'tp'), may hold values from -0.125 to 0.125
- expert_up: bfloat16 [64, 2048, 512], P('sp', None, 'tp'), may hold values from -0.125 to 0.125
- expert_down: bfloat16 [64, 512, 2048], P('sp', 'tp'), may hold values from -0.25 to 0.25
- shared_gate: bfloat16 [2048, 512], replicated, may hold values from -0.125 to 0.125
- shared_up: bfloat16 [2048, 512], replicated, may hold values from -0.125 to 0.125
- shared_down: bfloat16 [512, 2048], replicated, may hold values from -0.25 to 0.25
Outputs:
- output: bfloat16 [16384, 2048], P(('sp', 'tp'))
The draws below stay inside these ranges and needn't reach their ends.
Inputs may be any that keep to these rules, and one draw needn't show every extreme that they name: `routes`: each row names 8 different experts. In each aligned block of 128 rows (the rows of one device) no expert is named more than 20 times, a bound that some block reaches.
All inputs are finite; a program needn't handle non-finite values.
Results may differ from the reference program's by a relative error of at most 0.012.
Values may be sent and summed in bfloat16 or wider, within the bound.
No kernel may reach another device: no remote copies, remote signals or barrier semaphores. Data moves between devices by JAX's collectives and lax.ppermute only.
A program may use at most 192 MiB of HBM per device.

```python
import math
import jax
import jax.numpy as jnp
import numpy as np
from jax import lax

D = 2048
FOCUS_CHANNELS = 8
HEAD_DIM = 64
FFE = 512
SHARED = 512
TOPK = 8
TOK_DEV = 256
STRING_ITEMS = 16384
ATT = 512
EXPERTS = 64
CAP = 20
N_TP = 2


def channel_arrangement(key):
    starting_shift = jax.random.fold_in(key, 101)
    heading_seed, layering_seed, permuting_seed, segment_seed, cluster_seed = jax.random.split(starting_shift, 5)
    movement_heading = jax.random.normal(heading_seed, (FOCUS_CHANNELS, HEAD_DIM), jnp.float32)
    movement_heading = movement_heading / jnp.sqrt(jnp.sum(movement_heading * movement_heading, axis=1, keepdims=True))
    order = jax.random.permutation(permuting_seed, FOCUS_CHANNELS)
    quick = order < FOCUS_CHANNELS // 2
    slow_depth = jax.random.uniform(layering_seed, (FOCUS_CHANNELS,), jnp.float32, 11.5, 13.0)
    quick_depth = jax.random.uniform(jax.random.fold_in(layering_seed, 1), (FOCUS_CHANNELS,), jnp.float32, 3.5, 5.0)
    layering_count = jnp.where(quick, quick_depth, slow_depth)
    segment_multiplier = jax.random.uniform(segment_seed, (STRING_ITEMS // TOK_DEV, FOCUS_CHANNELS), jnp.float32, 0.92, 1.08)
    cluster_count = jax.random.randint(cluster_seed, (4, FOCUS_CHANNELS), 0, STRING_ITEMS)
    return (movement_heading, layering_count, segment_multiplier, cluster_count)


def draw_queries(key, part):
    movement_heading, layering_count, segment_multiplier, cluster_count = channel_arrangement(key)
    noise_key = jax.random.fold_in(key, 202)
    noise = 0.5 * jnp.clip(jax.random.normal(noise_key, (STRING_ITEMS, FOCUS_CHANNELS, HEAD_DIM), jnp.float32), -5.0, 5.0)
    rows = layering_count[None, :, None] * movement_heading[None, :, :] + noise
    return rows.reshape(STRING_ITEMS, FOCUS_CHANNELS * HEAD_DIM).astype(jnp.bfloat16)


def draw_key_rows(key, part):
    movement_heading, layering_count, segment_multiplier, cluster_count = channel_arrangement(key)
    noise_key = jax.random.fold_in(key, 303)
    item_indices = jnp.arange(STRING_ITEMS, dtype=jnp.int32)
    strength = 8.0 * segment_multiplier[item_indices // TOK_DEV]
    broken_entries = jnp.any(item_indices[:, None, None] == cluster_count[None, :, :], axis=1)
    strength = jnp.where(broken_entries, 5.6 / layering_count[None, :], strength)
    noise = jnp.clip(jax.random.normal(noise_key, (STRING_ITEMS, FOCUS_CHANNELS, HEAD_DIM), jnp.float32), -5.0, 5.0)
    rows = noise - strength[:, :, None] * movement_heading[None, :, :]
    return rows.reshape(STRING_ITEMS, FOCUS_CHANNELS * HEAD_DIM).astype(jnp.bfloat16)


def shard_levels(own_key, dims, cuts, low, high):
    loudness = 1.0
    for dim, blocks in cuts:
        steps = jax.random.uniform(jax.random.fold_in(jax.random.fold_in(own_key, 6), dim), (blocks,), jnp.float32, low / len(cuts), high / len(cuts))
        loudness = loudness * jnp.repeat(jnp.exp(steps), dims[dim] // blocks).reshape((-1,) + (1,) * (len(dims) - 1 - dim))
    return loudness


def routed_block(key, own, number, rows, number_of, top, bound, skew):
    order = jax.random.permutation(key, number_of)
    heavy_load, usual = load_shares(number_of, rows * top, bound, skew, True), load_shares(number_of, rows * top, bound, skew, False)
    places = jnp.arange(number_of)

    def named(lengths, rotation):
        used = int((lengths > 0).sum())
        fixed = max(1, used // 4)
        shifted = fixed + (places - fixed + rotation * (used - fixed)) % max(1, number_of - fixed)
        return jnp.zeros((number_of,), jnp.int32).at[order[jnp.where(places < fixed, places, shifted)]].set(jnp.asarray(lengths, jnp.int32))

    lengths = jnp.where(number % 4 == 0, named(heavy_load, number // 4), named(usual, number - number // 4 - 1))
    mixed = jax.random.permutation(jax.random.fold_in(own, 3), number_of)
    source_of, receiver = mixed[0:number_of // 2 * 2:2], mixed[1:number_of // 2 * 2:2]
    room = jnp.minimum(lengths[source_of] - 1, bound - lengths[receiver]) // 2
    room = jnp.where((source_of == order[0]) | (receiver == order[0]) | (lengths[receiver] == 0), 0, jnp.maximum(room, 0))
    shifted = jax.random.randint(jax.random.fold_in(own, 4), (number_of // 2,), 0, 1 << 20) % (room + 1)
    lengths = lengths.at[source_of].add(-shifted).at[receiver].add(shifted)
    items = jnp.searchsorted(jnp.cumsum(lengths), jnp.arange(rows * top), side="right").astype(jnp.int32)
    grid = items.reshape(top, rows).T
    grid = grid[jax.random.permutation(jax.random.fold_in(own, 1), rows)]
    rotation = jax.random.randint(jax.random.fold_in(own, 2), (rows, 1), 0, top)
    return jnp.take_along_axis(grid, (jnp.arange(top)[None, :] + rotation) % top, axis=1)


def load_shares(count, total, reach, lean, full):
    loads = [(1 << 20) // math.isqrt(rank ** lean) + 1 for rank in range(1, count + 1)]
    largest = reach if full else min(reach, max(-(-total // count), total * loads[0] // sum(loads)))
    least = 1 if total - largest >= count - 1 else 0
    counts, spare = [largest] + [least] * (count - 1), total - largest - least * (count - 1)
    while spare > 0:
        candidates = [i for i in range(1, count) if counts[i] < largest] or [i for i in range(1, count) if counts[i] < reach]
        whole, budget = sum([loads[i] for i in candidates]), spare
        for i in candidates:
            addition = min(reach - counts[i], max(1, budget * loads[i] // whole), spare)
            counts[i] = counts[i] + addition
            spare = spare - addition
    return np.array(counts)


def scatter_about(stream_key, shape, deviation, most, shards=(), held_as=jnp.bfloat16):
    values = jax.random.normal(stream_key, shape, jnp.float32) * deviation
    if len(shards) > 0:
        values = shard_levels(stream_key, shape, shards, -0.22, 0.18) * values
    return jnp.clip(values, min=-most, max=most).astype(held_as)


def setup_inputs(seed: int = 0) -> dict:
    seeds = jax.random.split(jax.random.key(seed), 15)
    queries = draw_queries(jax.random.fold_in(seeds[14], 71), 0)
    key_rows = draw_key_rows(jax.random.fold_in(seeds[14], 71), 0)
    value_rows = scatter_about(seeds[2], (STRING_ITEMS, ATT), 1.0, 6.0, ((0, 64), (1, 2)))
    residual = scatter_about(seeds[3], (STRING_ITEMS, D), 1.0, 6.0, ((0, 128),))
    out_weight = scatter_about(seeds[4], (ATT, D), (ATT // 9) ** -0.5, 0.75)
    norm_gain = jnp.clip(1.0 + 0.18 * jax.random.normal(seeds[5], (D,), jnp.float32), 0.1, 1.9)
    routes_keys = jax.random.split(jax.random.fold_in(seeds[6], 1), STRING_ITEMS // (TOK_DEV // N_TP))
    routes_turns = jax.random.permutation(jax.random.fold_in(seeds[6], 3), STRING_ITEMS // (TOK_DEV // N_TP))
    routes = jax.vmap(lambda own, number: routed_block(jax.random.fold_in(seeds[6], 2), own, number, TOK_DEV // N_TP, EXPERTS, TOPK, CAP, 1))(routes_keys, routes_turns).reshape((STRING_ITEMS, TOPK))
    route_weight = jnp.clip(jnp.exp(math.log(0.6) - 1.7917595 * jax.random.uniform(seeds[7], (STRING_ITEMS, TOPK), jnp.float32) ** shard_levels(seeds[7], (STRING_ITEMS, TOPK), ((0, 128),), -0.2, 0.2)), 0.1, 0.6)
    expert_gate = scatter_about(seeds[8], (EXPERTS, D, FFE), D ** -0.5, 0.125, ((0, 64), (2, 2)))
    expert_up = scatter_about(seeds[9], (EXPERTS, D, FFE), D ** -0.5, 0.125, ((0, 64), (2, 2)))
    expert_down = scatter_about(seeds[10], (EXPERTS, FFE, D), FFE ** -0.5, 0.25, ((0, 64), (1, 2)))
    shared_gate = scatter_about(seeds[11], (D, SHARED), D ** -0.5, 0.125)
    shared_up = scatter_about(seeds[12], (D, SHARED), D ** -0.5, 0.125)
    shared_down = scatter_about(seeds[13], (SHARED, D), SHARED ** -0.5, 0.25)
    return {"queries": queries, "key_rows": key_rows, "value_rows": value_rows, "residual": residual, "out_weight": out_weight, "norm_gain": norm_gain, "routes": routes, "route_weight": route_weight, "expert_gate": expert_gate, "expert_up": expert_up, "expert_down": expert_down, "shared_gate": shared_gate, "shared_up": shared_up, "shared_down": shared_down}


def reference(queries, key_rows, value_rows, residual, out_weight, norm_gain, routes, route_weight, expert_gate, expert_up, expert_down, shared_gate, shared_up, shared_down):
    factor = HEAD_DIM ** (-0.5)
    blocks = STRING_ITEMS // TOK_DEV
    key_heads = key_rows.astype(jnp.float32).reshape(blocks, TOK_DEV, FOCUS_CHANNELS, HEAD_DIM)
    value_heads = value_rows.astype(jnp.float32).reshape(blocks, TOK_DEV, FOCUS_CHANNELS, HEAD_DIM)
    key_pos = jnp.arange(STRING_ITEMS, dtype=jnp.int32).reshape(blocks, TOK_DEV)

    def query_block(index):
        query_heads = lax.dynamic_slice_in_dim(queries, index * TOK_DEV, TOK_DEV, 0).astype(jnp.float32).reshape(TOK_DEV, FOCUS_CHANNELS, HEAD_DIM)
        scores = jnp.einsum('thd,bshd->hbts', query_heads, key_heads, precision=lax.Precision.HIGHEST) * factor
        query_pos = index * TOK_DEV + jnp.arange(TOK_DEV, dtype=jnp.int32)
        live = key_pos[None, :, None, :] < query_pos[None, None, :, None]
        cost = jnp.where(live, jax.nn.softplus(scores), 0.0)
        inside = lax.cumsum(cost, axis=3, reverse=True) - cost
        weight = jnp.where(live, jnp.exp(jax.nn.log_sigmoid(scores) - inside), 0.0).astype(jnp.bfloat16)
        partial_value = jnp.einsum('hbts,bshd->bthd', weight.astype(jnp.float32), value_heads, precision=lax.Precision.HIGHEST)
        total = lax.optimization_barrier(jnp.sum(cost, axis=3))
        later = lax.cumsum(total, axis=1, reverse=True) - total
        attended = jnp.einsum('hbt,bthd->thd', jnp.exp(-later), partial_value, precision=lax.Precision.HIGHEST)
        return attended.reshape(TOK_DEV, ATT).astype(jnp.bfloat16)
    attended = lax.map(query_block, jnp.arange(blocks, dtype=jnp.int32)).reshape(STRING_ITEMS, ATT)
    projected = jnp.dot(attended, out_weight, preferred_element_type=jnp.float32)
    mixed = (residual.astype(jnp.float32) + projected).astype(jnp.bfloat16)
    mixed_wide = mixed.astype(jnp.float32)
    inverse = lax.rsqrt(lax.optimization_barrier(jnp.mean(mixed_wide * mixed_wide, axis=1, keepdims=True)) + 1e-06)
    normed = (mixed_wide * inverse * norm_gain.astype(jnp.float32)).astype(jnp.bfloat16)
    row_count = TOK_DEV // N_TP
    sources = STRING_ITEMS // row_count

    def slots(block_routes):
        flat = block_routes.reshape(-1)
        picks = (flat[:, None] == jnp.arange(EXPERTS, dtype=jnp.int32)[None, :]).astype(jnp.int32)
        earlier = jnp.cumsum(picks, axis=0) - picks
        return flat * CAP + lax.optimization_barrier(jnp.sum(earlier * picks, axis=1))
    position = lax.map(slots, routes.reshape(sources, row_count, TOPK))
    flat_slot = (jnp.arange(sources, dtype=jnp.int32)[:, None] * (EXPERTS * CAP) + position).reshape(-1)
    filler = jnp.zeros((sources * EXPERTS * CAP,), jnp.int32).at[flat_slot].set(jnp.arange(STRING_ITEMS * TOPK, dtype=jnp.int32) + 1)
    filler = filler.reshape(sources, EXPERTS, CAP).transpose(1, 0, 2).reshape(EXPERTS, sources * CAP)
    flat_weight = route_weight.reshape(-1)
    half = FFE // N_TP

    def one_expert(accum, inputs):
        fill_row, gate_matrix, up_matrix, down_matrix = inputs
        occupied = fill_row > 0
        assignment = jnp.maximum(fill_row - 1, 0)
        token_index = assignment // TOPK
        rows_in = normed[token_index]
        summed = jnp.zeros((rows_in.shape[0], D), jnp.float32)
        for section in range(N_TP):
            gate = jnp.dot(rows_in, gate_matrix[:, section * half:(section + 1) * half], preferred_element_type=jnp.float32)
            upward = jnp.dot(rows_in, up_matrix[:, section * half:(section + 1) * half], preferred_element_type=jnp.float32)
            hidden = (jax.nn.silu(gate) * upward).astype(jnp.bfloat16)
            result = jnp.dot(hidden, down_matrix[section * half:(section + 1) * half], preferred_element_type=jnp.float32)
            summed = summed + lax.optimization_barrier(result.astype(jnp.bfloat16)).astype(jnp.float32)
        expert_out = lax.optimization_barrier(summed.astype(jnp.bfloat16)).astype(jnp.float32)
        contribution = jnp.where(occupied[:, None], expert_out * flat_weight[assignment][:, None], 0.0)
        return (accum.at[token_index].add(contribution), None)
    routed, _ = lax.scan(one_expert, jnp.zeros((STRING_ITEMS, D), jnp.float32), (filler, expert_gate, expert_up, expert_down))
    shared_gate_out = jnp.dot(normed, shared_gate, preferred_element_type=jnp.float32)
    shared_up_out = jnp.dot(normed, shared_up, preferred_element_type=jnp.float32)
    shared_act = (jax.nn.silu(shared_gate_out) * shared_up_out).astype(jnp.bfloat16)
    shared_out = jnp.dot(shared_act, shared_down, preferred_element_type=jnp.float32)
    return (mixed_wide + routed + shared_out).astype(jnp.bfloat16)
```

```python
import jax
import jax.numpy as jnp
from jax import lax
from jax.experimental import pallas as pl
from jax.experimental.pallas import tpu as pltpu
from jax.sharding import PartitionSpec as P

HEAD_DIM = 64
LANES = 128
TOPK = 8
LOG2E = 1.4426950408889634
norm_eps = 1e-06


def attention_kernel(meta_ref, query_ref, kv_ref, out_ref, tri_ref, acc_ref):
    own, plane = meta_ref[0], meta_ref[1]
    side = tri_ref.shape[0]
    row = lax.broadcasted_iota(jnp.int32, (side, side), 0)
    col = lax.broadcasted_iota(jnp.int32, (side, side), 1)
    tri_ref[...] = (row > col).astype(jnp.bfloat16)

    def key_block(block):
        quarter, place = block // 16, block % 16
        slot = jnp.where((quarter + plane) % 2 == 1, 15 - place, place)
        return kv_ref[slot, quarter]

    def tile(query, block, diagonal):
        kv = key_block(block)
        score = lax.dot_general(
            query, kv, (((1,), (1,)), ((), ())), preferred_element_type=jnp.float32
        ) * (HEAD_DIM**-0.5 * LOG2E)
        cost = jnp.maximum(score, 0.0) + jnp.log2(1.0 + jnp.exp2(-jnp.abs(score)))
        slack = score - cost
        if diagonal is not None:
            live = col + block * side < row + diagonal * side
            cost = jnp.where(live, cost, 0.0)
        high = cost.astype(jnp.bfloat16)
        low = (cost - high.astype(jnp.float32)).astype(jnp.bfloat16)
        tri = tri_ref[...]
        inside = jnp.dot(high, tri, preferred_element_type=jnp.float32) + jnp.dot(
            low, tri, preferred_element_type=jnp.float32
        )
        weight = jnp.exp2(slack - inside)
        if diagonal is not None:
            weight = jnp.where(live, weight, 0.0)
        part = jnp.dot(weight.astype(jnp.bfloat16), kv, preferred_element_type=jnp.float32)
        decay = jnp.exp2(-(inside[:, 0:1] + cost[:, 0:1]))
        return part, decay

    @pl.loop(0, 4)
    def _(quarter):
        block = quarter * 16 + jnp.where(quarter % 2 == 1, 15 - own, own)
        query = query_ref[quarter]
        acc_ref[...] = jnp.zeros_like(acc_ref)

        @pl.loop(0, block // 2)
        def _(pair):
            part0, decay0 = tile(query, pair * 2, None)
            part1, decay1 = tile(query, pair * 2 + 1, None)
            acc_ref[...] = (acc_ref[...] * decay0 + part0) * decay1 + part1

        last = block // 2 * 2
        part0, decay0 = tile(query, last, block)
        part1, decay1 = tile(query, last + 1, block)
        out_ref[quarter] = ((acc_ref[...] * decay0 + part0) * decay1 + part1).astype(jnp.bfloat16)


def attention(meta, query, kv):
    side = query.shape[1]
    pairs = 132 * side * side
    return pl.pallas_call(
        attention_kernel,
        out_shape=jax.ShapeDtypeStruct((4, side, LANES), jnp.bfloat16),
        in_specs=[pl.BlockSpec(memory_space=pltpu.SMEM)] + [pl.BlockSpec(memory_space=pltpu.VMEM)] * 2,
        out_specs=pl.BlockSpec(memory_space=pltpu.VMEM),
        scratch_shapes=[pltpu.VMEM((side, side), jnp.bfloat16), pltpu.VMEM((side, LANES), jnp.float32)],
        compiler_params=pltpu.CompilerParams(vmem_limit_bytes=24 * 2**20),
        cost_estimate=pl.CostEstimate(
            flops=pairs * 2 * 768, bytes_accessed=6 * 2**20, transcendentals=pairs * 3
        ),
        name="attend",
    )(meta, query, kv)


def local(
    queries,
    key_rows,
    value_rows,
    residual,
    out_weight,
    norm_gain,
    routes,
    route_weight,
    expert_gate,
    expert_up,
    expert_down,
    shared_gate,
    shared_up,
    shared_down,
):
    side = queries.shape[0]
    position = lax.axis_index("sp")
    plane = position // 16
    spot = position % 16
    own = jnp.where(plane % 2 == 1, 15 - spot, spot)
    meta = jnp.stack([own, plane]).astype(jnp.int32)
    columns = [[i, 31 - i, 32 + i, 63 - i] for i in range(16)]
    planes = [[16 * z + j for j in range(16)] for z in range(4)]

    def heads(rows):
        return rows.reshape(side, 4, HEAD_DIM).transpose(1, 0, 2)

    query_heads = heads(queries)
    packed = jnp.concatenate(
        [query_heads, jnp.zeros_like(query_heads), heads(key_rows), heads(value_rows)], axis=2
    )
    packed = lax.all_to_all(packed, "sp", 0, 0, axis_index_groups=columns, tiled=True)
    kv = lax.all_gather(packed[:, :, LANES:], "sp", axis_index_groups=planes, axis=0)
    peer = [(0, 1), (1, 0)]
    kv, expert_gate_, expert_up_, expert_down_ = lax.optimization_barrier(
        (kv, expert_gate, expert_up, expert_down)
    )
    gate_other = lax.ppermute(expert_gate_, "tp", peer)
    up_other = lax.ppermute(expert_up_, "tp", peer)
    down_other = lax.ppermute(expert_down_, "tp", peer)
    attended = attention(meta, packed[:, :, :LANES], kv)[:, :, HEAD_DIM:]
    tokens = residual.shape[0]
    eights = [[2 * s + c for s in g for c in range(2)] for g in columns]
    attended = attended.reshape(8, tokens, HEAD_DIM)
    attended = lax.all_to_all(attended, ("sp", "tp"), 0, 0, axis_index_groups=eights, tiled=True)
    attended = attended.reshape(4, 2, tokens, HEAD_DIM).transpose(2, 1, 0, 3).reshape(tokens, 512)

    projected = jnp.dot(attended, out_weight, preferred_element_type=jnp.float32)
    mixed = (residual.astype(jnp.float32) + projected).astype(jnp.bfloat16).astype(jnp.float32)
    inverse = lax.rsqrt(jnp.mean(mixed * mixed, axis=1, keepdims=True) + norm_eps)
    normed = (mixed * inverse * norm_gain).astype(jnp.bfloat16)
    width = normed.shape[1]
    experts = lax.axis_size("sp")
    capacity = 20
    named = routes[:, :, None] == jnp.arange(experts, dtype=jnp.int32)
    pick = jnp.any(named, axis=1)
    share = jnp.sum(jnp.where(named, route_weight[:, :, None], 0.0), axis=1)
    below = jnp.tril(jnp.ones((tokens, tokens), jnp.bfloat16), -1)
    rank = jnp.dot(below, pick.astype(jnp.bfloat16), preferred_element_type=jnp.float32)
    rank = jnp.where(pick, rank, -1.0).T
    slot = rank[:, None, :] == jnp.arange(capacity, dtype=jnp.float32)[None, :, None]
    send = slot.astype(jnp.bfloat16).reshape(experts * capacity, tokens)
    outgoing = jnp.dot(send, normed, preferred_element_type=jnp.bfloat16)
    incoming = lax.all_to_all(
        outgoing.reshape(experts, capacity, width), "sp", 0, 0, tiled=True
    ).reshape(experts * capacity, width)

    def half(gate_half, up_half, down_half):
        gate = jnp.dot(incoming, gate_half[0], preferred_element_type=jnp.float32)
        upward = jnp.dot(incoming, up_half[0], preferred_element_type=jnp.float32)
        hidden = (jax.nn.silu(gate) * upward).astype(jnp.bfloat16)
        return jnp.dot(hidden, down_half[0], preferred_element_type=jnp.float32)

    result = half(expert_gate, expert_up, expert_down) + half(gate_other, up_other, down_other)
    returned = lax.all_to_all(
        result.astype(jnp.bfloat16).reshape(experts, capacity, width), "sp", 0, 0, tiled=True
    ).reshape(experts * capacity, width)
    weighted = jnp.where(slot, share.T[:, None, :], 0.0).reshape(experts * capacity, tokens)
    high = weighted.astype(jnp.bfloat16)
    low = (weighted - high.astype(jnp.float32)).astype(jnp.bfloat16)
    both = jnp.concatenate([high, low], axis=1)
    routed = lax.dot_general(
        both, returned, (((0,), (0,)), ((), ())), preferred_element_type=jnp.float32
    )
    routed = routed[:tokens] + routed[tokens:]
    shared_gate_out = jnp.dot(normed, shared_gate, preferred_element_type=jnp.float32)
    shared_up_out = jnp.dot(normed, shared_up, preferred_element_type=jnp.float32)
    shared_act = (jax.nn.silu(shared_gate_out) * shared_up_out).astype(jnp.bfloat16)
    shared_out = jnp.dot(shared_act, shared_down, preferred_element_type=jnp.float32)
    return (mixed + routed + shared_out).astype(jnp.bfloat16)


def solution(mesh):
    return jax.shard_map(
        local,
        mesh=mesh,
        in_specs=(
            P("sp", "tp"),
            P("sp", "tp"),
            P("sp", "tp"),
            P(("sp", "tp"), None),
            P(),
            P(),
            P(("sp", "tp"), None),
            P(("sp", "tp"), None),
            P("sp", None, "tp"),
            P("sp", None, "tp"),
            P("sp", "tp", None),
            P(),
            P(),
            P(),
        ),
        out_specs=P(("sp", "tp"), None),
        check_vma=False,
    )
```

```python
import jax
import jax.numpy as jnp
from jax import lax
from jax.experimental import pallas as pl
from jax.experimental.pallas import tpu as pltpu
from jax.sharding import PartitionSpec as P

HEAD_DIM = 64
LANES = 128
TOPK = 8
LOG2E = 1.4426950408889634
norm_eps = 1e-06


def attention_kernel(meta_ref, query_ref, kv_ref, out_ref, tri_ref, acc_ref):
    own, plane = meta_ref[0], meta_ref[1]
    side = tri_ref.shape[0]
    row = lax.broadcasted_iota(jnp.int32, (side, side), 0)
    col = lax.broadcasted_iota(jnp.int32, (side, side), 1)
    tri_ref[...] = (row > col).astype(jnp.bfloat16)

    def key_block(block):
        quarter, place = block // 16, block % 16
        slot = jnp.where((quarter + plane) % 2 == 1, 15 - place, place)
        return kv_ref[slot, quarter]

    def tile(query, block, diagonal):
        kv = key_block(block)
        score = lax.dot_general(
            query, kv, (((1,), (1,)), ((), ())), preferred_element_type=jnp.float32
        ) * (HEAD_DIM**-0.5 * LOG2E)
        cost = jnp.maximum(score, 0.0) + jnp.log2(1.0 + jnp.exp2(-jnp.abs(score)))
        slack = score - cost
        if diagonal is not None:
            live = col + block * side < row + diagonal * side
            cost = jnp.where(live, cost, 0.0)
        high = cost.astype(jnp.bfloat16)
        low = (cost - high.astype(jnp.float32)).astype(jnp.bfloat16)
        tri = tri_ref[...]
        inside = jnp.dot(high, tri, preferred_element_type=jnp.float32) + jnp.dot(
            low, tri, preferred_element_type=jnp.float32
        )
        weight = jnp.exp2(slack - inside)
        if diagonal is not None:
            weight = jnp.where(live, weight, 0.0)
        part = jnp.dot(weight.astype(jnp.bfloat16), kv, preferred_element_type=jnp.float32)
        decay = jnp.exp2(-(inside[:, 0:1] + cost[:, 0:1]))
        return part, decay

    @pl.loop(0, 4)
    def _(quarter):
        block = quarter * 16 + jnp.where(quarter % 2 == 1, 15 - own, own)
        query = query_ref[quarter]
        acc_ref[...] = jnp.zeros_like(acc_ref)

        @pl.loop(0, block // 2)
        def _(pair):
            part0, decay0 = tile(query, pair * 2, None)
            part1, decay1 = tile(query, pair * 2 + 1, None)
            acc_ref[...] = (acc_ref[...] * decay0 + part0) * decay1 + part1

        last = block // 2 * 2
        part0, decay0 = tile(query, last, block)
        part1, decay1 = tile(query, last + 1, block)
        out_ref[quarter] = ((acc_ref[...] * decay0 + part0) * decay1 + part1).astype(jnp.bfloat16)


def attention(meta, query, kv):
    side = query.shape[1]
    pairs = 132 * side * side
    return pl.pallas_call(
        attention_kernel,
        out_shape=jax.ShapeDtypeStruct((4, side, LANES), jnp.bfloat16),
        in_specs=[pl.BlockSpec(memory_space=pltpu.SMEM)] + [pl.BlockSpec(memory_space=pltpu.VMEM)] * 2,
        out_specs=pl.BlockSpec(memory_space=pltpu.VMEM),
        scratch_shapes=[pltpu.VMEM((side, side), jnp.bfloat16), pltpu.VMEM((side, LANES), jnp.float32)],
        compiler_params=pltpu.CompilerParams(vmem_limit_bytes=24 * 2**20),
        cost_estimate=pl.CostEstimate(
            flops=pairs * 2 * 768, bytes_accessed=6 * 2**20, transcendentals=pairs * 3
        ),
        name="attend",
    )(meta, query, kv)


MAIN = 16
TAIL = 4


def dispatch_kernel(
    attended_ref, residual_ref, weight_ref, gain_ref, main_ref, tail_ref, mixed_ref, normed_ref, out_ref
):
    half = out_ref.shape[2]

    @pl.when(pl.program_id(0) == 0)
    def _():
        projected = jnp.dot(attended_ref[...], weight_ref[...], preferred_element_type=jnp.float32)
        mixed = (residual_ref[...].astype(jnp.float32) + projected).astype(jnp.bfloat16)
        mixed_ref[...] = mixed
        mixed = mixed.astype(jnp.float32)
        inverse = lax.rsqrt(jnp.mean(mixed * mixed, axis=1, keepdims=True) + norm_eps)
        normed_ref[...] = (mixed * inverse * gain_ref[...]).astype(jnp.bfloat16)

    left, right = normed_ref[:, :half], normed_ref[:, half:]
    experts = out_ref.shape[0]
    main, tail = main_ref[...], tail_ref[...]

    def pick(rows, side):
        return jnp.dot(rows, side, preferred_element_type=jnp.float32)

    out_ref[:, 0:MAIN, :] = pick(main, left).astype(jnp.bfloat16).reshape(experts, MAIN, half)
    out_ref[:, MAIN : 2 * MAIN, :] = pick(main, right).astype(jnp.bfloat16).reshape(experts, MAIN, half)
    first = lax.broadcasted_iota(jnp.int32, (tail.shape[0], half), 0) % (2 * TAIL) < TAIL
    both = jnp.where(first, pick(tail, left), pick(tail, right))
    out_ref[:, 2 * MAIN :, :] = both.astype(jnp.bfloat16).reshape(experts, 2 * TAIL, half)


def dispatch(attended, residual, out_weight, gain, main, tail):
    tokens, width = residual.shape
    experts = main.shape[0] // MAIN
    step = 16
    whole = lambda i: (0, 0)
    return pl.pallas_call(
        dispatch_kernel,
        grid=(experts // step,),
        in_specs=[
            pl.BlockSpec(attended.shape, whole),
            pl.BlockSpec(residual.shape, whole),
            pl.BlockSpec(out_weight.shape, whole),
            pl.BlockSpec(gain.shape, whole),
            pl.BlockSpec((step * MAIN, tokens), lambda i: (i, 0)),
            pl.BlockSpec((step * 2 * TAIL, tokens), lambda i: (i, 0)),
        ],
        out_specs=[
            pl.BlockSpec((tokens, width), whole),
            pl.BlockSpec((tokens, width), whole),
            pl.BlockSpec((step, 2 * (MAIN + TAIL), width // 2), lambda i: (i, 0, 0)),
        ],
        out_shape=[
            jax.ShapeDtypeStruct((tokens, width), jnp.bfloat16),
            jax.ShapeDtypeStruct((tokens, width), jnp.bfloat16),
            jax.ShapeDtypeStruct((experts, 2 * (MAIN + TAIL), width // 2), jnp.bfloat16),
        ],
        compiler_params=pltpu.CompilerParams(vmem_limit_bytes=32 * 2**20),
        cost_estimate=pl.CostEstimate(flops=10**9, bytes_accessed=10**7, transcendentals=0),
        name="dispatch",
    )(attended, residual, out_weight, gain, main, tail)


def expert_kernel(
    rows_ref, gate0_ref, up0_ref, down0_ref, gate1_ref, up1_ref, down1_ref, out_ref, spread_ref, rows2_ref
):
    sources, _, half = rows_ref.shape
    tails = sources * TAIL

    @pl.when(pl.program_id(0) == 0)
    def _():
        row = lax.broadcasted_iota(jnp.int32, (2 * tails, 2 * tails), 0)
        col = lax.broadcasted_iota(jnp.int32, (2 * tails, 2 * tails), 1)
        slot = row % tails
        home = slot // TAIL * (2 * TAIL) + row // tails * TAIL + slot % TAIL
        spread_ref[...] = (home == col).astype(jnp.bfloat16)

    spread = spread_ref[...]
    mains = sources * MAIN
    rows2_ref[:mains, :half] = rows_ref[:, 0:MAIN, :].reshape(mains, half)
    rows2_ref[:mains, half:] = rows_ref[:, MAIN : 2 * MAIN, :].reshape(mains, half)
    ends = jnp.dot(
        spread, rows_ref[:, 2 * MAIN :, :].reshape(2 * tails, half), preferred_element_type=jnp.float32
    ).astype(jnp.bfloat16)
    rows2_ref[mains:, :half] = ends[:tails]
    rows2_ref[mains:, half:] = ends[tails:]
    rows = rows2_ref[...]

    def hidden(gate_ref, up_ref):
        gate = jnp.dot(rows, gate_ref[0], preferred_element_type=jnp.float32)
        upward = jnp.dot(rows, up_ref[0], preferred_element_type=jnp.float32)
        return (jax.nn.silu(gate) * upward).astype(jnp.bfloat16)

    act0 = hidden(gate0_ref, up0_ref)
    act1 = hidden(gate1_ref, up1_ref)
    for part in range(2):
        span = pl.ds(part * half, half)
        result = jnp.dot(act0, down0_ref[0, :, span], preferred_element_type=jnp.float32) + jnp.dot(
            act1, down1_ref[0, :, span], preferred_element_type=jnp.float32
        )
        result = result.astype(jnp.bfloat16)
        out_ref[:, part * MAIN : (part + 1) * MAIN, :] = result[:mains].reshape(sources, MAIN, half)
        if part == 0:
            first = result[mains:]
        else:
            ends = jnp.concatenate([first, result[mains:]], axis=0)
            ends = lax.dot_general(
                spread, ends, (((0,), (0,)), ((), ())), preferred_element_type=jnp.float32
            )
            out_ref[:, 2 * MAIN :, :] = ends.astype(jnp.bfloat16).reshape(sources, 2 * TAIL, half)


def expert(rows, mine, other):
    step = 16
    whole = [pl.BlockSpec(memory_space=pltpu.VMEM)] * 6
    block = pl.BlockSpec((step,) + rows.shape[1:], lambda i: (i, 0, 0))
    return pl.pallas_call(
        expert_kernel,
        grid=(rows.shape[0] // step,),
        in_specs=[block] + whole,
        out_specs=block,
        out_shape=jax.ShapeDtypeStruct(rows.shape, jnp.bfloat16),
        scratch_shapes=[
            pltpu.VMEM((step * 2 * TAIL, step * 2 * TAIL), jnp.bfloat16),
            pltpu.VMEM((step * (MAIN + TAIL), 2 * rows.shape[2]), jnp.bfloat16),
        ],
        compiler_params=pltpu.CompilerParams(vmem_limit_bytes=32 * 2**20),
        cost_estimate=pl.CostEstimate(flops=8 * 10**9, bytes_accessed=17 * 10**6, transcendentals=10**6),
        name="expert",
    )(rows, *mine, *other)


def combine_kernel(rows_ref, main_ref, left_ref, right_ref, base_ref, out_ref, acc_ref):
    sources, _, half = rows_ref.shape
    tokens = base_ref.shape[0]
    at = pl.program_id(0)

    @pl.when(at == 0)
    def _():
        acc_ref[...] = base_ref[...]

    ends = rows_ref[:, 2 * MAIN :, :].reshape(sources * 2 * TAIL, half)
    for part, tail_ref in ((0, left_ref), (1, right_ref)):
        rows = rows_ref[:, part * MAIN : (part + 1) * MAIN, :].reshape(sources * MAIN, half)
        total = jnp.dot(main_ref[...], rows, preferred_element_type=jnp.float32) + jnp.dot(
            tail_ref[...], ends, preferred_element_type=jnp.float32
        )
        span = pl.ds(part * half, half)
        acc_ref[:, span] += total[:tokens] + total[tokens:]

    @pl.when(at == pl.num_programs(0) - 1)
    def _():
        out_ref[...] = acc_ref[...].astype(jnp.bfloat16)


def combine(rows, main, left, right, base):
    step = 16
    whole = lambda i: (0, 0)
    return pl.pallas_call(
        combine_kernel,
        grid=(rows.shape[0] // step,),
        in_specs=[
            pl.BlockSpec((step,) + rows.shape[1:], lambda i: (i, 0, 0)),
            pl.BlockSpec((main.shape[0], step * MAIN), lambda i: (0, i)),
            pl.BlockSpec((main.shape[0], step * 2 * TAIL), lambda i: (0, i)),
            pl.BlockSpec((main.shape[0], step * 2 * TAIL), lambda i: (0, i)),
            pl.BlockSpec(base.shape, whole),
        ],
        out_specs=pl.BlockSpec(base.shape, whole),
        out_shape=jax.ShapeDtypeStruct(base.shape, jnp.bfloat16),
        scratch_shapes=[pltpu.VMEM(base.shape, jnp.float32)],
        compiler_params=pltpu.CompilerParams(vmem_limit_bytes=32 * 2**20),
        cost_estimate=pl.CostEstimate(flops=10**9, bytes_accessed=10**7, transcendentals=0),
        name="combine",
    )(rows, main, left, right, base)


def local(
    queries,
    key_rows,
    value_rows,
    residual,
    out_weight,
    norm_gain,
    routes,
    route_weight,
    expert_gate,
    expert_up,
    expert_down,
    shared_gate,
    shared_up,
    shared_down,
):
    side = queries.shape[0]
    position = lax.axis_index("sp")
    plane = position // 16
    spot = position % 16
    own = jnp.where(plane % 2 == 1, 15 - spot, spot)
    meta = jnp.stack([own, plane]).astype(jnp.int32)
    columns = [[i, 31 - i, 32 + i, 63 - i] for i in range(16)]
    planes = [[16 * z + j for j in range(16)] for z in range(4)]

    def heads(rows):
        return rows.reshape(side, 4, HEAD_DIM).transpose(1, 0, 2)

    query_heads = heads(queries)
    packed = jnp.concatenate(
        [query_heads, jnp.zeros_like(query_heads), heads(key_rows), heads(value_rows)], axis=2
    )
    packed = lax.all_to_all(packed, "sp", 0, 0, axis_index_groups=columns, tiled=True)
    kv = lax.all_gather(packed[:, :, LANES:], "sp", axis_index_groups=planes, axis=0)
    peer = [(0, 1), (1, 0)]
    kv, expert_gate_, expert_up_, expert_down_ = lax.optimization_barrier(
        (kv, expert_gate, expert_up, expert_down)
    )
    gate_other = lax.ppermute(expert_gate_, "tp", peer)
    up_other = lax.ppermute(expert_up_, "tp", peer)
    down_other = lax.ppermute(expert_down_, "tp", peer)
    attended = attention(meta, packed[:, :, :LANES], kv)[:, :, HEAD_DIM:]
    tokens = residual.shape[0]
    eights = [[2 * s + c for s in g for c in range(2)] for g in columns]
    attended = attended.reshape(8, tokens, HEAD_DIM)
    attended = lax.all_to_all(attended, ("sp", "tp"), 0, 0, axis_index_groups=eights, tiled=True)
    attended = attended.reshape(4, 2, tokens, HEAD_DIM).transpose(2, 1, 0, 3).reshape(tokens, 512)

    experts = lax.axis_size("sp")
    named = routes[:, :, None] == jnp.arange(experts, dtype=jnp.int32)
    pick = jnp.any(named, axis=1)
    share = jnp.sum(jnp.where(named, route_weight[:, :, None], 0.0), axis=1)
    below = jnp.tril(jnp.ones((tokens, tokens), jnp.bfloat16), -1)
    rank = jnp.dot(below, pick.astype(jnp.bfloat16), preferred_element_type=jnp.float32)
    rank = jnp.where(pick, rank, -1.0).astype(jnp.int32)

    def slots(numbers):
        numbers = jnp.asarray(numbers, jnp.int32)
        send = rank.T[:, None, :] == numbers[None, :, None]
        back = rank[:, :, None] == numbers[None, None, :]
        send = send.astype(jnp.bfloat16).reshape(-1, tokens)
        weight = jnp.where(back, share[:, :, None], 0.0).reshape(tokens, -1)
        high = weight.astype(jnp.bfloat16)
        low = (weight - high.astype(jnp.float32)).astype(jnp.bfloat16)
        return send, jnp.concatenate([high, low], axis=0)

    ends = list(range(MAIN, MAIN + TAIL))
    none = [-2] * TAIL
    send_main, back_main = slots(list(range(MAIN)))
    send_tail, _ = slots(ends + ends)
    _, back_left = slots(ends + none)
    _, back_right = slots(none + ends)
    mixed, normed, outgoing = dispatch(
        attended, residual, out_weight, norm_gain[None, :], send_main, send_tail
    )
    incoming = lax.all_to_all(outgoing, "sp", 0, 0, tiled=True)
    shared_gate_out = jnp.dot(normed, shared_gate, preferred_element_type=jnp.float32)
    shared_up_out = jnp.dot(normed, shared_up, preferred_element_type=jnp.float32)
    shared_act = (jax.nn.silu(shared_gate_out) * shared_up_out).astype(jnp.bfloat16)
    base = mixed.astype(jnp.float32) + jnp.dot(
        shared_act, shared_down, preferred_element_type=jnp.float32
    )
    result = expert(
        incoming, (expert_gate, expert_up, expert_down), (gate_other, up_other, down_other)
    )
    returned = lax.all_to_all(result, "sp", 0, 0, tiled=True)
    return combine(returned, back_main, back_left, back_right, base)


def solution(mesh):
    return jax.shard_map(
        local,
        mesh=mesh,
        in_specs=(
            P("sp", "tp"),
            P("sp", "tp"),
            P("sp", "tp"),
            P(("sp", "tp"), None),
            P(),
            P(),
            P(("sp", "tp"), None),
            P(("sp", "tp"), None),
            P("sp", None, "tp"),
            P("sp", None, "tp"),
            P("sp", "tp", None),
            P(),
            P(),
            P(),
        ),
        out_specs=P(("sp", "tp"), None),
        check_vma=False,
    )
```

```python
import jax
import jax.numpy as jnp
from jax import lax
from jax.experimental import pallas as pl
from jax.experimental.pallas import tpu as pltpu
from jax.sharding import PartitionSpec as P

HEAD_DIM = 64
LANES = 128
TOPK = 8
LOG2E = 1.4426950408889634
norm_eps = 1e-06


def pack_kernel(core_ref, query_ref, key_ref, value_ref, query_out, keep_out, send_out):
    core = core_ref[0]
    heads, rows, _ = keep_out.shape
    mine, peers = pl.ds(core * rows, rows), pl.ds((1 - core) * rows, rows)
    for head in range(heads):
        span = slice(head * HEAD_DIM, (head + 1) * HEAD_DIM)
        query = query_ref[:, span]
        query_out[head] = jnp.concatenate([query, jnp.zeros_like(query)], axis=1)
        keep_out[head] = jnp.concatenate([key_ref[mine, span], value_ref[mine, span]], axis=1)
        send_out[head] = jnp.concatenate([key_ref[peers, span], value_ref[peers, span]], axis=1)


def pack(core, queries, key_rows, value_rows):
    side, width = queries.shape
    heads = width // HEAD_DIM
    half = jax.ShapeDtypeStruct((heads, side // 2, LANES), jnp.bfloat16)
    return pl.pallas_call(
        pack_kernel,
        in_specs=[pl.BlockSpec(memory_space=pltpu.SMEM)] + [pl.BlockSpec(memory_space=pltpu.VMEM)] * 3,
        out_specs=[pl.BlockSpec(memory_space=pltpu.VMEM)] * 3,
        out_shape=[jax.ShapeDtypeStruct((heads, side, LANES), jnp.bfloat16), half, half],
        name="pack",
    )(core, queries, key_rows, value_rows)


GROUP = 4


def attention_kernel(meta_ref, q0, q1, q2, q3, mine_ref, peer_ref, out_ref, kv_ref, tri_ref, query_ref, acc_ref, sems):
    core = meta_ref[0]
    side = tri_ref.shape[0]
    rows = mine_ref.shape[1]
    loads = [
        pltpu.make_async_copy(mine_ref, kv_ref.at[:, pl.ds(core * rows, rows)], sems.at[0]),
        pltpu.make_async_copy(peer_ref, kv_ref.at[:, pl.ds((1 - core) * rows, rows)], sems.at[1]),
    ]
    for load in loads:
        load.start()
    row = lax.broadcasted_iota(jnp.int32, (side, side), 0)
    col = lax.broadcasted_iota(jnp.int32, (side, side), 1)
    tri_ref[...] = (row > col).astype(jnp.float32)
    for turn, ref in enumerate((q0, q1, q2, q3)):
        query_ref[turn] = ref[...]
    for load in loads:
        load.wait()

    def advance(query, first, own):
        keys = [kv_ref[first + i] for i in range(GROUP)]
        scores = [
            lax.dot_general(query, kv, (((1,), (1,)), ((), ())), preferred_element_type=jnp.float32)
            * (HEAD_DIM**-0.5 * LOG2E)
            for kv in keys
        ]
        costs = [jnp.maximum(s, 0.0) + jnp.log2(1.0 + jnp.exp2(-jnp.abs(s))) for s in scores]
        slacks = [s - c for s, c in zip(scores, costs)]
        if own is not None:
            live = [col + (first + i - own) * side < row for i in range(GROUP)]
            costs = [jnp.where(l, c, 0.0) for l, c in zip(live, costs)]
        tri = tri_ref[...]
        insides = [jnp.dot(c, tri, preferred_element_type=jnp.float32) for c in costs]
        acc = acc_ref[...]
        for i in range(GROUP):
            weight = jnp.exp2(slacks[i] - insides[i])
            if own is not None:
                weight = jnp.where(live[i], weight, 0.0)
            part = jnp.dot(weight.astype(jnp.bfloat16), keys[i], preferred_element_type=jnp.float32)
            acc = acc * jnp.exp2(-(insides[i][:, 0:1] + costs[i][:, 0:1])) + part
        acc_ref[...] = acc

    @pl.loop(0, 4)
    def _(turn):
        own = meta_ref[1 + turn]
        query = query_ref[turn]
        acc_ref[...] = jnp.zeros_like(acc_ref)

        @pl.loop(0, own // GROUP)
        def _(step):
            advance(query, step * GROUP, None)

        advance(query, own // GROUP * GROUP, own)
        done = acc_ref[:, HEAD_DIM:].astype(jnp.bfloat16)
        slot = meta_ref[5 + turn]
        out_ref[slot] = done[:rows]
        out_ref[slot + 1] = done[rows:]


def attention(meta, queries, mine, peer):
    side = queries[0].shape[0]
    pairs = 136 * side * side
    return pl.pallas_call(
        attention_kernel,
        out_shape=jax.ShapeDtypeStruct((16, side // 2, HEAD_DIM), jnp.bfloat16),
        in_specs=[pl.BlockSpec(memory_space=pltpu.SMEM)]
        + [pl.BlockSpec(memory_space=pltpu.VMEM)] * 4
        + [pl.BlockSpec(memory_space=pl.ANY)] * 2,
        out_specs=pl.BlockSpec(memory_space=pltpu.VMEM),
        scratch_shapes=[
            pltpu.VMEM((mine.shape[0], side, LANES), jnp.bfloat16),
            pltpu.VMEM((side, side), jnp.float32),
            pltpu.VMEM((4, side, LANES), jnp.bfloat16),
            pltpu.VMEM((side, LANES), jnp.float32),
            pltpu.SemaphoreType.DMA((2,)),
        ],
        compiler_params=pltpu.CompilerParams(vmem_limit_bytes=56 * 2**20),
        cost_estimate=pl.CostEstimate(
            flops=pairs * 2 * 768, bytes_accessed=6 * 2**20, transcendentals=pairs * 3
        ),
        name="attend",
    )(meta, *queries, mine, peer)


MAIN = 16
TAIL = 4


def dispatch_kernel(
    side_ref,
    attended_ref,
    residual_ref,
    weight_ref,
    gain_ref,
    main_ref,
    tail_ref,
    mixed_ref,
    normed_ref,
    out_ref,
    heads_ref,
):
    half = out_ref.shape[2]

    @pl.when(pl.program_id(0) == 0)
    def _():
        for head in range(8):
            heads_ref[:, head * HEAD_DIM : (head + 1) * HEAD_DIM] = attended_ref[2 * head + side_ref[0]]
        projected = jnp.dot(heads_ref[...], weight_ref[...], preferred_element_type=jnp.float32)
        mixed = (residual_ref[...].astype(jnp.float32) + projected).astype(jnp.bfloat16)
        mixed_ref[...] = mixed
        mixed = mixed.astype(jnp.float32)
        inverse = lax.rsqrt(jnp.mean(mixed * mixed, axis=1, keepdims=True) + norm_eps)
        normed_ref[...] = (mixed * inverse * gain_ref[...]).astype(jnp.bfloat16)

    left, right = normed_ref[:, :half], normed_ref[:, half:]
    experts = out_ref.shape[0]
    main, tail = main_ref[...], tail_ref[...]

    def pick(rows, side):
        return jnp.dot(rows, side, preferred_element_type=jnp.float32)

    out_ref[:, 0:MAIN, :] = pick(main, left).astype(jnp.bfloat16).reshape(experts, MAIN, half)
    out_ref[:, MAIN : 2 * MAIN, :] = pick(main, right).astype(jnp.bfloat16).reshape(experts, MAIN, half)
    first = lax.broadcasted_iota(jnp.int32, (tail.shape[0], half), 0) % (2 * TAIL) < TAIL
    both = jnp.where(first, pick(tail, left), pick(tail, right))
    out_ref[:, 2 * MAIN :, :] = both.astype(jnp.bfloat16).reshape(experts, 2 * TAIL, half)


def dispatch(side, attended, residual, out_weight, gain, main, tail):
    tokens, width = residual.shape
    experts = main.shape[0] // MAIN
    step = 16
    whole = lambda i: (0, 0)
    return pl.pallas_call(
        dispatch_kernel,
        grid=(experts // step,),
        in_specs=[
            pl.BlockSpec(memory_space=pltpu.SMEM),
            pl.BlockSpec(attended.shape, lambda i: (0, 0, 0)),
            pl.BlockSpec(residual.shape, whole),
            pl.BlockSpec(out_weight.shape, whole),
            pl.BlockSpec(gain.shape, whole),
            pl.BlockSpec((step * MAIN, tokens), lambda i: (i, 0)),
            pl.BlockSpec((step * 2 * TAIL, tokens), lambda i: (i, 0)),
        ],
        out_specs=[
            pl.BlockSpec((tokens, width), whole),
            pl.BlockSpec((tokens, width), whole),
            pl.BlockSpec((step, 2 * (MAIN + TAIL), width // 2), lambda i: (i, 0, 0)),
        ],
        out_shape=[
            jax.ShapeDtypeStruct((tokens, width), jnp.bfloat16),
            jax.ShapeDtypeStruct((tokens, width), jnp.bfloat16),
            jax.ShapeDtypeStruct((experts, 2 * (MAIN + TAIL), width // 2), jnp.bfloat16),
        ],
        scratch_shapes=[pltpu.VMEM((tokens, 8 * HEAD_DIM), jnp.bfloat16)],
        compiler_params=pltpu.CompilerParams(vmem_limit_bytes=60 * 2**20),
        cost_estimate=pl.CostEstimate(flops=10**9, bytes_accessed=10**7, transcendentals=0),
        name="dispatch",
    )(side, attended, residual, out_weight, gain, main, tail)


def expert_kernel(
    rows_ref,
    gate0,
    up0,
    gate1,
    up1,
    down0,
    down1,
    out_ref,
    spread_ref,
    rows2_ref,
    gate0_ref,
    up0_ref,
    gate1_ref,
    up1_ref,
    down0_ref,
    down1_ref,
    sems,
):
    sources, _, half = rows_ref.shape
    tails = sources * TAIL
    first_step = pl.program_id(0) == 0
    loads = [
        pltpu.make_async_copy(source, target, sems.at[i])
        for i, (source, target) in enumerate(
            (
                (gate0, gate0_ref),
                (up0, up0_ref),
                (gate1, gate1_ref),
                (up1, up1_ref),
                (down0, down0_ref),
                (down1, down1_ref),
            )
        )
    ]

    def arrived(*which):
        @pl.when(first_step)
        def _():
            for i in which:
                loads[i].wait()

    @pl.when(first_step)
    def _():
        for load in loads:
            load.start()
        row = lax.broadcasted_iota(jnp.int32, (2 * tails, 2 * tails), 0)
        col = lax.broadcasted_iota(jnp.int32, (2 * tails, 2 * tails), 1)
        slot = row % tails
        home = slot // TAIL * (2 * TAIL) + row // tails * TAIL + slot % TAIL
        spread_ref[...] = (home == col).astype(jnp.bfloat16)

    spread = spread_ref[...]
    mains = sources * MAIN
    rows2_ref[:mains, :half] = rows_ref[:, 0:MAIN, :].reshape(mains, half)
    rows2_ref[:mains, half:] = rows_ref[:, MAIN : 2 * MAIN, :].reshape(mains, half)
    ends = jnp.dot(
        spread, rows_ref[:, 2 * MAIN :, :].reshape(2 * tails, half), preferred_element_type=jnp.float32
    ).astype(jnp.bfloat16)
    rows2_ref[mains:, :half] = ends[:tails]
    rows2_ref[mains:, half:] = ends[tails:]
    rows = rows2_ref[...]

    def hidden(gate_ref, up_ref):
        gate = jnp.dot(rows, gate_ref[0], preferred_element_type=jnp.float32)
        upward = jnp.dot(rows, up_ref[0], preferred_element_type=jnp.float32)
        return (jax.nn.silu(gate) * upward).astype(jnp.bfloat16)

    arrived(0, 1)
    act0 = hidden(gate0_ref, up0_ref)
    arrived(2, 3)
    act1 = hidden(gate1_ref, up1_ref)
    arrived(4, 5)
    for part in range(2):
        span = pl.ds(part * half, half)
        result = jnp.dot(act0, down0_ref[0, :, span], preferred_element_type=jnp.float32) + jnp.dot(
            act1, down1_ref[0, :, span], preferred_element_type=jnp.float32
        )
        result = result.astype(jnp.bfloat16)
        out_ref[:, part * MAIN : (part + 1) * MAIN, :] = result[:mains].reshape(sources, MAIN, half)
        if part == 0:
            first = result[mains:]
        else:
            ends = jnp.concatenate([first, result[mains:]], axis=0)
            ends = lax.dot_general(
                spread, ends, (((0,), (0,)), ((), ())), preferred_element_type=jnp.float32
            )
            out_ref[:, 2 * MAIN :, :] = ends.astype(jnp.bfloat16).reshape(sources, 2 * TAIL, half)


def expert(rows, weights):
    step = 16
    block = pl.BlockSpec((step,) + rows.shape[1:], lambda i: (i, 0, 0))
    return pl.pallas_call(
        expert_kernel,
        grid=(rows.shape[0] // step,),
        in_specs=[block] + [pl.BlockSpec(memory_space=pl.ANY)] * 6,
        out_specs=block,
        out_shape=jax.ShapeDtypeStruct(rows.shape, jnp.bfloat16),
        scratch_shapes=[
            pltpu.VMEM((step * 2 * TAIL, step * 2 * TAIL), jnp.bfloat16),
            pltpu.VMEM((step * (MAIN + TAIL), 2 * rows.shape[2]), jnp.bfloat16),
        ]
        + [pltpu.VMEM(w.shape, w.dtype) for w in weights]
        + [pltpu.SemaphoreType.DMA((6,))],
        compiler_params=pltpu.CompilerParams(vmem_limit_bytes=60 * 2**20),
        cost_estimate=pl.CostEstimate(flops=8 * 10**9, bytes_accessed=17 * 10**6, transcendentals=10**6),
        name="expert",
    )(rows, *weights)


def combine_kernel(rows_ref, main_ref, left_ref, right_ref, base_ref, out_ref, acc_ref):
    sources, _, half = rows_ref.shape
    tokens = base_ref.shape[0]
    at = pl.program_id(0)

    @pl.when(at == 0)
    def _():
        acc_ref[...] = base_ref[...]

    ends = rows_ref[:, 2 * MAIN :, :].reshape(sources * 2 * TAIL, half)
    for part, tail_ref in ((0, left_ref), (1, right_ref)):
        rows = rows_ref[:, part * MAIN : (part + 1) * MAIN, :].reshape(sources * MAIN, half)
        total = jnp.dot(main_ref[...], rows, preferred_element_type=jnp.float32) + jnp.dot(
            tail_ref[...], ends, preferred_element_type=jnp.float32
        )
        span = pl.ds(part * half, half)
        acc_ref[:, span] += total[:tokens] + total[tokens:]

    @pl.when(at == pl.num_programs(0) - 1)
    def _():
        out_ref[...] = acc_ref[...].astype(jnp.bfloat16)


def combine(rows, main, left, right, base):
    step = 16
    whole = lambda i: (0, 0)
    return pl.pallas_call(
        combine_kernel,
        grid=(rows.shape[0] // step,),
        in_specs=[
            pl.BlockSpec((step,) + rows.shape[1:], lambda i: (i, 0, 0)),
            pl.BlockSpec((main.shape[0], step * MAIN), lambda i: (0, i)),
            pl.BlockSpec((main.shape[0], step * 2 * TAIL), lambda i: (0, i)),
            pl.BlockSpec((main.shape[0], step * 2 * TAIL), lambda i: (0, i)),
            pl.BlockSpec(base.shape, whole),
        ],
        out_specs=pl.BlockSpec(base.shape, whole),
        out_shape=jax.ShapeDtypeStruct(base.shape, jnp.bfloat16),
        scratch_shapes=[pltpu.VMEM(base.shape, jnp.float32)],
        compiler_params=pltpu.CompilerParams(vmem_limit_bytes=60 * 2**20),
        cost_estimate=pl.CostEstimate(flops=10**9, bytes_accessed=10**7, transcendentals=0),
        name="combine",
    )(rows, main, left, right, base)


def local(
    queries,
    key_rows,
    value_rows,
    residual,
    out_weight,
    norm_gain,
    routes,
    route_weight,
    expert_gate,
    expert_up,
    expert_down,
    shared_gate,
    shared_up,
    shared_down,
):
    chips = [[i, 31 - i, 32 + i, 63 - i, 8 + i, 23 - i, 40 + i, 55 - i] for i in range(8)]
    devices = [[2 * s + c for s in g for c in range(2)] for g in chips]
    core = lax.axis_index("tp")
    position = lax.axis_index("sp")
    plane, spot = position // 16, position % 16
    place = jnp.where(plane % 2 == 1, 15 - spot, spot)
    group, member = place % 8, plane + place // 8 * 4

    query_heads, keep, send = pack(core[None].astype(jnp.int32), queries, key_rows, value_rows)
    swap = [(0, 1), (1, 0)]
    taken = lax.ppermute(send, "tp", swap)
    low, high = jnp.where(core == 0, keep, taken), jnp.where(core == 0, taken, keep)
    order = jnp.stack([low[0], high[0], high[1], low[1], low[2], high[2], high[3], low[3]])
    order = jnp.broadcast_to(order[:, None], (8,) + order.shape)
    mine = lax.all_to_all(order.reshape((64,) + order.shape[2:]), "sp", 0, 0, tiled=True)
    turns = []
    for turn in range(4):
        pairs = [
            (devices[g][2 * m + c], devices[g][2 * (4 * c + ((m % 4) ^ turn)) + m // 4])
            for g in range(8)
            for m in range(8)
            for c in range(2)
        ]
        head = lax.dynamic_index_in_dim(query_heads, (member % 4) ^ turn, 0, keepdims=False)
        turns.append(lax.ppermute(head, ("sp", "tp"), pairs))
    peer = lax.ppermute(mine, "tp", swap)
    sender = [4 * core + ((member % 4) ^ turn) for turn in range(4)]
    block = [
        16 * (m % 4) + jnp.where(m % 2 == 1, 15 - group - m // 4 * 8, group + m // 4 * 8) for m in sender
    ]
    meta = jnp.stack([core] + block + [2 * m for m in sender]).astype(jnp.int32)
    attended = attention(meta, turns, mine, peer)
    peer, expert_gate_, expert_up_, expert_down_ = lax.optimization_barrier(
        (peer, expert_gate, expert_up, expert_down)
    )
    gate_other = lax.ppermute(expert_gate_, "tp", swap)
    up_other = lax.ppermute(expert_up_, "tp", swap)
    down_other = lax.ppermute(expert_down_, "tp", swap)
    tokens = residual.shape[0]
    attended = lax.all_to_all(attended, ("sp", "tp"), 0, 0, axis_index_groups=devices, tiled=True)
    side = (member // 4)[None].astype(jnp.int32)

    experts = lax.axis_size("sp")
    named = routes[:, :, None] == jnp.arange(experts, dtype=jnp.int32)
    pick = jnp.any(named, axis=1)
    share = jnp.sum(jnp.where(named, route_weight[:, :, None], 0.0), axis=1)
    below = jnp.tril(jnp.ones((tokens, tokens), jnp.bfloat16), -1)
    rank = jnp.dot(below, pick.astype(jnp.bfloat16), preferred_element_type=jnp.float32)
    rank = jnp.where(pick, rank, -1.0).astype(jnp.int32)

    def slots(numbers):
        numbers = jnp.asarray(numbers, jnp.int32)
        send = rank.T[:, None, :] == numbers[None, :, None]
        back = rank[:, :, None] == numbers[None, None, :]
        send = send.astype(jnp.bfloat16).reshape(-1, tokens)
        weight = jnp.where(back, share[:, :, None], 0.0).reshape(tokens, -1)
        high = weight.astype(jnp.bfloat16)
        low = (weight - high.astype(jnp.float32)).astype(jnp.bfloat16)
        return send, jnp.concatenate([high, low], axis=0)

    ends = list(range(MAIN, MAIN + TAIL))
    none = [-2] * TAIL
    send_main, back_main = slots(list(range(MAIN)))
    send_tail, _ = slots(ends + ends)
    _, back_left = slots(ends + none)
    _, back_right = slots(none + ends)
    mixed, normed, outgoing = dispatch(
        side, attended, residual, out_weight, norm_gain[None, :], send_main, send_tail
    )
    incoming = lax.all_to_all(outgoing, "sp", 0, 0, tiled=True)
    shared_gate_out = jnp.dot(normed, shared_gate, preferred_element_type=jnp.float32)
    shared_up_out = jnp.dot(normed, shared_up, preferred_element_type=jnp.float32)
    shared_act = (jax.nn.silu(shared_gate_out) * shared_up_out).astype(jnp.bfloat16)
    base = mixed.astype(jnp.float32) + jnp.dot(
        shared_act, shared_down, preferred_element_type=jnp.float32
    )
    result = expert(
        incoming, (expert_gate, expert_up, gate_other, up_other, expert_down, down_other)
    )
    returned = lax.all_to_all(result, "sp", 0, 0, tiled=True)
    return combine(returned, back_main, back_left, back_right, base)


def solution(mesh):
    return jax.shard_map(
        local,
        mesh=mesh,
        in_specs=(
            P("sp", "tp"),
            P("sp", "tp"),
            P("sp", "tp"),
            P(("sp", "tp"), None),
            P(),
            P(),
            P(("sp", "tp"), None),
            P(("sp", "tp"), None),
            P("sp", None, "tp"),
            P("sp", None, "tp"),
            P("sp", "tp", None),
            P(),
            P(),
            P(),
        ),
        out_specs=P(("sp", "tp"), None),
        check_vma=False,
    )
```

```python
import jax
import jax.numpy as jnp
from jax import lax
from jax.experimental import pallas as pl
from jax.experimental.pallas import tpu as pltpu
from jax.sharding import PartitionSpec as P

HEAD_DIM = 64
LANES = 128
TOPK = 8
LOG2E = 1.4426950408889634
norm_eps = 1e-06


def pack_kernel(meta_ref, key_ref, value_ref, keep_out, send_out):
    core = meta_ref[0]
    heads, rows, _ = keep_out.shape
    mine, peers = pl.ds(core * rows, rows), pl.ds((1 - core) * rows, rows)
    for head in range(heads):
        span = slice(head * HEAD_DIM, (head + 1) * HEAD_DIM)
        keep_out[head] = jnp.concatenate([key_ref[mine, span], value_ref[mine, span]], axis=1)
        send_out[head] = jnp.concatenate([key_ref[peers, span], value_ref[peers, span]], axis=1)


def pack(meta, key_rows, value_rows):
    side, width = key_rows.shape
    heads = width // HEAD_DIM
    half = jax.ShapeDtypeStruct((heads, side // 2, LANES), jnp.bfloat16)
    return pl.pallas_call(
        pack_kernel,
        in_specs=[pl.BlockSpec(memory_space=pltpu.SMEM)] + [pl.BlockSpec(memory_space=pltpu.VMEM)] * 2,
        out_specs=[pl.BlockSpec(memory_space=pltpu.VMEM)] * 2,
        out_shape=[half, half],
        name="pack",
    )(meta, key_rows, value_rows)


def turn_kernel(meta_ref, query_ref, *refs):
    outs, held_ref = refs[:-1], refs[-1]
    for head in range(4):
        query = query_ref[:, head * HEAD_DIM : (head + 1) * HEAD_DIM]
        held_ref[head] = jnp.concatenate([query, jnp.zeros_like(query)], axis=1)
    for turn, out in enumerate(outs):
        out[...] = held_ref[meta_ref[1] ^ turn]


def split_queries(meta, queries):
    side = queries.shape[0]
    return pl.pallas_call(
        turn_kernel,
        in_specs=[pl.BlockSpec(memory_space=pltpu.SMEM), pl.BlockSpec(memory_space=pltpu.VMEM)],
        out_specs=[pl.BlockSpec(memory_space=pltpu.VMEM)] * 4,
        out_shape=[jax.ShapeDtypeStruct((side, LANES), jnp.bfloat16)] * 4,
        scratch_shapes=[pltpu.VMEM((4, side, LANES), jnp.bfloat16)],
        name="turns",
    )(meta, queries)


def route_kernel(routes_ref, weight_ref, out_ref):
    tokens, experts = routes_ref.shape[0], out_ref.shape[1]
    names = lax.broadcasted_iota(jnp.int32, (tokens, experts), 1)
    pick = jnp.zeros((tokens, experts), jnp.float32)
    share = jnp.zeros((tokens, experts), jnp.float32)
    for k in range(TOPK):
        named = routes_ref[:, k : k + 1] == names
        pick = jnp.where(named, 1.0, pick)
        share = jnp.where(named, weight_ref[:, k : k + 1], share)
    row = lax.broadcasted_iota(jnp.int32, (tokens, tokens), 0)
    col = lax.broadcasted_iota(jnp.int32, (tokens, tokens), 1)
    below = (col < row).astype(jnp.bfloat16)
    rank = jnp.dot(below, pick.astype(jnp.bfloat16), preferred_element_type=jnp.float32)
    out_ref[0:tokens] = jnp.where(pick > 0.0, rank, -1.0).astype(jnp.bfloat16)
    high = share.astype(jnp.bfloat16)
    out_ref[tokens : 2 * tokens] = high
    out_ref[2 * tokens :] = (share - high.astype(jnp.float32)).astype(jnp.bfloat16)


def route(routes, route_weight, experts):
    return pl.pallas_call(
        route_kernel,
        out_shape=jax.ShapeDtypeStruct((3 * routes.shape[0], experts), jnp.bfloat16),
        in_specs=[pl.BlockSpec(memory_space=pltpu.VMEM)] * 2,
        out_specs=pl.BlockSpec(memory_space=pltpu.VMEM),
        name="route",
    )(routes, route_weight)


GROUP = 4


def attention_kernel(meta_ref, q0, q1, q2, q3, mine_ref, peer_ref, out_ref, kv_ref, tri_ref, query_ref, acc_ref, sems):
    core = meta_ref[0]
    side = tri_ref.shape[0]
    rows = mine_ref.shape[1]
    loads = [
        pltpu.make_async_copy(mine_ref, kv_ref.at[:, pl.ds(core * rows, rows)], sems.at[0]),
        pltpu.make_async_copy(peer_ref, kv_ref.at[:, pl.ds((1 - core) * rows, rows)], sems.at[1]),
    ]
    for load in loads:
        load.start()
    row = lax.broadcasted_iota(jnp.int32, (side, side), 0)
    col = lax.broadcasted_iota(jnp.int32, (side, side), 1)
    tri_ref[...] = (row > col).astype(jnp.float32)
    for turn, ref in enumerate((q0, q1, q2, q3)):
        query_ref[turn] = ref[...]
    for load in loads:
        load.wait()

    def advance(query, first, own):
        keys = [kv_ref[first + i] for i in range(GROUP)]
        scores = [
            lax.dot_general(query, kv, (((1,), (1,)), ((), ())), preferred_element_type=jnp.float32)
            * (HEAD_DIM**-0.5 * LOG2E)
            for kv in keys
        ]
        costs = [jnp.maximum(s, 0.0) + jnp.log2(1.0 + jnp.exp2(-jnp.abs(s))) for s in scores]
        slacks = [s - c for s, c in zip(scores, costs)]
        if own is not None:
            live = [col + (first + i - own) * side < row for i in range(GROUP)]
            costs = [jnp.where(l, c, 0.0) for l, c in zip(live, costs)]
        tri = tri_ref[...]
        insides = [jnp.dot(c, tri, preferred_element_type=jnp.float32) for c in costs]
        acc = acc_ref[...]
        for i in range(GROUP):
            weight = jnp.exp2(slacks[i] - insides[i])
            if own is not None:
                weight = jnp.where(live[i], weight, 0.0)
            part = jnp.dot(weight.astype(jnp.bfloat16), keys[i], preferred_element_type=jnp.float32)
            acc = acc * jnp.exp2(-(insides[i][:, 0:1] + costs[i][:, 0:1])) + part
        acc_ref[...] = acc

    @pl.loop(0, 4)
    def _(turn):
        own = meta_ref[1 + turn]
        query = query_ref[turn]
        acc_ref[...] = jnp.zeros_like(acc_ref)

        @pl.loop(0, own // GROUP)
        def _(step):
            advance(query, step * GROUP, None)

        advance(query, own // GROUP * GROUP, own)
        done = acc_ref[...].T[HEAD_DIM:].astype(jnp.bfloat16)
        slot = meta_ref[5 + turn]
        out_ref[slot] = done[:, :rows]
        out_ref[slot + 1] = done[:, rows:]


def attention(meta, queries, mine, peer):
    side = queries[0].shape[0]
    pairs = 136 * side * side
    return pl.pallas_call(
        attention_kernel,
        out_shape=jax.ShapeDtypeStruct((16, HEAD_DIM, side // 2), jnp.bfloat16),
        in_specs=[pl.BlockSpec(memory_space=pltpu.SMEM)]
        + [pl.BlockSpec(memory_space=pltpu.VMEM)] * 4
        + [pl.BlockSpec(memory_space=pl.ANY)] * 2,
        out_specs=pl.BlockSpec(memory_space=pltpu.VMEM),
        scratch_shapes=[
            pltpu.VMEM((mine.shape[0], side, LANES), jnp.bfloat16),
            pltpu.VMEM((side, side), jnp.float32),
            pltpu.VMEM((4, side, LANES), jnp.bfloat16),
            pltpu.VMEM((side, LANES), jnp.float32),
            pltpu.SemaphoreType.DMA((2,)),
        ],
        compiler_params=pltpu.CompilerParams(vmem_limit_bytes=56 * 2**20),
        cost_estimate=pl.CostEstimate(
            flops=pairs * 2 * 768, bytes_accessed=6 * 2**20, transcendentals=pairs * 3
        ),
        name="attend",
    )(meta, *queries, mine, peer)


MAIN = 16
TAIL = 4


def expand(count, slots, experts, first):
    row = lax.broadcasted_iota(jnp.int32, (count * slots, experts), 0)
    col = lax.broadcasted_iota(jnp.int32, (count * slots, experts), 1)
    return (col == first + row // slots).astype(jnp.bfloat16)


def dispatch_kernel(
    side_ref,
    attended_ref,
    residual_ref,
    weight_ref,
    gain_ref,
    rank_ref,
    mixed_ref,
    normed_ref,
    out_ref,
    heads_ref,
):
    count, _, half = out_ref.shape
    tokens, experts = rank_ref.shape

    @pl.when(pl.program_id(0) == 0)
    def _():
        for head in range(8):
            heads_ref[head * HEAD_DIM : (head + 1) * HEAD_DIM] = attended_ref[2 * head + side_ref[0]]
        projected = lax.dot_general(
            heads_ref[...], weight_ref[...], (((0,), (0,)), ((), ())), preferred_element_type=jnp.float32
        )
        mixed = (residual_ref[...].astype(jnp.float32) + projected).astype(jnp.bfloat16)
        mixed_ref[...] = mixed
        mixed = mixed.astype(jnp.float32)
        inverse = lax.rsqrt(jnp.mean(mixed * mixed, axis=1, keepdims=True) + norm_eps)
        normed_ref[...] = (mixed * inverse * gain_ref[...]).astype(jnp.bfloat16)

    left, right = normed_ref[:, :half], normed_ref[:, half:]
    first = pl.program_id(0) * count

    def chosen(slots, lowest):
        rank = lax.dot_general(
            expand(count, slots, experts, first),
            rank_ref[...],
            (((1,), (1,)), ((), ())),
            preferred_element_type=jnp.float32,
        )
        slot = lowest + lax.broadcasted_iota(jnp.int32, rank.shape, 0) % (slots if lowest == 0 else TAIL)
        return (rank == slot.astype(jnp.float32)).astype(jnp.bfloat16)

    def pick(rows, side):
        return jnp.dot(rows, side, preferred_element_type=jnp.float32)

    main, tail = chosen(MAIN, 0), chosen(2 * TAIL, MAIN)
    out_ref[:, 0:MAIN, :] = pick(main, left).astype(jnp.bfloat16).reshape(count, MAIN, half)
    out_ref[:, MAIN : 2 * MAIN, :] = pick(main, right).astype(jnp.bfloat16).reshape(count, MAIN, half)
    early = lax.broadcasted_iota(jnp.int32, (tail.shape[0], half), 0) % (2 * TAIL) < TAIL
    both = jnp.where(early, pick(tail, left), pick(tail, right))
    out_ref[:, 2 * MAIN :, :] = both.astype(jnp.bfloat16).reshape(count, 2 * TAIL, half)


def dispatch(side, attended, residual, out_weight, gain, ranks, experts):
    tokens, width = residual.shape
    step = 16
    whole = lambda i: (0, 0)
    return pl.pallas_call(
        dispatch_kernel,
        grid=(experts // step,),
        in_specs=[
            pl.BlockSpec(memory_space=pltpu.SMEM),
            pl.BlockSpec(attended.shape, lambda i: (0, 0, 0)),
            pl.BlockSpec(residual.shape, whole),
            pl.BlockSpec(out_weight.shape, whole),
            pl.BlockSpec(gain.shape, whole),
            pl.BlockSpec((tokens, experts), whole),
        ],
        out_specs=[
            pl.BlockSpec((tokens, width), whole),
            pl.BlockSpec((tokens, width), whole),
            pl.BlockSpec((step, 2 * (MAIN + TAIL), width // 2), lambda i: (i, 0, 0)),
        ],
        out_shape=[
            jax.ShapeDtypeStruct((tokens, width), jnp.bfloat16),
            jax.ShapeDtypeStruct((tokens, width), jnp.bfloat16),
            jax.ShapeDtypeStruct((experts, 2 * (MAIN + TAIL), width // 2), jnp.bfloat16),
        ],
        scratch_shapes=[pltpu.VMEM((8 * HEAD_DIM, tokens), jnp.bfloat16)],
        compiler_params=pltpu.CompilerParams(vmem_limit_bytes=60 * 2**20),
        cost_estimate=pl.CostEstimate(flops=10**9, bytes_accessed=10**7, transcendentals=0),
        name="dispatch",
    )(side, attended, residual, out_weight, gain, ranks)


def expert_kernel(
    rows_ref,
    gate0,
    up0,
    gate1,
    up1,
    down0,
    down1,
    shared_gate,
    shared_up,
    shared_down,
    mixed_ref,
    normed_ref,
    out_ref,
    base_ref,
    spread_ref,
    rows2_ref,
    gate0_ref,
    up0_ref,
    gate1_ref,
    up1_ref,
    down0_ref,
    down1_ref,
    shared_gate_ref,
    shared_up_ref,
    shared_down_ref,
    sems,
):
    sources, _, half = rows_ref.shape
    tails = sources * TAIL
    first_step = pl.program_id(0) == 0
    loads = [
        pltpu.make_async_copy(source, target, sems.at[i])
        for i, (source, target) in enumerate(
            (
                (gate0, gate0_ref),
                (up0, up0_ref),
                (gate1, gate1_ref),
                (up1, up1_ref),
                (down0, down0_ref),
                (down1, down1_ref),
                (shared_gate, shared_gate_ref),
                (shared_up, shared_up_ref),
                (shared_down, shared_down_ref),
            )
        )
    ]

    def arrived(*which):
        @pl.when(first_step)
        def _():
            for i in which:
                loads[i].wait()

    @pl.when(first_step)
    def _():
        for load in loads:
            load.start()
        row = lax.broadcasted_iota(jnp.int32, (2 * tails, 2 * tails), 0)
        col = lax.broadcasted_iota(jnp.int32, (2 * tails, 2 * tails), 1)
        slot = row % tails
        home = slot // TAIL * (2 * TAIL) + row // tails * TAIL + slot % TAIL
        spread_ref[...] = (home == col).astype(jnp.bfloat16)

    spread = spread_ref[...]
    mains = sources * MAIN
    rows2_ref[:mains, :half] = rows_ref[:, 0:MAIN, :].reshape(mains, half)
    rows2_ref[:mains, half:] = rows_ref[:, MAIN : 2 * MAIN, :].reshape(mains, half)
    ends = jnp.dot(
        spread, rows_ref[:, 2 * MAIN :, :].reshape(2 * tails, half), preferred_element_type=jnp.float32
    ).astype(jnp.bfloat16)
    rows2_ref[mains:, :half] = ends[:tails]
    rows2_ref[mains:, half:] = ends[tails:]
    rows = rows2_ref[...]

    def hidden(rows, gate_matrix, up_matrix):
        gate = jnp.dot(rows, gate_matrix, preferred_element_type=jnp.float32)
        upward = jnp.dot(rows, up_matrix, preferred_element_type=jnp.float32)
        return (jax.nn.silu(gate) * upward).astype(jnp.bfloat16)

    arrived(0, 1)
    act0 = hidden(rows, gate0_ref[0], up0_ref[0])
    arrived(2, 3)
    act1 = hidden(rows, gate1_ref[0], up1_ref[0])
    arrived(4, 5)
    for part in range(2):
        span = pl.ds(part * half, half)
        result = jnp.dot(act0, down0_ref[0, :, span], preferred_element_type=jnp.float32) + jnp.dot(
            act1, down1_ref[0, :, span], preferred_element_type=jnp.float32
        )
        result = result.astype(jnp.bfloat16)
        out_ref[:, part * MAIN : (part + 1) * MAIN, :] = result[:mains].reshape(sources, MAIN, half)
        if part == 0:
            first = result[mains:]
        else:
            ends = jnp.concatenate([first, result[mains:]], axis=0)
            ends = lax.dot_general(
                spread, ends, (((0,), (0,)), ((), ())), preferred_element_type=jnp.float32
            )
            out_ref[:, 2 * MAIN :, :] = ends.astype(jnp.bfloat16).reshape(sources, 2 * TAIL, half)

    @pl.when(pl.program_id(0) == pl.num_programs(0) - 1)
    def _():
        for load in loads[6:]:
            load.wait()
        act = hidden(normed_ref[...], shared_gate_ref[...], shared_up_ref[...])
        base_ref[...] = mixed_ref[...].astype(jnp.float32) + jnp.dot(
            act, shared_down_ref[...], preferred_element_type=jnp.float32
        )


def expert(rows, weights, mixed, normed):
    step = 16
    block = pl.BlockSpec((step,) + rows.shape[1:], lambda i: (i, 0, 0))
    whole = pl.BlockSpec(mixed.shape, lambda i: (0, 0))
    return pl.pallas_call(
        expert_kernel,
        grid=(rows.shape[0] // step,),
        in_specs=[block] + [pl.BlockSpec(memory_space=pl.ANY)] * len(weights) + [whole] * 2,
        out_specs=[block, whole],
        out_shape=[
            jax.ShapeDtypeStruct(rows.shape, jnp.bfloat16),
            jax.ShapeDtypeStruct(mixed.shape, jnp.float32),
        ],
        scratch_shapes=[
            pltpu.VMEM((step * 2 * TAIL, step * 2 * TAIL), jnp.bfloat16),
            pltpu.VMEM((step * (MAIN + TAIL), 2 * rows.shape[2]), jnp.bfloat16),
        ]
        + [pltpu.VMEM(w.shape, w.dtype) for w in weights]
        + [pltpu.SemaphoreType.DMA((len(weights),))],
        compiler_params=pltpu.CompilerParams(vmem_limit_bytes=60 * 2**20),
        cost_estimate=pl.CostEstimate(flops=8 * 10**9, bytes_accessed=17 * 10**6, transcendentals=10**6),
        name="expert",
    )(rows, *weights, mixed, normed)


def combine_kernel(rows_ref, ranks_ref, base_ref, out_ref, acc_ref):
    count, _, half = rows_ref.shape
    tokens = base_ref.shape[0]
    experts = ranks_ref.shape[1]
    at = pl.program_id(0)

    @pl.when(at == 0)
    def _():
        acc_ref[...] = base_ref[...]

    def weights(slots, wanted):
        spread = lax.dot_general(
            ranks_ref[...],
            expand(count, slots, experts, at * count),
            (((1,), (1,)), ((), ())),
            preferred_element_type=jnp.float32,
        )
        rank = spread[:tokens]
        slot = wanted(lax.broadcasted_iota(jnp.int32, rank.shape, 1) % slots).astype(jnp.float32)
        here = rank == slot
        parts = [jnp.where(here, spread[i * tokens : (i + 1) * tokens], 0.0) for i in (1, 2)]
        return jnp.concatenate(parts, axis=0).astype(jnp.bfloat16)

    main = weights(MAIN, lambda slot: slot)
    ends = rows_ref[:, 2 * MAIN :, :].reshape(count * 2 * TAIL, half)
    for part in range(2):
        tail = weights(
            2 * TAIL, lambda slot: jnp.where(slot // TAIL == part, MAIN + slot % TAIL, -2)
        )
        rows = rows_ref[:, part * MAIN : (part + 1) * MAIN, :].reshape(count * MAIN, half)
        total = jnp.dot(main, rows, preferred_element_type=jnp.float32) + jnp.dot(
            tail, ends, preferred_element_type=jnp.float32
        )
        span = pl.ds(part * half, half)
        acc_ref[:, span] += total[:tokens] + total[tokens:]

    @pl.when(at == pl.num_programs(0) - 1)
    def _():
        out_ref[...] = acc_ref[...].astype(jnp.bfloat16)


def combine(rows, ranks, base):
    step = 16
    whole = lambda i: (0, 0)
    return pl.pallas_call(
        combine_kernel,
        grid=(rows.shape[0] // step,),
        in_specs=[
            pl.BlockSpec((step,) + rows.shape[1:], lambda i: (i, 0, 0)),
            pl.BlockSpec(ranks.shape, whole),
            pl.BlockSpec(base.shape, whole),
        ],
        out_specs=pl.BlockSpec(base.shape, whole),
        out_shape=jax.ShapeDtypeStruct(base.shape, jnp.bfloat16),
        scratch_shapes=[pltpu.VMEM(base.shape, jnp.float32)],
        compiler_params=pltpu.CompilerParams(vmem_limit_bytes=60 * 2**20),
        cost_estimate=pl.CostEstimate(flops=10**9, bytes_accessed=10**7, transcendentals=0),
        name="combine",
    )(rows, ranks, base)


def local(
    queries,
    key_rows,
    value_rows,
    residual,
    out_weight,
    norm_gain,
    routes,
    route_weight,
    expert_gate,
    expert_up,
    expert_down,
    shared_gate,
    shared_up,
    shared_down,
):
    chips = [[i, 31 - i, 32 + i, 63 - i, 8 + i, 23 - i, 40 + i, 55 - i] for i in range(8)]
    devices = [[2 * s + c for s in g for c in range(2)] for g in chips]
    core = lax.axis_index("tp")
    position = lax.axis_index("sp")
    plane, spot = position // 16, position % 16
    place = jnp.where(plane % 2 == 1, 15 - spot, spot)
    group, member = place % 8, plane + place // 8 * 4

    place_meta = jnp.stack([core, member % 4]).astype(jnp.int32)
    turn_heads = split_queries(place_meta, queries)
    keep, send = pack(place_meta, key_rows, value_rows)
    swap = [(0, 1), (1, 0)]
    taken = lax.ppermute(send, "tp", swap)
    low, high = jnp.where(core == 0, keep, taken), jnp.where(core == 0, taken, keep)
    order = jnp.stack([low[0], high[0], high[1], low[1], low[2], high[2], high[3], low[3]])
    order = jnp.broadcast_to(order[:, None], (8,) + order.shape).reshape((64,) + order.shape[1:])
    turns = []
    for turn in range(4):
        pairs = [
            (devices[g][2 * m + c], devices[g][2 * (4 * c + ((m % 4) ^ turn)) + m // 4])
            for g in range(8)
            for m in range(8)
            for c in range(2)
        ]
        turns.append(lax.ppermute(turn_heads[turn], ("sp", "tp"), pairs))
    ranks = route(routes, route_weight, 64)
    order, ranks, *turns = lax.optimization_barrier((order, ranks, *turns))
    mine = lax.all_to_all(order, "sp", 0, 0, tiled=True)
    peer = lax.ppermute(mine, "tp", swap)
    sender = [4 * core + ((member % 4) ^ turn) for turn in range(4)]
    block = [
        16 * (m % 4) + jnp.where(m % 2 == 1, 15 - group - m // 4 * 8, group + m // 4 * 8) for m in sender
    ]
    meta = jnp.stack([core] + block + [2 * m for m in sender]).astype(jnp.int32)
    attended = attention(meta, turns, mine, peer)
    peer, expert_gate_, expert_up_, expert_down_ = lax.optimization_barrier(
        (peer, expert_gate, expert_up, expert_down)
    )
    gate_other = lax.ppermute(expert_gate_, "tp", swap)
    up_other = lax.ppermute(expert_up_, "tp", swap)
    down_other = lax.ppermute(expert_down_, "tp", swap)
    attended, gate_other, up_other, down_other = lax.optimization_barrier(
        (attended, gate_other, up_other, down_other)
    )
    attended = lax.all_to_all(attended, ("sp", "tp"), 0, 0, axis_index_groups=devices, tiled=True)
    side = (member // 4)[None].astype(jnp.int32)

    experts = lax.axis_size("sp")
    mixed, normed, outgoing = dispatch(
        side, attended, residual, out_weight, norm_gain[None, :], ranks, experts
    )
    incoming = lax.all_to_all(outgoing, "sp", 0, 0, tiled=True)
    result, base = expert(
        incoming,
        (
            expert_gate,
            expert_up,
            gate_other,
            up_other,
            expert_down,
            down_other,
            shared_gate,
            shared_up,
            shared_down,
        ),
        mixed,
        normed,
    )
    returned = lax.all_to_all(result, "sp", 0, 0, tiled=True)
    return combine(returned, ranks, base)


def solution(mesh):
    return jax.shard_map(
        local,
        mesh=mesh,
        in_specs=(
            P("sp", "tp"),
            P("sp", "tp"),
            P("sp", "tp"),
            P(("sp", "tp"), None),
            P(),
            P(),
            P(("sp", "tp"), None),
            P(("sp", "tp"), None),
            P("sp", None, "tp"),
            P("sp", None, "tp"),
            P("sp", "tp", None),
            P(),
            P(),
            P(),
        ),
        out_specs=P(("sp", "tp"), None),
        check_vma=False,
    )
```

```python
import jax
import jax.numpy as jnp
from jax import lax
from jax.experimental import pallas as pl
from jax.experimental.pallas import tpu as pltpu
from jax.sharding import PartitionSpec as P

HEAD_DIM = 64
LANES = 128
TOPK = 8
LOG2E = 1.4426950408889634
norm_eps = 1e-06


VMEM_BYTES = 67043328


def pack_kernel(core_ref, query_ref, key_ref, value_ref, keep_out, send_out):
    heads, rows = keep_out.shape[0], query_ref.shape[0] // 2
    core = core_ref[0]
    for out, half in ((keep_out, core), (send_out, 1 - core)):
        own = pl.ds(half * rows, rows)
        for head in range(heads):
            span = slice(head * HEAD_DIM, (head + 1) * HEAD_DIM)
            out[head, :rows] = jnp.concatenate([key_ref[own, span], value_ref[own, span]], axis=1)
            query = query_ref[own, span].reshape(rows // 16, 16, HEAD_DIM)
            query = jnp.concatenate([query[:, :8], query[:, 8:]], axis=2)
            out[head, rows:] = query.reshape(rows // 2, LANES)


def pack(core, queries, key_rows, value_rows):
    side, width = key_rows.shape
    half = jax.ShapeDtypeStruct((width // HEAD_DIM, side // 2 + side // 4, LANES), jnp.bfloat16)
    return pl.pallas_call(
        pack_kernel,
        in_specs=[pl.BlockSpec(memory_space=pltpu.SMEM)] + [pl.BlockSpec(memory_space=pltpu.VMEM)] * 3,
        out_specs=[pl.BlockSpec(memory_space=pltpu.VMEM)] * 2,
        out_shape=[half, half],
        name="pack",
    )(core, queries, key_rows, value_rows)


def spread_kernel(core_ref, keep_ref, taken_ref, out_ref):
    head = pl.program_id(0)
    mine = head // 4 == core_ref[0]
    count, depth, _ = out_ref.shape
    rows = depth - 8
    held = jnp.where(mine, keep_ref[head % 4], taken_ref[head % 4])
    for chip in range(count):
        out_ref[chip, :rows] = held[:rows]
        out_ref[chip, rows:] = held[rows + 8 * chip : rows + 8 * chip + 8]


def spread(core, keep, taken):
    heads = 8
    rows = keep.shape[1] * 2 // 3
    whole = pl.BlockSpec(keep.shape, lambda i: (0, 0, 0))
    return pl.pallas_call(
        spread_kernel,
        grid=(heads,),
        in_specs=[pl.BlockSpec(memory_space=pltpu.SMEM), whole, whole],
        out_specs=pl.BlockSpec((8, rows + 8, LANES), lambda i: (i, 0, 0)),
        out_shape=jax.ShapeDtypeStruct((8 * heads, rows + 8, LANES), jnp.bfloat16),
        compiler_params=pltpu.CompilerParams(vmem_limit_bytes=VMEM_BYTES),
        name="spread",
    )(core, keep, taken)


def route_kernel(routes_ref, weight_ref, out_ref):
    tokens, experts = routes_ref.shape[1], out_ref.shape[0] // 3
    names = lax.broadcasted_iota(jnp.int32, (experts, tokens), 0)
    pick = jnp.zeros((experts, tokens), jnp.float32)
    share = jnp.zeros((experts, tokens), jnp.float32)
    for k in range(TOPK):
        named = routes_ref[k : k + 1, :] == names
        pick = jnp.where(named, 1.0, pick)
        share = jnp.where(named, weight_ref[k : k + 1, :], share)
    row = lax.broadcasted_iota(jnp.int32, (tokens, tokens), 0)
    col = lax.broadcasted_iota(jnp.int32, (tokens, tokens), 1)
    above = (row < col).astype(jnp.bfloat16)
    rank = jnp.dot(pick.astype(jnp.bfloat16), above, preferred_element_type=jnp.float32)
    out_ref[0:experts] = jnp.where(pick > 0.0, rank, -1.0).astype(jnp.bfloat16)
    high = share.astype(jnp.bfloat16)
    out_ref[experts : 2 * experts] = high
    out_ref[2 * experts :] = (share - high.astype(jnp.float32)).astype(jnp.bfloat16)


def route(routes, route_weight, experts):
    return pl.pallas_call(
        route_kernel,
        out_shape=jax.ShapeDtypeStruct((3 * experts, routes.shape[1]), jnp.bfloat16),
        in_specs=[pl.BlockSpec(memory_space=pltpu.VMEM)] * 2,
        out_specs=pl.BlockSpec(memory_space=pltpu.VMEM),
        name="route",
    )(routes, route_weight)


GROUP = 4


def attention_kernel(meta_ref, mine_ref, peer_ref, out_ref, kv_ref, tri_ref, raw_ref, query_ref, acc_ref, sems):
    core, offset = meta_ref[0], meta_ref[1]
    side = tri_ref.shape[0]
    rows = side // 2
    loads = [
        pltpu.make_async_copy(mine_ref.at[:, pl.ds(rows, 8)], raw_ref, sems.at[0]),
        pltpu.make_async_copy(mine_ref.at[:, pl.ds(0, rows)], kv_ref.at[:, pl.ds(core * rows, rows)], sems.at[1]),
        pltpu.make_async_copy(
            peer_ref.at[:, pl.ds(0, rows)], kv_ref.at[:, pl.ds((1 - core) * rows, rows)], sems.at[2]
        ),
    ]
    for load in loads:
        load.start()
    row = lax.broadcasted_iota(jnp.int32, (side, side), 0)
    col = lax.broadcasted_iota(jnp.int32, (side, side), 1)
    tri_ref[...] = (row > col).astype(jnp.float32)
    loads[0].wait()
    raw = raw_ref[...]
    none = jnp.zeros(raw.shape[:2] + (HEAD_DIM,), jnp.bfloat16)
    early = jnp.concatenate([raw[:, :, :HEAD_DIM], none], axis=2)
    late = jnp.concatenate([raw[:, :, HEAD_DIM:], none], axis=2)
    query_ref[...] = jnp.concatenate([early, late], axis=1).reshape(query_ref.shape)
    loads[1].wait()
    loads[2].wait()

    def advance(tile, first, skip, diagonal):
        query = query_ref[tile, skip:]
        keys = [kv_ref[first + i] for i in range(GROUP)]
        scores = [
            lax.dot_general(query, kv, (((1,), (1,)), ((), ())), preferred_element_type=jnp.float32)
            * (HEAD_DIM**-0.5 * LOG2E)
            for kv in keys
        ]
        costs = [jnp.maximum(s, 0.0) + jnp.log2(1.0 + jnp.exp2(-jnp.abs(s))) for s in scores]
        slacks = [s - c for s, c in zip(scores, costs)]
        if diagonal is not None:
            shape = scores[0].shape
            place = skip + lax.broadcasted_iota(jnp.int32, shape, 0)
            place = place // 16 * side + place % 16 + offset - lax.broadcasted_iota(jnp.int32, shape, 1)
            live = [place > (diagonal + i) * side for i in range(GROUP)]
            costs = [jnp.where(l, c, 0.0) for l, c in zip(live, costs)]
        tri = tri_ref[...]
        insides = [jnp.dot(c, tri, preferred_element_type=jnp.float32) for c in costs]
        acc = acc_ref[skip:]
        for i in range(GROUP):
            weight = jnp.exp2(slacks[i] - insides[i])
            if diagonal is not None:
                weight = jnp.where(live[i], weight, 0.0)
            part = jnp.dot(weight.astype(jnp.bfloat16), keys[i], preferred_element_type=jnp.float32)
            acc = acc * jnp.exp2(-(insides[i][:, 0:1] + costs[i][:, 0:1])) + part
        acc_ref[skip:] = acc

    @pl.loop(0, 4)
    def _(tile):
        acc_ref[...] = jnp.zeros_like(acc_ref)

        @pl.loop(0, 4 * tile)
        def _(step):
            advance(tile, step * GROUP, 0, None)

        for step in range(4):
            advance(tile, 16 * tile + step * GROUP, step * GROUP * 16, step * GROUP)
        done = acc_ref[:, HEAD_DIM:].reshape(16, 16, HEAD_DIM)
        done = jnp.concatenate([done[:, :8], done[:, 8:]], axis=2).astype(jnp.bfloat16)
        out_ref[pl.ds(tile * 16, 16)] = done


def attention(meta, mine, peer):
    chips, depth, _ = mine.shape
    side = 2 * (depth - 8)
    pairs = 136 * side * side
    return pl.pallas_call(
        attention_kernel,
        out_shape=jax.ShapeDtypeStruct((chips, 8, LANES), jnp.bfloat16),
        in_specs=[pl.BlockSpec(memory_space=pltpu.SMEM)] + [pl.BlockSpec(memory_space=pl.ANY)] * 2,
        out_specs=pl.BlockSpec(memory_space=pltpu.VMEM),
        scratch_shapes=[
            pltpu.VMEM((chips, side, LANES), jnp.bfloat16),
            pltpu.VMEM((side, side), jnp.float32),
            pltpu.VMEM((chips, 8, LANES), jnp.bfloat16),
            pltpu.VMEM((4, side, LANES), jnp.bfloat16),
            pltpu.VMEM((side, LANES), jnp.float32),
            pltpu.SemaphoreType.DMA((3,)),
        ],
        compiler_params=pltpu.CompilerParams(vmem_limit_bytes=VMEM_BYTES),
        cost_estimate=pl.CostEstimate(
            flops=pairs * 2 * 768, bytes_accessed=6 * 2**20, transcendentals=pairs * 3
        ),
        name="attend",
    )(meta, mine, peer)


MAIN = 16
TAIL = 4


def expand(count, slots, experts, first):
    row = lax.broadcasted_iota(jnp.int32, (count * slots, experts), 0)
    col = lax.broadcasted_iota(jnp.int32, (count * slots, experts), 1)
    return (col == first + row // slots).astype(jnp.bfloat16)


def dispatch_kernel(
    attended_ref,
    residual_ref,
    weight_ref,
    gain_ref,
    rank_ref,
    mixed_ref,
    normed_ref,
    out_ref,
    heads_ref,
):
    count, _, half = out_ref.shape
    experts, tokens = rank_ref.shape

    @pl.when(pl.program_id(0) == 0)
    def _():
        for head in range(8):
            rows = attended_ref[8 * head : 8 * head + 8]
            rows = jnp.concatenate([rows[:, :, :HEAD_DIM], rows[:, :, HEAD_DIM:]], axis=1)
            heads_ref[:, head * HEAD_DIM : (head + 1) * HEAD_DIM] = rows.reshape(tokens, HEAD_DIM)
        projected = jnp.dot(heads_ref[...], weight_ref[...], preferred_element_type=jnp.float32)
        mixed = (residual_ref[...].astype(jnp.float32) + projected).astype(jnp.bfloat16)
        mixed_ref[...] = mixed
        mixed = mixed.astype(jnp.float32)
        inverse = lax.rsqrt(jnp.mean(mixed * mixed, axis=1, keepdims=True) + norm_eps)
        normed_ref[...] = (mixed * inverse * gain_ref[...]).astype(jnp.bfloat16)

    left, right = normed_ref[:, :half], normed_ref[:, half:]
    first = pl.program_id(0) * count

    def chosen(slots, lowest):
        rank = jnp.dot(
            expand(count, slots, experts, first), rank_ref[...], preferred_element_type=jnp.float32
        )
        slot = lowest + lax.broadcasted_iota(jnp.int32, rank.shape, 0) % (slots if lowest == 0 else TAIL)
        return (rank == slot.astype(jnp.float32)).astype(jnp.bfloat16)

    def pick(rows, side):
        return jnp.dot(rows, side, preferred_element_type=jnp.float32)

    main, tail = chosen(MAIN, 0), chosen(2 * TAIL, MAIN)
    out_ref[:, 0:MAIN, :] = pick(main, left).astype(jnp.bfloat16).reshape(count, MAIN, half)
    out_ref[:, MAIN : 2 * MAIN, :] = pick(main, right).astype(jnp.bfloat16).reshape(count, MAIN, half)
    early = lax.broadcasted_iota(jnp.int32, (tail.shape[0], half), 0) % (2 * TAIL) < TAIL
    both = jnp.where(early, pick(tail, left), pick(tail, right))
    out_ref[:, 2 * MAIN :, :] = both.astype(jnp.bfloat16).reshape(count, 2 * TAIL, half)


def dispatch(attended, residual, out_weight, gain, ranks, experts):
    tokens, width = residual.shape
    step = 16
    whole = lambda i: (0, 0)
    return pl.pallas_call(
        dispatch_kernel,
        grid=(experts // step,),
        in_specs=[
            pl.BlockSpec(attended.shape, lambda i: (0, 0, 0)),
            pl.BlockSpec(residual.shape, whole),
            pl.BlockSpec(out_weight.shape, whole),
            pl.BlockSpec(gain.shape, whole),
            pl.BlockSpec((experts, tokens), whole),
        ],
        out_specs=[
            pl.BlockSpec((tokens, width), whole),
            pl.BlockSpec((tokens, width), whole),
            pl.BlockSpec((step, 2 * (MAIN + TAIL), width // 2), lambda i: (i, 0, 0)),
        ],
        out_shape=[
            jax.ShapeDtypeStruct((tokens, width), jnp.bfloat16),
            jax.ShapeDtypeStruct((tokens, width), jnp.bfloat16),
            jax.ShapeDtypeStruct((experts, 2 * (MAIN + TAIL), width // 2), jnp.bfloat16),
        ],
        scratch_shapes=[pltpu.VMEM((tokens, 8 * HEAD_DIM), jnp.bfloat16)],
        compiler_params=pltpu.CompilerParams(vmem_limit_bytes=VMEM_BYTES),
        cost_estimate=pl.CostEstimate(flops=10**9, bytes_accessed=10**7, transcendentals=0),
        name="dispatch",
    )(attended, residual, out_weight, gain, ranks)


def expert_kernel(
    rows_ref,
    gate0,
    up0,
    gate1,
    up1,
    down0,
    down1,
    shared_gate,
    shared_up,
    shared_down,
    mixed_ref,
    normed_ref,
    out_ref,
    base_ref,
    spread_ref,
    rows2_ref,
    gate0_ref,
    up0_ref,
    gate1_ref,
    up1_ref,
    down0_ref,
    down1_ref,
    shared_gate_ref,
    shared_up_ref,
    shared_down_ref,
    sems,
):
    sources, _, half = rows_ref.shape
    tails = sources * TAIL
    first_step = pl.program_id(0) == 0
    loads = [
        pltpu.make_async_copy(source, target, sems.at[i])
        for i, (source, target) in enumerate(
            (
                (gate0, gate0_ref),
                (up0, up0_ref),
                (gate1, gate1_ref),
                (up1, up1_ref),
                (down0, down0_ref),
                (down1, down1_ref),
                (shared_gate, shared_gate_ref),
                (shared_up, shared_up_ref),
                (shared_down, shared_down_ref),
            )
        )
    ]

    def arrived(*which):
        @pl.when(first_step)
        def _():
            for i in which:
                loads[i].wait()

    @pl.when(first_step)
    def _():
        for load in loads:
            load.start()
        row = lax.broadcasted_iota(jnp.int32, (2 * tails, 2 * tails), 0)
        col = lax.broadcasted_iota(jnp.int32, (2 * tails, 2 * tails), 1)
        slot = row % tails
        home = slot // TAIL * (2 * TAIL) + row // tails * TAIL + slot % TAIL
        spread_ref[...] = (home == col).astype(jnp.bfloat16)

    spread = spread_ref[...]
    mains = sources * MAIN
    rows2_ref[:mains, :half] = rows_ref[:, 0:MAIN, :].reshape(mains, half)
    rows2_ref[:mains, half:] = rows_ref[:, MAIN : 2 * MAIN, :].reshape(mains, half)
    ends = jnp.dot(
        spread, rows_ref[:, 2 * MAIN :, :].reshape(2 * tails, half), preferred_element_type=jnp.float32
    ).astype(jnp.bfloat16)
    rows2_ref[mains:, :half] = ends[:tails]
    rows2_ref[mains:, half:] = ends[tails:]
    rows = rows2_ref[...]

    def hidden(rows, gate_matrix, up_matrix):
        gate = jnp.dot(rows, gate_matrix, preferred_element_type=jnp.float32)
        upward = jnp.dot(rows, up_matrix, preferred_element_type=jnp.float32)
        return (jax.nn.silu(gate) * upward).astype(jnp.bfloat16)

    arrived(0, 1)
    act0 = hidden(rows, gate0_ref[0], up0_ref[0])
    arrived(2, 3)
    act1 = hidden(rows, gate1_ref[0], up1_ref[0])
    arrived(4, 5)
    for part in range(2):
        span = pl.ds(part * half, half)
        result = jnp.dot(act0, down0_ref[0, :, span], preferred_element_type=jnp.float32) + jnp.dot(
            act1, down1_ref[0, :, span], preferred_element_type=jnp.float32
        )
        result = result.astype(jnp.bfloat16)
        out_ref[:, part * MAIN : (part + 1) * MAIN, :] = result[:mains].reshape(sources, MAIN, half)
        if part == 0:
            first = result[mains:]
        else:
            ends = jnp.concatenate([first, result[mains:]], axis=0)
            ends = lax.dot_general(
                spread, ends, (((0,), (0,)), ((), ())), preferred_element_type=jnp.float32
            )
            out_ref[:, 2 * MAIN :, :] = ends.astype(jnp.bfloat16).reshape(sources, 2 * TAIL, half)

    @pl.when(pl.program_id(0) == pl.num_programs(0) - 1)
    def _():
        for load in loads[6:]:
            load.wait()
        act = hidden(normed_ref[...], shared_gate_ref[...], shared_up_ref[...])
        base_ref[...] = mixed_ref[...].astype(jnp.float32) + jnp.dot(
            act, shared_down_ref[...], preferred_element_type=jnp.float32
        )


def expert(rows, weights, mixed, normed):
    step = 16
    block = pl.BlockSpec((step,) + rows.shape[1:], lambda i: (i, 0, 0))
    whole = pl.BlockSpec(mixed.shape, lambda i: (0, 0))
    return pl.pallas_call(
        expert_kernel,
        grid=(rows.shape[0] // step,),
        in_specs=[block] + [pl.BlockSpec(memory_space=pl.ANY)] * len(weights) + [whole] * 2,
        out_specs=[block, whole],
        out_shape=[
            jax.ShapeDtypeStruct(rows.shape, jnp.bfloat16),
            jax.ShapeDtypeStruct(mixed.shape, jnp.float32),
        ],
        scratch_shapes=[
            pltpu.VMEM((step * 2 * TAIL, step * 2 * TAIL), jnp.bfloat16),
            pltpu.VMEM((step * (MAIN + TAIL), 2 * rows.shape[2]), jnp.bfloat16),
        ]
        + [pltpu.VMEM(w.shape, w.dtype) for w in weights]
        + [pltpu.SemaphoreType.DMA((len(weights),))],
        compiler_params=pltpu.CompilerParams(vmem_limit_bytes=VMEM_BYTES),
        cost_estimate=pl.CostEstimate(flops=8 * 10**9, bytes_accessed=17 * 10**6, transcendentals=10**6),
        name="expert",
    )(rows, *weights, mixed, normed)


def combine_kernel(rows_ref, ranks_ref, base_ref, out_ref, acc_ref):
    count, _, half = rows_ref.shape
    tokens = base_ref.shape[0]
    experts = ranks_ref.shape[0] // 3
    at = pl.program_id(0)

    @pl.when(at == 0)
    def _():
        acc_ref[...] = base_ref[...]

    def weights(slots, wanted):
        chosen = expand(count, slots, experts, at * count)
        rank, high, low = [
            jnp.dot(chosen, ranks_ref[i * experts : (i + 1) * experts], preferred_element_type=jnp.float32)
            for i in range(3)
        ]
        slot = wanted(lax.broadcasted_iota(jnp.int32, rank.shape, 0) % slots).astype(jnp.float32)
        here = rank == slot
        parts = [jnp.where(here, part, 0.0) for part in (high, low)]
        return jnp.concatenate(parts, axis=1).T.astype(jnp.bfloat16)

    main = weights(MAIN, lambda slot: slot)
    ends = rows_ref[:, 2 * MAIN :, :].reshape(count * 2 * TAIL, half)
    for part in range(2):
        tail = weights(
            2 * TAIL, lambda slot: jnp.where(slot // TAIL == part, MAIN + slot % TAIL, -2)
        )
        rows = rows_ref[:, part * MAIN : (part + 1) * MAIN, :].reshape(count * MAIN, half)
        total = jnp.dot(main, rows, preferred_element_type=jnp.float32) + jnp.dot(
            tail, ends, preferred_element_type=jnp.float32
        )
        span = pl.ds(part * half, half)
        acc_ref[:, span] += total[:tokens] + total[tokens:]

    @pl.when(at == pl.num_programs(0) - 1)
    def _():
        out_ref[...] = acc_ref[...].astype(jnp.bfloat16)


def combine(rows, ranks, base):
    step = 16
    whole = lambda i: (0, 0)
    return pl.pallas_call(
        combine_kernel,
        grid=(rows.shape[0] // step,),
        in_specs=[
            pl.BlockSpec((step,) + rows.shape[1:], lambda i: (i, 0, 0)),
            pl.BlockSpec(ranks.shape, whole),
            pl.BlockSpec(base.shape, whole),
        ],
        out_specs=pl.BlockSpec(base.shape, whole),
        out_shape=jax.ShapeDtypeStruct(base.shape, jnp.bfloat16),
        scratch_shapes=[pltpu.VMEM(base.shape, jnp.float32)],
        compiler_params=pltpu.CompilerParams(vmem_limit_bytes=VMEM_BYTES),
        cost_estimate=pl.CostEstimate(flops=10**9, bytes_accessed=10**7, transcendentals=0),
        name="combine",
    )(rows, ranks, base)


def local(
    queries,
    key_rows,
    value_rows,
    residual,
    out_weight,
    norm_gain,
    routes,
    route_weight,
    expert_gate,
    expert_up,
    expert_down,
    shared_gate,
    shared_up,
    shared_down,
):
    core = lax.axis_index("tp")
    offset = 128 * core + 16 * (lax.axis_index("sp") % 8)
    swap = [(0, 1), (1, 0)]
    cores = core[None].astype(jnp.int32)
    keep, send = pack(cores, queries, key_rows, value_rows)
    taken = lax.ppermute(send, "tp", swap)
    mine = lax.all_to_all(spread(cores, keep, taken), "sp", 0, 0, tiled=True)
    peer = lax.ppermute(mine, "tp", swap)
    mine, routes, route_weight = lax.optimization_barrier((mine, routes, route_weight))
    ranks = route(routes.T, route_weight.T, 64)
    peer, ranks, expert_gate_, expert_up_, expert_down_ = lax.optimization_barrier(
        (peer, ranks, expert_gate, expert_up, expert_down)
    )
    attended = attention(jnp.stack([core, offset]).astype(jnp.int32), mine, peer)
    gate_other = lax.ppermute(expert_gate_, "tp", swap)
    up_other = lax.ppermute(expert_up_, "tp", swap)
    down_other = lax.ppermute(expert_down_, "tp", swap)
    attended, gate_other, up_other, down_other = lax.optimization_barrier(
        (attended, gate_other, up_other, down_other)
    )
    attended = lax.all_to_all(attended, "sp", 0, 0, tiled=True)
    experts = lax.axis_size("sp")
    mixed, normed, outgoing = dispatch(
        attended, residual, out_weight, norm_gain[None, :], ranks, experts
    )
    incoming = lax.all_to_all(outgoing, "sp", 0, 0, tiled=True)
    result, base = expert(
        incoming,
        (
            expert_gate,
            expert_up,
            gate_other,
            up_other,
            expert_down,
            down_other,
            shared_gate,
            shared_up,
            shared_down,
        ),
        mixed,
        normed,
    )
    returned = lax.all_to_all(result, "sp", 0, 0, tiled=True)
    return combine(returned, ranks, base)


def solution(mesh):
    return jax.shard_map(
        local,
        mesh=mesh,
        in_specs=(
            P("sp", "tp"),
            P("sp", "tp"),
            P("sp", "tp"),
            P(("sp", "tp"), None),
            P(),
            P(),
            P(("sp", "tp"), None),
            P(("sp", "tp"), None),
            P("sp", None, "tp"),
            P("sp", None, "tp"),
            P("sp", "tp", None),
            P(),
            P(),
            P(),
        ),
        out_specs=P(("sp", "tp"), None),
        check_vma=False,
    )
```

```python
import jax
import jax.numpy as jnp
from jax import lax
from jax.experimental import pallas as pl
from jax.experimental.pallas import tpu as pltpu
from jax.sharding import PartitionSpec as P

HEAD_DIM = 64
LANES = 128
TOPK = 8
LOG2E = 1.4426950408889634
norm_eps = 1e-06


VMEM_BYTES = 67043328


def pack_kernel(core_ref, query_ref, key_ref, value_ref, keep_out, send_out):
    heads, rows = keep_out.shape[0], query_ref.shape[0] // 2
    core = core_ref[0]
    for out, half in ((keep_out, core), (send_out, 1 - core)):
        own = pl.ds(half * rows, rows)
        for head in range(heads):
            span = slice(head * HEAD_DIM, (head + 1) * HEAD_DIM)
            out[head, :rows] = jnp.concatenate([key_ref[own, span], value_ref[own, span]], axis=1)
            query = query_ref[own, span].reshape(rows // 16, 16, HEAD_DIM)
            query = jnp.concatenate([query[:, :8], query[:, 8:]], axis=2)
            out[head, rows:] = query.reshape(rows // 2, LANES)


def pack(core, queries, key_rows, value_rows):
    side, width = key_rows.shape
    half = jax.ShapeDtypeStruct((width // HEAD_DIM, side // 2 + side // 4, LANES), jnp.bfloat16)
    return pl.pallas_call(
        pack_kernel,
        in_specs=[pl.BlockSpec(memory_space=pltpu.SMEM)] + [pl.BlockSpec(memory_space=pltpu.VMEM)] * 3,
        out_specs=[pl.BlockSpec(memory_space=pltpu.VMEM)] * 2,
        out_shape=[half, half],
        name="pack",
    )(core, queries, key_rows, value_rows)


def spread_kernel(core_ref, keep_ref, taken_ref, out_ref, held_ref, sems):
    chips, depth, _ = held_ref.shape
    heads = chips // 8
    rows = depth - 8
    copies = []
    for head in range(heads):
        mine = head // 4 == core_ref[0]
        held = jnp.where(mine, keep_ref[head % 4], taken_ref[head % 4])
        for chip in range(8):
            held_ref[8 * head + chip, :rows] = held[:rows]
            held_ref[8 * head + chip, rows:] = held[rows + 8 * chip : rows + 8 * chip + 8]
        span = pl.ds(8 * head, 8)
        copies.append(pltpu.make_async_copy(held_ref.at[span], out_ref.at[span], sems.at[head]))
        copies[-1].start()
    for copy in copies:
        copy.wait()


def spread(core, keep, taken):
    shape = (64, keep.shape[1] * 2 // 3 + 8, LANES)
    return pl.pallas_call(
        spread_kernel,
        in_specs=[pl.BlockSpec(memory_space=pltpu.SMEM)] + [pl.BlockSpec(memory_space=pltpu.VMEM)] * 2,
        out_specs=pl.BlockSpec(memory_space=pl.ANY),
        out_shape=jax.ShapeDtypeStruct(shape, jnp.bfloat16),
        scratch_shapes=[pltpu.VMEM(shape, jnp.bfloat16), pltpu.SemaphoreType.DMA((8,))],
        compiler_params=pltpu.CompilerParams(vmem_limit_bytes=VMEM_BYTES - 2**20),
        name="spread",
    )(core, keep, taken)


def route_kernel(routes_ref, weight_ref, out_ref):
    tokens, experts = routes_ref.shape[1], out_ref.shape[0] // 3
    names = lax.broadcasted_iota(jnp.int32, (experts, tokens), 0)
    pick = jnp.zeros((experts, tokens), jnp.float32)
    share = jnp.zeros((experts, tokens), jnp.float32)
    for k in range(TOPK):
        named = routes_ref[k : k + 1, :] == names
        pick = jnp.where(named, 1.0, pick)
        share = jnp.where(named, weight_ref[k : k + 1, :], share)
    row = lax.broadcasted_iota(jnp.int32, (tokens, tokens), 0)
    col = lax.broadcasted_iota(jnp.int32, (tokens, tokens), 1)
    above = (row < col).astype(jnp.bfloat16)
    rank = jnp.dot(pick.astype(jnp.bfloat16), above, preferred_element_type=jnp.float32)
    out_ref[0:experts] = jnp.where(pick > 0.0, rank, -1.0).astype(jnp.bfloat16)
    high = share.astype(jnp.bfloat16)
    out_ref[experts : 2 * experts] = high
    out_ref[2 * experts :] = (share - high.astype(jnp.float32)).astype(jnp.bfloat16)


def route(routes, route_weight, experts):
    return pl.pallas_call(
        route_kernel,
        out_shape=jax.ShapeDtypeStruct((3 * experts, routes.shape[1]), jnp.bfloat16),
        in_specs=[pl.BlockSpec(memory_space=pltpu.VMEM)] * 2,
        out_specs=pl.BlockSpec(memory_space=pltpu.VMEM),
        name="route",
    )(routes, route_weight)


GROUP = 4


PIECES = 16


def attention_kernel(meta_ref, mine, peer, out_ref, kv_ref, raw_ref, tri_ref, query_ref, acc_ref, sems):
    core, offset = meta_ref[0], meta_ref[1]
    side = tri_ref.shape[0]
    rows = side // 2
    span = kv_ref.shape[0] // PIECES
    first_rows = pl.ds(pl.multiple_of(core * rows, rows), rows)
    other_rows = pl.ds(pl.multiple_of((1 - core) * rows, rows), rows)
    loads = [pltpu.make_async_copy(mine.at[:, pl.ds(rows, 8)], raw_ref, sems.at[2 * PIECES])]
    for piece in range(PIECES):
        chips = pl.ds(piece * span, span)
        for i, (source, place) in enumerate(((mine, first_rows), (peer, other_rows))):
            loads.append(
                pltpu.make_async_copy(
                    source.at[chips, pl.ds(0, rows)], kv_ref.at[chips, place], sems.at[2 * piece + i]
                )
            )
    for load in loads:
        load.start()
    row = lax.broadcasted_iota(jnp.int32, (side, side), 0)
    col = lax.broadcasted_iota(jnp.int32, (side, side), 1)
    tri_ref[...] = (row > col).astype(jnp.float32)
    loads[0].wait()
    raw = raw_ref[...]
    none = jnp.zeros(raw.shape[:2] + (HEAD_DIM,), jnp.bfloat16)
    early = jnp.concatenate([raw[:, :, :HEAD_DIM], none], axis=2)
    late = jnp.concatenate([raw[:, :, HEAD_DIM:], none], axis=2)
    query_ref[...] = jnp.concatenate([early, late], axis=1).reshape(query_ref.shape)
    for load in loads[1:]:
        load.wait()

    def advance(tile, first, skip, diagonal):
        query = query_ref[tile, skip:]
        keys = [kv_ref[first + i] for i in range(GROUP)]
        scores = [
            lax.dot_general(query, kv, (((1,), (1,)), ((), ())), preferred_element_type=jnp.float32)
            * (HEAD_DIM**-0.5 * LOG2E)
            for kv in keys
        ]
        costs = [jnp.maximum(s, 0.0) + jnp.log2(1.0 + jnp.exp2(-jnp.abs(s))) for s in scores]
        slacks = [s - c for s, c in zip(scores, costs)]
        if diagonal is not None:
            shape = scores[0].shape
            place = skip + lax.broadcasted_iota(jnp.int32, shape, 0)
            place = place // 16 * side + place % 16 + offset - lax.broadcasted_iota(jnp.int32, shape, 1)
            live = [place > (diagonal + i) * side for i in range(GROUP)]
            costs = [jnp.where(l, c, 0.0) for l, c in zip(live, costs)]
        tri = tri_ref[...]
        insides = [jnp.dot(c, tri, preferred_element_type=jnp.float32) for c in costs]
        acc = acc_ref[skip:]
        for i in range(GROUP):
            weight = jnp.exp2(slacks[i] - insides[i])
            if diagonal is not None:
                weight = jnp.where(live[i], weight, 0.0)
            part = jnp.dot(weight.astype(jnp.bfloat16), keys[i], preferred_element_type=jnp.float32)
            acc = acc * jnp.exp2(-(insides[i][:, 0:1] + costs[i][:, 0:1])) + part
        acc_ref[skip:] = acc

    blocks = query_ref.shape[1] // 16
    steps = blocks // GROUP

    @pl.loop(0, query_ref.shape[0])
    def _(tile):
        acc_ref[...] = jnp.zeros_like(acc_ref)

        @pl.loop(0, steps * tile)
        def _(step):
            advance(tile, step * GROUP, 0, None)

        for step in range(steps):
            advance(tile, blocks * tile + step * GROUP, step * GROUP * 16, step * GROUP)
        done = acc_ref[:, HEAD_DIM:].reshape(blocks, 16, HEAD_DIM)
        done = jnp.concatenate([done[:, :8], done[:, 8:]], axis=2).astype(jnp.bfloat16)
        out_ref[pl.ds(tile * blocks, blocks)] = done


def attention(meta, mine, peer):
    chips, depth, _ = mine.shape
    side = 2 * (depth - 8)
    pairs = 136 * side * side
    return pl.pallas_call(
        attention_kernel,
        out_shape=jax.ShapeDtypeStruct((chips, 8, LANES), jnp.bfloat16),
        in_specs=[
            pl.BlockSpec(memory_space=pltpu.SMEM),
            pl.BlockSpec(memory_space=pl.ANY),
            pl.BlockSpec(memory_space=pl.ANY),
        ],
        out_specs=pl.BlockSpec(memory_space=pltpu.VMEM),
        scratch_shapes=[
            pltpu.VMEM((chips, side, LANES), jnp.bfloat16),
            pltpu.VMEM((chips, 8, LANES), jnp.bfloat16),
            pltpu.VMEM((side, side), jnp.float32),
            pltpu.VMEM((2, 2 * side, LANES), jnp.bfloat16),
            pltpu.VMEM((2 * side, LANES), jnp.float32),
            pltpu.SemaphoreType.DMA((2 * PIECES + 1,)),
        ],
        compiler_params=pltpu.CompilerParams(vmem_limit_bytes=VMEM_BYTES),
        cost_estimate=pl.CostEstimate(
            flops=pairs * 2 * 768, bytes_accessed=6 * 2**20, transcendentals=pairs * 3
        ),
        name="attend",
    )(meta, mine, peer)


MAIN = 16
TAIL = 4


def expand(count, slots, experts, first):
    row = lax.broadcasted_iota(jnp.int32, (count * slots, experts), 0)
    col = lax.broadcasted_iota(jnp.int32, (count * slots, experts), 1)
    return (col == first + row // slots).astype(jnp.bfloat16)


STEP = 16


def copy_group(source, target, sems, start, count, parts):
    each = count // parts
    return [
        pltpu.make_async_copy(
            source.at[pl.ds(start + i * each, each)],
            target.at[pl.ds(start + i * each, each)],
            sems.at[start // each + i],
        )
        for i in range(parts)
    ]


def dispatch_kernel(
    attended_ref,
    residual_ref,
    weight_ref,
    gain_ref,
    rank_ref,
    mixed_ref,
    normed_ref,
    out_ref,
    heads_ref,
):
    count, _, half = out_ref.shape
    experts, tokens = rank_ref.shape

    @pl.when(pl.program_id(0) == 0)
    def _():
        for head in range(8):
            rows = attended_ref[8 * head : 8 * head + 8]
            rows = jnp.concatenate([rows[:, :, :HEAD_DIM], rows[:, :, HEAD_DIM:]], axis=1)
            heads_ref[:, head * HEAD_DIM : (head + 1) * HEAD_DIM] = rows.reshape(tokens, HEAD_DIM)
        projected = jnp.dot(heads_ref[...], weight_ref[...], preferred_element_type=jnp.float32)
        mixed = (residual_ref[...].astype(jnp.float32) + projected).astype(jnp.bfloat16)
        mixed_ref[...] = mixed
        mixed = mixed.astype(jnp.float32)
        inverse = lax.rsqrt(jnp.mean(mixed * mixed, axis=1, keepdims=True) + norm_eps)
        normed_ref[...] = (mixed * inverse * gain_ref[...]).astype(jnp.bfloat16)

    left, right = normed_ref[:, :half], normed_ref[:, half:]
    first = pl.program_id(0) * count

    def chosen(slots, lowest):
        rank = jnp.dot(
            expand(count, slots, experts, first), rank_ref[...], preferred_element_type=jnp.float32
        )
        slot = lowest + lax.broadcasted_iota(jnp.int32, rank.shape, 0) % (slots if lowest == 0 else TAIL)
        return (rank == slot.astype(jnp.float32)).astype(jnp.bfloat16)

    def pick(rows, side):
        return jnp.dot(rows, side, preferred_element_type=jnp.float32)

    main, tail = chosen(MAIN, 0), chosen(2 * TAIL, MAIN)
    out_ref[:, 0:MAIN, :] = pick(main, left).astype(jnp.bfloat16).reshape(count, MAIN, half)
    out_ref[:, MAIN : 2 * MAIN, :] = pick(main, right).astype(jnp.bfloat16).reshape(count, MAIN, half)
    early = lax.broadcasted_iota(jnp.int32, (tail.shape[0], half), 0) % (2 * TAIL) < TAIL
    both = jnp.where(early, pick(tail, left), pick(tail, right))
    out_ref[:, 2 * MAIN :, :] = both.astype(jnp.bfloat16).reshape(count, 2 * TAIL, half)


def dispatch(attended, residual, out_weight, gain, ranks, experts):
    tokens, width = residual.shape
    step = 32
    whole = lambda i: (0, 0)
    return pl.pallas_call(
        dispatch_kernel,
        grid=(experts // step,),
        in_specs=[
            pl.BlockSpec(attended.shape, lambda i: (0, 0, 0)),
            pl.BlockSpec(residual.shape, whole),
            pl.BlockSpec(out_weight.shape, whole),
            pl.BlockSpec(gain.shape, whole),
            pl.BlockSpec((experts, tokens), whole),
        ],
        out_specs=[
            pl.BlockSpec((tokens, width), whole),
            pl.BlockSpec((tokens, width), whole),
            pl.BlockSpec((step, 2 * (MAIN + TAIL), width // 2), lambda i: (i, 0, 0)),
        ],
        out_shape=[
            jax.ShapeDtypeStruct((tokens, width), jnp.bfloat16),
            jax.ShapeDtypeStruct((tokens, width), jnp.bfloat16),
            jax.ShapeDtypeStruct((experts, 2 * (MAIN + TAIL), width // 2), jnp.bfloat16),
        ],
        scratch_shapes=[pltpu.VMEM((tokens, 8 * HEAD_DIM), jnp.bfloat16)],
        compiler_params=pltpu.CompilerParams(vmem_limit_bytes=VMEM_BYTES),
        cost_estimate=pl.CostEstimate(flops=10**9, bytes_accessed=10**7, transcendentals=0),
        name="dispatch",
    )(attended, residual, out_weight, gain, ranks)


PASS = 16


def expert_kernel(
    rows,
    gate0,
    up0,
    gate1,
    up1,
    down0,
    down1,
    shared_gate,
    shared_up,
    shared_down,
    mixed,
    normed,
    out,
    base_ref,
    spread_ref,
    rows_ref,
    rows2_ref,
    out_ref,
    gate0_ref,
    up0_ref,
    gate1_ref,
    up1_ref,
    down0_ref,
    down1_ref,
    shared_gate_ref,
    shared_up_ref,
    shared_down_ref,
    mixed_ref,
    normed_ref,
    row_sems,
    sems,
    out_sems,
):
    total, _, half = rows_ref.shape
    tails, mains = PASS * TAIL, PASS * MAIN

    def halves(source, target, at):
        middle = source.shape[0] // 2
        return [
            pltpu.make_async_copy(source.at[part], target.at[part], sems.at[at + i])
            for i, part in enumerate((pl.ds(0, middle), pl.ds(middle, middle)))
        ]

    loads = []
    for source, target in (
        (gate0, gate0_ref),
        (up0, up0_ref),
        (gate1, gate1_ref),
        (up1, up1_ref),
        (down0, down0_ref),
        (down1, down1_ref),
    ):
        loads.append(halves(source.at[0], target.at[0], 2 * len(loads)))
    for source, target in (
        (shared_gate, shared_gate_ref),
        (shared_up, shared_up_ref),
        (shared_down, shared_down_ref),
        (mixed, mixed_ref),
        (normed, normed_ref),
    ):
        loads.append(halves(source, target, 2 * len(loads)))
    row_loads = [copy_group(rows, rows_ref, row_sems, first, PASS, 4) for first in range(0, total, PASS)]

    def start(groups):
        for group in groups:
            for copy in group:
                copy.start()

    def finish(groups):
        for group in groups:
            for copy in group:
                copy.wait()

    start(row_loads[:1])
    start(loads[:6])
    start(row_loads[1:])
    start(loads[6:])
    row = lax.broadcasted_iota(jnp.int32, (2 * tails, 2 * tails), 0)
    col = lax.broadcasted_iota(jnp.int32, (2 * tails, 2 * tails), 1)
    slot = row % tails
    home = slot // TAIL * (2 * TAIL) + row // tails * TAIL + slot % TAIL
    spread_ref[...] = (home == col).astype(jnp.bfloat16)

    def hidden(rows, gate_matrix, up_matrix):
        gate = jnp.dot(rows, gate_matrix, preferred_element_type=jnp.float32)
        upward = jnp.dot(rows, up_matrix, preferred_element_type=jnp.float32)
        return (jax.nn.silu(gate) * upward).astype(jnp.bfloat16)

    copies = []
    for turn, first in enumerate(range(0, total, PASS)):
        finish(row_loads[turn : turn + 1])
        part = slice(first, first + PASS)
        spread = spread_ref[...]
        rows2_ref[:mains, :half] = rows_ref[part, 0:MAIN, :].reshape(mains, half)
        rows2_ref[:mains, half:] = rows_ref[part, MAIN : 2 * MAIN, :].reshape(mains, half)
        ends = jnp.dot(
            spread, rows_ref[part, 2 * MAIN :, :].reshape(2 * tails, half), preferred_element_type=jnp.float32
        ).astype(jnp.bfloat16)
        rows2_ref[mains:, :half] = ends[:tails]
        rows2_ref[mains:, half:] = ends[tails:]
        if turn == 0:
            finish(loads[0:2])
        act0 = hidden(rows2_ref[...], gate0_ref[0], up0_ref[0])
        if turn == 0:
            finish(loads[2:4])
        act1 = hidden(rows2_ref[...], gate1_ref[0], up1_ref[0])
        if turn == 0:
            finish(loads[4:6])
        ends = []
        for side in range(2):
            span = slice(side * half, (side + 1) * half)
            result = jnp.dot(act0, down0_ref[0, :, span], preferred_element_type=jnp.float32) + jnp.dot(
                act1, down1_ref[0, :, span], preferred_element_type=jnp.float32
            )
            result = result.astype(jnp.bfloat16)
            out_ref[part, side * MAIN : (side + 1) * MAIN, :] = result[:mains].reshape(PASS, MAIN, half)
            ends.append(result[mains:])
        ends = lax.dot_general(
            spread, jnp.concatenate(ends, axis=0), (((0,), (0,)), ((), ())), preferred_element_type=jnp.float32
        )
        out_ref[part, 2 * MAIN :, :] = ends.astype(jnp.bfloat16).reshape(PASS, 2 * TAIL, half)
        group = copy_group(out_ref, out, out_sems, first, PASS, 4)
        start([group])
        copies.append(group)

    finish(loads[6:])
    act = hidden(normed_ref[...], shared_gate_ref[...], shared_up_ref[...])
    base_ref[...] = mixed_ref[...].astype(jnp.float32) + jnp.dot(
        act, shared_down_ref[...], preferred_element_type=jnp.float32
    )
    finish(copies)


def expert(rows, weights, mixed, normed):
    local_refs = list(weights) + [mixed, normed]
    return pl.pallas_call(
        expert_kernel,
        in_specs=[pl.BlockSpec(memory_space=pl.ANY)] * (1 + len(local_refs)),
        out_specs=[pl.BlockSpec(memory_space=pl.ANY), pl.BlockSpec(memory_space=pltpu.VMEM)],
        out_shape=[
            jax.ShapeDtypeStruct(rows.shape, jnp.bfloat16),
            jax.ShapeDtypeStruct(mixed.shape, jnp.float32),
        ],
        scratch_shapes=[
            pltpu.VMEM((PASS * 2 * TAIL, PASS * 2 * TAIL), jnp.bfloat16),
            pltpu.VMEM(rows.shape, jnp.bfloat16),
            pltpu.VMEM((PASS * (MAIN + TAIL), 2 * rows.shape[2]), jnp.bfloat16),
            pltpu.VMEM(rows.shape, jnp.bfloat16),
        ]
        + [pltpu.VMEM(w.shape, w.dtype) for w in local_refs]
        + [
            pltpu.SemaphoreType.DMA((16,)),
            pltpu.SemaphoreType.DMA((2 * len(local_refs),)),
            pltpu.SemaphoreType.DMA((16,)),
        ],
        compiler_params=pltpu.CompilerParams(vmem_limit_bytes=VMEM_BYTES - 2**21),
        cost_estimate=pl.CostEstimate(flops=8 * 10**9, bytes_accessed=17 * 10**6, transcendentals=10**6),
        name="expert",
    )(rows, *local_refs)


def combine_kernel(rows_ref, ranks_ref, base_ref, out_ref, acc_ref):
    count, _, half = rows_ref.shape
    tokens = base_ref.shape[0]
    experts = ranks_ref.shape[0] // 3
    at = pl.program_id(0)

    @pl.when(at == 0)
    def _():
        acc_ref[...] = base_ref[...]

    def weights(slots, wanted):
        chosen = expand(count, slots, experts, at * count)
        rank, high, low = [
            jnp.dot(chosen, ranks_ref[i * experts : (i + 1) * experts], preferred_element_type=jnp.float32)
            for i in range(3)
        ]
        slot = wanted(lax.broadcasted_iota(jnp.int32, rank.shape, 0) % slots).astype(jnp.float32)
        here = rank == slot
        parts = [jnp.where(here, part, 0.0) for part in (high, low)]
        return jnp.concatenate(parts, axis=1).T.astype(jnp.bfloat16)

    main = weights(MAIN, lambda slot: slot)
    ends = rows_ref[:, 2 * MAIN :, :].reshape(count * 2 * TAIL, half)
    for part in range(2):
        tail = weights(
            2 * TAIL, lambda slot: jnp.where(slot // TAIL == part, MAIN + slot % TAIL, -2)
        )
        rows = rows_ref[:, part * MAIN : (part + 1) * MAIN, :].reshape(count * MAIN, half)
        total = jnp.dot(main, rows, preferred_element_type=jnp.float32) + jnp.dot(
            tail, ends, preferred_element_type=jnp.float32
        )
        span = pl.ds(part * half, half)
        acc_ref[:, span] += total[:tokens] + total[tokens:]

    @pl.when(at == pl.num_programs(0) - 1)
    def _():
        out_ref[...] = acc_ref[...].astype(jnp.bfloat16)


def combine(rows, ranks, base):
    step = 32
    whole = lambda i: (0, 0)
    return pl.pallas_call(
        combine_kernel,
        grid=(rows.shape[0] // step,),
        in_specs=[
            pl.BlockSpec((step,) + rows.shape[1:], lambda i: (i, 0, 0)),
            pl.BlockSpec(ranks.shape, whole),
            pl.BlockSpec(base.shape, whole),
        ],
        out_specs=pl.BlockSpec(base.shape, whole),
        out_shape=jax.ShapeDtypeStruct(base.shape, jnp.bfloat16),
        scratch_shapes=[pltpu.VMEM(base.shape, jnp.float32)],
        compiler_params=pltpu.CompilerParams(vmem_limit_bytes=VMEM_BYTES),
        cost_estimate=pl.CostEstimate(flops=10**9, bytes_accessed=10**7, transcendentals=0),
        name="combine",
    )(rows, ranks, base)


def local(
    queries,
    key_rows,
    value_rows,
    residual,
    out_weight,
    norm_gain,
    routes,
    route_weight,
    expert_gate,
    expert_up,
    expert_down,
    shared_gate,
    shared_up,
    shared_down,
):
    core = lax.axis_index("tp")
    offset = 128 * core + 16 * (lax.axis_index("sp") % 8)
    swap = [(0, 1), (1, 0)]
    cores = core[None].astype(jnp.int32)
    keep, send = pack(cores, queries, key_rows, value_rows)
    taken = lax.ppermute(send, "tp", swap)
    mine = lax.all_to_all(spread(cores, keep, taken), "sp", 0, 0, tiled=True)
    peer = lax.ppermute(mine, "tp", swap)
    mine, routes, route_weight = lax.optimization_barrier((mine, routes, route_weight))
    ranks = route(routes.T, route_weight.T, 64)
    peer, ranks, expert_gate_, expert_up_, expert_down_ = lax.optimization_barrier(
        (peer, ranks, expert_gate, expert_up, expert_down)
    )
    attended = attention(jnp.stack([core, offset]).astype(jnp.int32), mine, peer)
    gate_other = lax.ppermute(expert_gate_, "tp", swap)
    up_other = lax.ppermute(expert_up_, "tp", swap)
    down_other = lax.ppermute(expert_down_, "tp", swap)
    attended, gate_other, up_other, down_other = lax.optimization_barrier(
        (attended, gate_other, up_other, down_other)
    )
    attended = lax.all_to_all(attended, "sp", 0, 0, tiled=True)
    experts = lax.axis_size("sp")
    mixed, normed, outgoing = dispatch(
        attended, residual, out_weight, norm_gain[None, :], ranks, experts
    )
    incoming = lax.all_to_all(outgoing, "sp", 0, 0, tiled=True)
    result, base = expert(
        incoming,
        (
            expert_gate,
            expert_up,
            gate_other,
            up_other,
            expert_down,
            down_other,
            shared_gate,
            shared_up,
            shared_down,
        ),
        mixed,
        normed,
    )
    returned = lax.all_to_all(result, "sp", 0, 0, tiled=True)
    return combine(returned, ranks, base)


def solution(mesh):
    return jax.shard_map(
        local,
        mesh=mesh,
        in_specs=(
            P("sp", "tp"),
            P("sp", "tp"),
            P("sp", "tp"),
            P(("sp", "tp"), None),
            P(),
            P(),
            P(("sp", "tp"), None),
            P(("sp", "tp"), None),
            P("sp", None, "tp"),
            P("sp", None, "tp"),
            P("sp", "tp", None),
            P(),
            P(),
            P(),
        ),
        out_specs=P(("sp", "tp"), None),
        check_vma=False,
    )
```

```python
import jax
import jax.numpy as jnp
from jax import lax
from jax.experimental import pallas as pl
from jax.experimental.pallas import tpu as pltpu
from jax.sharding import PartitionSpec as P

HEAD_DIM = 64
LANES = 128
TOPK = 8
LOG2E = 1.4426950408889634
norm_eps = 1e-06


VMEM_BYTES = 67043328


def pack_kernel(core_ref, query_ref, key_ref, value_ref, keep_out, send_out):
    heads, rows = keep_out.shape[0], query_ref.shape[0] // 2
    core = core_ref[0]
    for out, half in ((keep_out, core), (send_out, 1 - core)):
        own = pl.ds(half * rows, rows)
        for head in range(heads):
            span = slice(head * HEAD_DIM, (head + 1) * HEAD_DIM)
            out[head, :rows] = jnp.concatenate([key_ref[own, span], value_ref[own, span]], axis=1)
            query = query_ref[own, span].reshape(rows // 16, 16, HEAD_DIM)
            query = jnp.concatenate([query[:, :8], query[:, 8:]], axis=2)
            out[head, rows:] = query.reshape(rows // 2, LANES)


def pack(core, queries, key_rows, value_rows):
    side, width = key_rows.shape
    half = jax.ShapeDtypeStruct((width // HEAD_DIM, side // 2 + side // 4, LANES), jnp.bfloat16)
    return pl.pallas_call(
        pack_kernel,
        in_specs=[pl.BlockSpec(memory_space=pltpu.SMEM)] + [pl.BlockSpec(memory_space=pltpu.VMEM)] * 3,
        out_specs=[pl.BlockSpec(memory_space=pltpu.VMEM)] * 2,
        out_shape=[half, half],
        name="pack",
    )(core, queries, key_rows, value_rows)


def spread_kernel(core_ref, keep_ref, taken_ref, out_ref):
    chips, depth, _ = out_ref.shape
    rows = depth - 8
    for head in range(chips // 8):
        mine = head // 4 == core_ref[0]
        held = jnp.where(mine, keep_ref[head % 4], taken_ref[head % 4])
        for chip in range(8):
            out_ref[8 * head + chip, :rows] = held[:rows]
            out_ref[8 * head + chip, rows:] = held[rows + 8 * chip : rows + 8 * chip + 8]


def spread(core, keep, taken):
    shape = (64, keep.shape[1] * 2 // 3 + 8, LANES)
    return pl.pallas_call(
        spread_kernel,
        in_specs=[pl.BlockSpec(memory_space=pltpu.SMEM)] + [pl.BlockSpec(memory_space=pltpu.VMEM)] * 2,
        out_specs=pl.BlockSpec(memory_space=pltpu.VMEM),
        out_shape=jax.ShapeDtypeStruct(shape, jnp.bfloat16),
        compiler_params=pltpu.CompilerParams(vmem_limit_bytes=16 * 2**20),
        name="spread",
    )(core, keep, taken)


def route_kernel(routes_ref, weight_ref, out_ref):
    tokens, experts = routes_ref.shape[1], out_ref.shape[0] // 3
    names = lax.broadcasted_iota(jnp.int32, (experts, tokens), 0)
    pick = jnp.zeros((experts, tokens), jnp.float32)
    share = jnp.zeros((experts, tokens), jnp.float32)
    for k in range(TOPK):
        named = routes_ref[k : k + 1, :] == names
        pick = jnp.where(named, 1.0, pick)
        share = jnp.where(named, weight_ref[k : k + 1, :], share)
    row = lax.broadcasted_iota(jnp.int32, (tokens, tokens), 0)
    col = lax.broadcasted_iota(jnp.int32, (tokens, tokens), 1)
    above = (row < col).astype(jnp.bfloat16)
    rank = jnp.dot(pick.astype(jnp.bfloat16), above, preferred_element_type=jnp.float32)
    out_ref[0:experts] = jnp.where(pick > 0.0, rank, -1.0).astype(jnp.bfloat16)
    high = share.astype(jnp.bfloat16)
    out_ref[experts : 2 * experts] = high
    out_ref[2 * experts :] = (share - high.astype(jnp.float32)).astype(jnp.bfloat16)


def route(routes, route_weight, experts):
    return pl.pallas_call(
        route_kernel,
        out_shape=jax.ShapeDtypeStruct((3 * experts, routes.shape[1]), jnp.bfloat16),
        in_specs=[pl.BlockSpec(memory_space=pltpu.VMEM)] * 2,
        out_specs=pl.BlockSpec(memory_space=pltpu.VMEM),
        name="route",
    )(routes, route_weight)


GROUP = 4


def attention_kernel(meta_ref, mine_ref, peer, out_ref, kv_ref, tri_ref, query_ref, acc_ref, sems):
    core, offset = meta_ref[0], meta_ref[1]
    side = tri_ref.shape[0]
    rows = side // 2
    first_rows = pl.ds(pl.multiple_of(core * rows, rows), rows)
    other_rows = pl.ds(pl.multiple_of((1 - core) * rows, rows), rows)
    span = kv_ref.shape[0] // 4
    loads = []
    for piece in range(4):
        chips = pl.ds(piece * span, span)
        loads.append(
            pltpu.make_async_copy(peer.at[chips, pl.ds(0, rows)], kv_ref.at[chips, other_rows], sems.at[piece])
        )
        loads[-1].start()
    row = lax.broadcasted_iota(jnp.int32, (side, side), 0)
    col = lax.broadcasted_iota(jnp.int32, (side, side), 1)
    tri_ref[...] = (row > col).astype(jnp.float32)
    raw = mine_ref[:, rows:]
    none = jnp.zeros(raw.shape[:2] + (HEAD_DIM,), jnp.bfloat16)
    early = jnp.concatenate([raw[:, :, :HEAD_DIM], none], axis=2)
    late = jnp.concatenate([raw[:, :, HEAD_DIM:], none], axis=2)
    query_ref[...] = jnp.concatenate([early, late], axis=1).reshape(query_ref.shape)

    @pl.loop(0, kv_ref.shape[0] // 4)
    def _(turn):
        for i in range(4):
            kv_ref[4 * turn + i, first_rows] = mine_ref[4 * turn + i, :rows]

    for load in loads:
        load.wait()

    def advance(tile, first, skip, diagonal, count=GROUP):
        query = query_ref[tile, skip:]
        keys = [kv_ref[first + i] for i in range(count)]
        scores = [
            lax.dot_general(query, kv, (((1,), (1,)), ((), ())), preferred_element_type=jnp.float32)
            * (HEAD_DIM**-0.5 * LOG2E)
            for kv in keys
        ]
        costs = [jnp.maximum(s, 0.0) + jnp.log2(1.0 + jnp.exp2(-jnp.abs(s))) for s in scores]
        slacks = [s - c for s, c in zip(scores, costs)]
        if diagonal:
            edge = 16 * GROUP
            shape = (edge, side)
            place = lax.broadcasted_iota(jnp.int32, shape, 0)
            place = place // 16 * side + place % 16 + offset - lax.broadcasted_iota(jnp.int32, shape, 1)
            live = [place > i * side for i in range(count)]

            def masked(i, value):
                top = jnp.where(live[i], value[:edge], 0.0)
                return top if value.shape[0] == edge else jnp.concatenate([top, value[edge:]], axis=0)

            costs = [masked(i, c) for i, c in enumerate(costs)]
        tri = tri_ref[...]
        insides = [jnp.dot(c, tri, preferred_element_type=jnp.float32) for c in costs]
        acc = acc_ref[skip:]
        for i in range(count):
            weight = jnp.exp2(slacks[i] - insides[i])
            if diagonal:
                weight = masked(i, weight)
            part = jnp.dot(weight.astype(jnp.bfloat16), keys[i], preferred_element_type=jnp.float32)
            acc = acc * jnp.exp2(-jnp.sum(costs[i], axis=1, keepdims=True)) + part
        acc_ref[skip:] = acc

    blocks = query_ref.shape[1] // 16
    steps = blocks // GROUP

    @pl.loop(0, query_ref.shape[0])
    def _(tile):
        acc_ref[...] = jnp.zeros_like(acc_ref)

        @pl.loop(0, steps * tile // 2)
        def _(step):
            advance(tile, step * 2 * GROUP, 0, False, 2 * GROUP)

        for step in range(steps):
            advance(tile, blocks * tile + step * GROUP, step * GROUP * 16, True)
        done = acc_ref[:, HEAD_DIM:].reshape(blocks, 16, HEAD_DIM)
        done = jnp.concatenate([done[:, :8], done[:, 8:]], axis=2).astype(jnp.bfloat16)
        out_ref[pl.ds(tile * blocks, blocks)] = done


def attention(meta, mine, peer):
    chips, depth, _ = mine.shape
    side = 2 * (depth - 8)
    pairs = 136 * side * side
    return pl.pallas_call(
        attention_kernel,
        out_shape=jax.ShapeDtypeStruct((chips, 8, LANES), jnp.bfloat16),
        in_specs=[
            pl.BlockSpec(memory_space=pltpu.SMEM),
            pl.BlockSpec(memory_space=pltpu.VMEM),
            pl.BlockSpec(memory_space=pl.ANY),
        ],
        out_specs=pl.BlockSpec(memory_space=pltpu.VMEM),
        scratch_shapes=[
            pltpu.VMEM((chips, side, LANES), jnp.bfloat16),
            pltpu.VMEM((side, side), jnp.float32),
            pltpu.VMEM((2, 2 * side, LANES), jnp.bfloat16),
            pltpu.VMEM((2 * side, LANES), jnp.float32),
            pltpu.SemaphoreType.DMA((4,)),
        ],
        compiler_params=pltpu.CompilerParams(vmem_limit_bytes=40 * 2**20),
        cost_estimate=pl.CostEstimate(
            flops=pairs * 2 * 768, bytes_accessed=6 * 2**20, transcendentals=pairs * 3
        ),
        name="attend",
    )(meta, mine, peer)


MAIN = 16
TAIL = 4


def expand(count, slots, experts, first):
    row = lax.broadcasted_iota(jnp.int32, (count * slots, experts), 0)
    col = lax.broadcasted_iota(jnp.int32, (count * slots, experts), 1)
    return (col == first + row // slots).astype(jnp.bfloat16)


STEP = 16


def copy_group(source, target, sems, start, count, parts):
    each = count // parts
    return [
        pltpu.make_async_copy(
            source.at[pl.ds(start + i * each, each)],
            target.at[pl.ds(start + i * each, each)],
            sems.at[start // each + i],
        )
        for i in range(parts)
    ]


def dispatch_kernel(
    attended_ref,
    residual_ref,
    weight_ref,
    gain_ref,
    rank_ref,
    mixed_ref,
    normed_ref,
    out_ref,
    heads_ref,
):
    count, _, half = out_ref.shape
    experts, tokens = rank_ref.shape

    @pl.when(pl.program_id(0) == 0)
    def _():
        for head in range(8):
            rows = attended_ref[8 * head : 8 * head + 8]
            rows = jnp.concatenate([rows[:, :, :HEAD_DIM], rows[:, :, HEAD_DIM:]], axis=1)
            heads_ref[:, head * HEAD_DIM : (head + 1) * HEAD_DIM] = rows.reshape(tokens, HEAD_DIM)
        projected = jnp.dot(heads_ref[...], weight_ref[...], preferred_element_type=jnp.float32)
        mixed = (residual_ref[...].astype(jnp.float32) + projected).astype(jnp.bfloat16)
        mixed_ref[...] = mixed
        mixed = mixed.astype(jnp.float32)
        inverse = lax.rsqrt(jnp.mean(mixed * mixed, axis=1, keepdims=True) + norm_eps)
        normed_ref[...] = (mixed * inverse * gain_ref[...]).astype(jnp.bfloat16)

    left, right = normed_ref[:, :half], normed_ref[:, half:]
    first = pl.program_id(0) * count

    def chosen(slots, lowest):
        rank = jnp.dot(
            expand(count, slots, experts, first), rank_ref[...], preferred_element_type=jnp.float32
        )
        slot = lowest + lax.broadcasted_iota(jnp.int32, rank.shape, 0) % (slots if lowest == 0 else TAIL)
        return (rank == slot.astype(jnp.float32)).astype(jnp.bfloat16)

    def pick(rows, side):
        return jnp.dot(rows, side, preferred_element_type=jnp.float32)

    main, tail = chosen(MAIN, 0), chosen(2 * TAIL, MAIN)
    out_ref[:, 0:MAIN, :] = pick(main, left).astype(jnp.bfloat16).reshape(count, MAIN, half)
    out_ref[:, MAIN : 2 * MAIN, :] = pick(main, right).astype(jnp.bfloat16).reshape(count, MAIN, half)
    early = lax.broadcasted_iota(jnp.int32, (tail.shape[0], half), 0) % (2 * TAIL) < TAIL
    both = jnp.where(early, pick(tail, left), pick(tail, right))
    out_ref[:, 2 * MAIN :, :] = both.astype(jnp.bfloat16).reshape(count, 2 * TAIL, half)


def dispatch(attended, residual, out_weight, gain, ranks, experts):
    tokens, width = residual.shape
    step = 32
    whole = lambda i: (0, 0)
    return pl.pallas_call(
        dispatch_kernel,
        grid=(experts // step,),
        in_specs=[
            pl.BlockSpec(attended.shape, lambda i: (0, 0, 0)),
            pl.BlockSpec(residual.shape, whole),
            pl.BlockSpec(out_weight.shape, whole),
            pl.BlockSpec(gain.shape, whole),
            pl.BlockSpec((experts, tokens), whole),
        ],
        out_specs=[
            pl.BlockSpec((tokens, width), whole),
            pl.BlockSpec((tokens, width), whole),
            pl.BlockSpec((step, 2 * (MAIN + TAIL), width // 2), lambda i: (i, 0, 0)),
        ],
        out_shape=[
            jax.ShapeDtypeStruct((tokens, width), jnp.bfloat16),
            jax.ShapeDtypeStruct((tokens, width), jnp.bfloat16),
            jax.ShapeDtypeStruct((experts, 2 * (MAIN + TAIL), width // 2), jnp.bfloat16),
        ],
        scratch_shapes=[pltpu.VMEM((tokens, 8 * HEAD_DIM), jnp.bfloat16)],
        compiler_params=pltpu.CompilerParams(vmem_limit_bytes=32 * 2**20),
        cost_estimate=pl.CostEstimate(flops=10**9, bytes_accessed=10**7, transcendentals=0),
        name="dispatch",
    )(attended, residual, out_weight, gain, ranks)


PASS = 16


def expert_kernel(
    rows,
    gate0,
    up0,
    gate1,
    up1,
    down0,
    down1,
    shared_gate,
    shared_up,
    shared_down,
    mixed,
    normed,
    out,
    base_ref,
    spread_ref,
    rows_ref,
    rows2_ref,
    out_ref,
    gate0_ref,
    up0_ref,
    gate1_ref,
    up1_ref,
    down0_ref,
    down1_ref,
    shared_gate_ref,
    shared_up_ref,
    shared_down_ref,
    mixed_ref,
    normed_ref,
    row_sems,
    sems,
    out_sems,
):
    total, _, half = rows_ref.shape
    tails, mains = PASS * TAIL, PASS * MAIN

    def halves(source, target, at):
        middle = source.shape[0] // 2
        return [
            pltpu.make_async_copy(source.at[part], target.at[part], sems.at[at + i])
            for i, part in enumerate((pl.ds(0, middle), pl.ds(middle, middle)))
        ]

    loads = []
    for source, target in (
        (gate0, gate0_ref),
        (up0, up0_ref),
        (gate1, gate1_ref),
        (up1, up1_ref),
        (down0, down0_ref),
        (down1, down1_ref),
    ):
        loads.append(halves(source.at[0], target.at[0], 2 * len(loads)))
    for source, target in (
        (shared_gate, shared_gate_ref),
        (shared_up, shared_up_ref),
        (shared_down, shared_down_ref),
        (mixed, mixed_ref),
        (normed, normed_ref),
    ):
        loads.append(halves(source, target, 2 * len(loads)))
    row_loads = [copy_group(rows, rows_ref, row_sems, first, PASS, 4) for first in range(0, total, PASS)]

    def start(groups):
        for group in groups:
            for copy in group:
                copy.start()

    def finish(groups):
        for group in groups:
            for copy in group:
                copy.wait()

    start(row_loads[:1])
    start(loads[:6])
    start(row_loads[1:])
    start(loads[6:])
    row = lax.broadcasted_iota(jnp.int32, (2 * tails, 2 * tails), 0)
    col = lax.broadcasted_iota(jnp.int32, (2 * tails, 2 * tails), 1)
    slot = row % tails
    home = slot // TAIL * (2 * TAIL) + row // tails * TAIL + slot % TAIL
    spread_ref[...] = (home == col).astype(jnp.bfloat16)

    def hidden(rows, gate_matrix, up_matrix):
        gate = jnp.dot(rows, gate_matrix, preferred_element_type=jnp.float32)
        upward = jnp.dot(rows, up_matrix, preferred_element_type=jnp.float32)
        return (jax.nn.silu(gate) * upward).astype(jnp.bfloat16)

    copies = []
    for turn, first in enumerate(range(0, total, PASS)):
        finish(row_loads[turn : turn + 1])
        part = slice(first, first + PASS)
        spread = spread_ref[...]
        rows2_ref[:mains, :half] = rows_ref[part, 0:MAIN, :].reshape(mains, half)
        rows2_ref[:mains, half:] = rows_ref[part, MAIN : 2 * MAIN, :].reshape(mains, half)
        ends = jnp.dot(
            spread, rows_ref[part, 2 * MAIN :, :].reshape(2 * tails, half), preferred_element_type=jnp.float32
        ).astype(jnp.bfloat16)
        rows2_ref[mains:, :half] = ends[:tails]
        rows2_ref[mains:, half:] = ends[tails:]
        if turn == 0:
            finish(loads[0:2])
        act0 = hidden(rows2_ref[...], gate0_ref[0], up0_ref[0])
        if turn == 0:
            finish(loads[2:4])
        act1 = hidden(rows2_ref[...], gate1_ref[0], up1_ref[0])
        if turn == 0:
            finish(loads[4:6])
        ends = []
        for side in range(2):
            span = slice(side * half, (side + 1) * half)
            result = jnp.dot(act0, down0_ref[0, :, span], preferred_element_type=jnp.float32) + jnp.dot(
                act1, down1_ref[0, :, span], preferred_element_type=jnp.float32
            )
            result = result.astype(jnp.bfloat16)
            out_ref[part, side * MAIN : (side + 1) * MAIN, :] = result[:mains].reshape(PASS, MAIN, half)
            ends.append(result[mains:])
        ends = lax.dot_general(
            spread, jnp.concatenate(ends, axis=0), (((0,), (0,)), ((), ())), preferred_element_type=jnp.float32
        )
        out_ref[part, 2 * MAIN :, :] = ends.astype(jnp.bfloat16).reshape(PASS, 2 * TAIL, half)
        group = copy_group(out_ref, out, out_sems, first, PASS, 4)
        start([group])
        copies.append(group)

    finish(loads[6:])
    act = hidden(normed_ref[...], shared_gate_ref[...], shared_up_ref[...])
    base_ref[...] = mixed_ref[...].astype(jnp.float32) + jnp.dot(
        act, shared_down_ref[...], preferred_element_type=jnp.float32
    )
    finish(copies)


def expert(rows, weights, mixed, normed):
    local_refs = list(weights) + [mixed, normed]
    return pl.pallas_call(
        expert_kernel,
        in_specs=[pl.BlockSpec(memory_space=pl.ANY)] * (1 + len(local_refs)),
        out_specs=[pl.BlockSpec(memory_space=pl.ANY), pl.BlockSpec(memory_space=pltpu.VMEM)],
        out_shape=[
            jax.ShapeDtypeStruct(rows.shape, jnp.bfloat16),
            jax.ShapeDtypeStruct(mixed.shape, jnp.float32),
        ],
        scratch_shapes=[
            pltpu.VMEM((PASS * 2 * TAIL, PASS * 2 * TAIL), jnp.bfloat16),
            pltpu.VMEM(rows.shape, jnp.bfloat16),
            pltpu.VMEM((PASS * (MAIN + TAIL), 2 * rows.shape[2]), jnp.bfloat16),
            pltpu.VMEM(rows.shape, jnp.bfloat16),
        ]
        + [pltpu.VMEM(w.shape, w.dtype) for w in local_refs]
        + [
            pltpu.SemaphoreType.DMA((16,)),
            pltpu.SemaphoreType.DMA((2 * len(local_refs),)),
            pltpu.SemaphoreType.DMA((16,)),
        ],
        compiler_params=pltpu.CompilerParams(vmem_limit_bytes=VMEM_BYTES - 2**21),
        cost_estimate=pl.CostEstimate(flops=8 * 10**9, bytes_accessed=17 * 10**6, transcendentals=10**6),
        name="expert",
    )(rows, *local_refs)


def combine_kernel(rows_ref, ranks_ref, base_ref, out_ref, acc_ref):
    count, _, half = rows_ref.shape
    tokens = base_ref.shape[0]
    experts = ranks_ref.shape[0] // 3
    at = pl.program_id(0)

    @pl.when(at == 0)
    def _():
        acc_ref[...] = base_ref[...]

    def weights(slots, wanted):
        chosen = expand(count, slots, experts, at * count)
        rank, high, low = [
            jnp.dot(chosen, ranks_ref[i * experts : (i + 1) * experts], preferred_element_type=jnp.float32)
            for i in range(3)
        ]
        slot = wanted(lax.broadcasted_iota(jnp.int32, rank.shape, 0) % slots).astype(jnp.float32)
        here = rank == slot
        parts = [jnp.where(here, part, 0.0) for part in (high, low)]
        return jnp.concatenate(parts, axis=1).T.astype(jnp.bfloat16)

    main = weights(MAIN, lambda slot: slot)
    ends = rows_ref[:, 2 * MAIN :, :].reshape(count * 2 * TAIL, half)
    for part in range(2):
        tail = weights(
            2 * TAIL, lambda slot: jnp.where(slot // TAIL == part, MAIN + slot % TAIL, -2)
        )
        rows = rows_ref[:, part * MAIN : (part + 1) * MAIN, :].reshape(count * MAIN, half)
        total = jnp.dot(main, rows, preferred_element_type=jnp.float32) + jnp.dot(
            tail, ends, preferred_element_type=jnp.float32
        )
        span = pl.ds(part * half, half)
        acc_ref[:, span] += total[:tokens] + total[tokens:]

    @pl.when(at == pl.num_programs(0) - 1)
    def _():
        out_ref[...] = acc_ref[...].astype(jnp.bfloat16)


def combine(rows, ranks, base):
    step = 32
    whole = lambda i: (0, 0)
    return pl.pallas_call(
        combine_kernel,
        grid=(rows.shape[0] // step,),
        in_specs=[
            pl.BlockSpec((step,) + rows.shape[1:], lambda i: (i, 0, 0)),
            pl.BlockSpec(ranks.shape, whole),
            pl.BlockSpec(base.shape, whole),
        ],
        out_specs=pl.BlockSpec(base.shape, whole),
        out_shape=jax.ShapeDtypeStruct(base.shape, jnp.bfloat16),
        scratch_shapes=[pltpu.VMEM(base.shape, jnp.float32)],
        compiler_params=pltpu.CompilerParams(vmem_limit_bytes=VMEM_BYTES),
        cost_estimate=pl.CostEstimate(flops=10**9, bytes_accessed=10**7, transcendentals=0),
        name="combine",
    )(rows, ranks, base)


def local(
    queries,
    key_rows,
    value_rows,
    residual,
    out_weight,
    norm_gain,
    routes,
    route_weight,
    expert_gate,
    expert_up,
    expert_down,
    shared_gate,
    shared_up,
    shared_down,
):
    core = lax.axis_index("tp")
    offset = 128 * core + 16 * (lax.axis_index("sp") % 8)
    swap = [(0, 1), (1, 0)]
    cores = core[None].astype(jnp.int32)
    keep, send = pack(cores, queries, key_rows, value_rows)
    taken = lax.ppermute(send, "tp", swap)
    mine = lax.all_to_all(spread(cores, keep, taken), "sp", 0, 0, tiled=True)
    peer = lax.ppermute(mine, "tp", swap)
    mine, routes, route_weight = lax.optimization_barrier((mine, routes, route_weight))
    ranks = route(routes.T, route_weight.T, 64)
    peer, ranks, expert_gate_, expert_up_, expert_down_ = lax.optimization_barrier(
        (peer, ranks, expert_gate, expert_up, expert_down)
    )
    attended = attention(jnp.stack([core, offset]).astype(jnp.int32), mine, peer)
    gate_other = lax.ppermute(expert_gate_, "tp", swap)
    up_other = lax.ppermute(expert_up_, "tp", swap)
    down_other = lax.ppermute(expert_down_, "tp", swap)
    attended, gate_other, up_other, down_other = lax.optimization_barrier(
        (attended, gate_other, up_other, down_other)
    )
    attended = lax.all_to_all(attended, "sp", 0, 0, tiled=True)
    experts = lax.axis_size("sp")
    mixed, normed, outgoing = dispatch(
        attended, residual, out_weight, norm_gain[None, :], ranks, experts
    )
    incoming = lax.all_to_all(outgoing, "sp", 0, 0, tiled=True)
    result, base = expert(
        incoming,
        (
            expert_gate,
            expert_up,
            gate_other,
            up_other,
            expert_down,
            down_other,
            shared_gate,
            shared_up,
            shared_down,
        ),
        mixed,
        normed,
    )
    returned = lax.all_to_all(result, "sp", 0, 0, tiled=True)
    return combine(returned, ranks, base)


def solution(mesh):
    return jax.shard_map(
        local,
        mesh=mesh,
        in_specs=(
            P("sp", "tp"),
            P("sp", "tp"),
            P("sp", "tp"),
            P(("sp", "tp"), None),
            P(),
            P(),
            P(("sp", "tp"), None),
            P(("sp", "tp"), None),
            P("sp", None, "tp"),
            P("sp", None, "tp"),
            P("sp", "tp", None),
            P(),
            P(),
            P(),
        ),
        out_specs=P(("sp", "tp"), None),
        check_vma=False,
    )
```

```python
import jax
import jax.numpy as jnp
from jax import lax
from jax.experimental import pallas as pl
from jax.experimental.pallas import tpu as pltpu
from jax.sharding import PartitionSpec as P

HEAD_DIM = 64
LANES = 128
TOPK = 8
LOG2E = 1.4426950408889634
norm_eps = 1e-06


VMEM_BYTES = 67043328


def pack_kernel(core_ref, query_ref, key_ref, value_ref, keep_out, send_out):
    heads, rows = keep_out.shape[0], query_ref.shape[0] // 2
    core = core_ref[0]
    for out, half in ((keep_out, core), (send_out, 1 - core)):
        own = pl.ds(half * rows, rows)
        for head in range(heads):
            span = slice(head * HEAD_DIM, (head + 1) * HEAD_DIM)
            out[head, :rows] = jnp.concatenate([key_ref[own, span], value_ref[own, span]], axis=1)
            query = query_ref[own, span].reshape(rows // 16, 16, HEAD_DIM)
            query = jnp.concatenate([query[:, :8], query[:, 8:]], axis=2)
            out[head, rows:] = query.reshape(rows // 2, LANES)


def pack(core, queries, key_rows, value_rows):
    side, width = key_rows.shape
    half = jax.ShapeDtypeStruct((width // HEAD_DIM, side // 2 + side // 4, LANES), jnp.bfloat16)
    return pl.pallas_call(
        pack_kernel,
        in_specs=[pl.BlockSpec(memory_space=pltpu.SMEM)] + [pl.BlockSpec(memory_space=pltpu.VMEM)] * 3,
        out_specs=[pl.BlockSpec(memory_space=pltpu.VMEM)] * 2,
        out_shape=[half, half],
        name="pack",
    )(core, queries, key_rows, value_rows)


def spread_kernel(core_ref, keep_ref, taken_ref, out_ref):
    chips, depth, _ = out_ref.shape
    rows = depth - 8
    for head in range(chips // 8):
        mine = head // 4 == core_ref[0]
        held = jnp.where(mine, keep_ref[head % 4], taken_ref[head % 4])
        for chip in range(8):
            out_ref[8 * head + chip, :rows] = held[:rows]
            out_ref[8 * head + chip, rows:] = held[rows + 8 * chip : rows + 8 * chip + 8]


def spread(core, keep, taken):
    shape = (64, keep.shape[1] * 2 // 3 + 8, LANES)
    return pl.pallas_call(
        spread_kernel,
        in_specs=[pl.BlockSpec(memory_space=pltpu.SMEM)] + [pl.BlockSpec(memory_space=pltpu.VMEM)] * 2,
        out_specs=pl.BlockSpec(memory_space=pltpu.VMEM),
        out_shape=jax.ShapeDtypeStruct(shape, jnp.bfloat16),
        compiler_params=pltpu.CompilerParams(vmem_limit_bytes=16 * 2**20),
        name="spread",
    )(core, keep, taken)


def route_kernel(routes_ref, weight_ref, out_ref):
    tokens, experts = routes_ref.shape[1], out_ref.shape[0] // 3
    names = lax.broadcasted_iota(jnp.int32, (experts, tokens), 0)
    pick = jnp.zeros((experts, tokens), jnp.float32)
    share = jnp.zeros((experts, tokens), jnp.float32)
    for k in range(TOPK):
        named = routes_ref[k : k + 1, :] == names
        pick = jnp.where(named, 1.0, pick)
        share = jnp.where(named, weight_ref[k : k + 1, :], share)
    row = lax.broadcasted_iota(jnp.int32, (tokens, tokens), 0)
    col = lax.broadcasted_iota(jnp.int32, (tokens, tokens), 1)
    above = (row < col).astype(jnp.bfloat16)
    rank = jnp.dot(pick.astype(jnp.bfloat16), above, preferred_element_type=jnp.float32)
    out_ref[0:experts] = jnp.where(pick > 0.0, rank, -1.0).astype(jnp.bfloat16)
    high = share.astype(jnp.bfloat16)
    out_ref[experts : 2 * experts] = high
    out_ref[2 * experts :] = (share - high.astype(jnp.float32)).astype(jnp.bfloat16)


def route(routes, route_weight, experts):
    return pl.pallas_call(
        route_kernel,
        out_shape=jax.ShapeDtypeStruct((3 * experts, routes.shape[1]), jnp.bfloat16),
        in_specs=[pl.BlockSpec(memory_space=pltpu.VMEM)] * 2,
        out_specs=pl.BlockSpec(memory_space=pltpu.VMEM),
        name="route",
    )(routes, route_weight)


GROUP = 4


def attention_kernel(meta_ref, mine_ref, peer, out_ref, kv_ref, tri_ref, query_ref, acc_ref, sems):
    core, offset = meta_ref[0], meta_ref[1]
    side = tri_ref.shape[0]
    rows = side // 2
    first_rows = pl.ds(pl.multiple_of(core * rows, rows), rows)
    other_rows = pl.ds(pl.multiple_of((1 - core) * rows, rows), rows)
    span = kv_ref.shape[0] // 4
    loads = []
    for piece in range(4):
        chips = pl.ds(piece * span, span)
        loads.append(
            pltpu.make_async_copy(peer.at[chips, pl.ds(0, rows)], kv_ref.at[chips, other_rows], sems.at[piece])
        )
        loads[-1].start()
    row = lax.broadcasted_iota(jnp.int32, (side, side), 0)
    col = lax.broadcasted_iota(jnp.int32, (side, side), 1)
    tri_ref[...] = (row > col).astype(jnp.float32)
    raw = mine_ref[:, rows:]
    none = jnp.zeros(raw.shape[:2] + (HEAD_DIM,), jnp.bfloat16)
    early = jnp.concatenate([raw[:, :, :HEAD_DIM], none], axis=2)
    late = jnp.concatenate([raw[:, :, HEAD_DIM:], none], axis=2)
    query_ref[...] = jnp.concatenate([early, late], axis=1).reshape(query_ref.shape)

    @pl.loop(0, kv_ref.shape[0] // 4)
    def _(turn):
        for i in range(4):
            kv_ref[4 * turn + i, first_rows] = mine_ref[4 * turn + i, :rows]

    for load in loads:
        load.wait()

    def advance(tile, first, skip, diagonal, count=GROUP):
        query = query_ref[tile, skip:]
        keys = [kv_ref[first + i] for i in range(count)]
        scores = [
            lax.dot_general(query, kv, (((1,), (1,)), ((), ())), preferred_element_type=jnp.float32)
            * (HEAD_DIM**-0.5 * LOG2E)
            for kv in keys
        ]
        costs = [jnp.maximum(s, 0.0) + jnp.log2(1.0 + jnp.exp2(-jnp.abs(s))) for s in scores]
        slacks = [s - c for s, c in zip(scores, costs)]
        if diagonal:
            edge = 16 * GROUP
            shape = (edge, side)
            place = lax.broadcasted_iota(jnp.int32, shape, 0)
            place = place // 16 * side + place % 16 + offset - lax.broadcasted_iota(jnp.int32, shape, 1)
            live = [place > i * side for i in range(count)]

            def masked(i, value):
                top = jnp.where(live[i], value[:edge], 0.0)
                return top if value.shape[0] == edge else jnp.concatenate([top, value[edge:]], axis=0)

            costs = [masked(i, c) for i, c in enumerate(costs)]
        tri = tri_ref[...]
        insides = [jnp.dot(c, tri, preferred_element_type=jnp.float32) for c in costs]
        acc = acc_ref[skip:]
        for i in range(count):
            weight = jnp.exp2(slacks[i] - insides[i])
            if diagonal:
                weight = masked(i, weight)
            part = jnp.dot(weight.astype(jnp.bfloat16), keys[i], preferred_element_type=jnp.float32)
            acc = acc * jnp.exp2(-jnp.sum(costs[i], axis=1, keepdims=True)) + part
        acc_ref[skip:] = acc

    blocks = query_ref.shape[1] // 16
    steps = blocks // GROUP

    @pl.loop(0, query_ref.shape[0])
    def _(tile):
        acc_ref[...] = jnp.zeros_like(acc_ref)

        @pl.loop(0, steps * tile // 2)
        def _(step):
            advance(tile, step * 2 * GROUP, 0, False, 2 * GROUP)

        for step in range(steps):
            advance(tile, blocks * tile + step * GROUP, step * GROUP * 16, True)
        done = acc_ref[:, HEAD_DIM:].reshape(blocks, 16, HEAD_DIM)
        done = jnp.concatenate([done[:, :8], done[:, 8:]], axis=2).astype(jnp.bfloat16)
        out_ref[pl.ds(tile * blocks, blocks)] = done


def attention(meta, mine, peer):
    chips, depth, _ = mine.shape
    side = 2 * (depth - 8)
    pairs = 136 * side * side
    return pl.pallas_call(
        attention_kernel,
        out_shape=jax.ShapeDtypeStruct((chips, 8, LANES), jnp.bfloat16),
        in_specs=[
            pl.BlockSpec(memory_space=pltpu.SMEM),
            pl.BlockSpec(memory_space=pltpu.VMEM),
            pl.BlockSpec(memory_space=pl.ANY),
        ],
        out_specs=pl.BlockSpec(memory_space=pltpu.VMEM),
        scratch_shapes=[
            pltpu.VMEM((chips, side, LANES), jnp.bfloat16),
            pltpu.VMEM((side, side), jnp.float32),
            pltpu.VMEM((2, 2 * side, LANES), jnp.bfloat16),
            pltpu.VMEM((2 * side, LANES), jnp.float32),
            pltpu.SemaphoreType.DMA((4,)),
        ],
        compiler_params=pltpu.CompilerParams(vmem_limit_bytes=40 * 2**20),
        cost_estimate=pl.CostEstimate(
            flops=pairs * 2 * 768, bytes_accessed=6 * 2**20, transcendentals=pairs * 3
        ),
        name="attend",
    )(meta, mine, peer)


MAIN = 16
TAIL = 4


def expand(count, slots, experts, first):
    row = lax.broadcasted_iota(jnp.int32, (count * slots, experts), 0)
    col = lax.broadcasted_iota(jnp.int32, (count * slots, experts), 1)
    return (col == first + row // slots).astype(jnp.bfloat16)


STEP = 16


def copy_group(source, target, sems, start, count, parts):
    each = count // parts
    return [
        pltpu.make_async_copy(
            source.at[pl.ds(start + i * each, each)],
            target.at[pl.ds(start + i * each, each)],
            sems.at[start // each + i],
        )
        for i in range(parts)
    ]


def dispatch_kernel(
    attended_ref,
    residual_ref,
    weight_ref,
    gain_ref,
    rank_ref,
    mixed_ref,
    normed_ref,
    out_ref,
    heads_ref,
):
    count, _, half = out_ref.shape
    experts, tokens = rank_ref.shape

    @pl.when(pl.program_id(0) == 0)
    def _():
        for head in range(8):
            rows = attended_ref[8 * head : 8 * head + 8]
            rows = jnp.concatenate([rows[:, :, :HEAD_DIM], rows[:, :, HEAD_DIM:]], axis=1)
            heads_ref[:, head * HEAD_DIM : (head + 1) * HEAD_DIM] = rows.reshape(tokens, HEAD_DIM)
        projected = jnp.dot(heads_ref[...], weight_ref[...], preferred_element_type=jnp.float32)
        mixed = (residual_ref[...].astype(jnp.float32) + projected).astype(jnp.bfloat16)
        mixed_ref[...] = mixed
        mixed = mixed.astype(jnp.float32)
        inverse = lax.rsqrt(jnp.mean(mixed * mixed, axis=1, keepdims=True) + norm_eps)
        normed_ref[...] = (mixed * inverse * gain_ref[...]).astype(jnp.bfloat16)

    left, right = normed_ref[:, :half], normed_ref[:, half:]
    first = pl.program_id(0) * count

    def chosen(slots, lowest):
        rank = jnp.dot(
            expand(count, slots, experts, first), rank_ref[...], preferred_element_type=jnp.float32
        )
        slot = lowest + lax.broadcasted_iota(jnp.int32, rank.shape, 0) % (slots if lowest == 0 else TAIL)
        return (rank == slot.astype(jnp.float32)).astype(jnp.bfloat16)

    def pick(rows, side):
        return jnp.dot(rows, side, preferred_element_type=jnp.float32)

    main, tail = chosen(MAIN, 0), chosen(2 * TAIL, MAIN)
    out_ref[:, 0:MAIN, :] = pick(main, left).astype(jnp.bfloat16).reshape(count, MAIN, half)
    out_ref[:, MAIN : 2 * MAIN, :] = pick(main, right).astype(jnp.bfloat16).reshape(count, MAIN, half)
    early = lax.broadcasted_iota(jnp.int32, (tail.shape[0], half), 0) % (2 * TAIL) < TAIL
    both = jnp.where(early, pick(tail, left), pick(tail, right))
    out_ref[:, 2 * MAIN :, :] = both.astype(jnp.bfloat16).reshape(count, 2 * TAIL, half)


def dispatch(attended, residual, out_weight, gain, ranks, experts):
    tokens, width = residual.shape
    step = 32
    whole = lambda i: (0, 0)
    return pl.pallas_call(
        dispatch_kernel,
        grid=(experts // step,),
        in_specs=[
            pl.BlockSpec(attended.shape, lambda i: (0, 0, 0)),
            pl.BlockSpec(residual.shape, whole),
            pl.BlockSpec(out_weight.shape, whole),
            pl.BlockSpec(gain.shape, whole),
            pl.BlockSpec((experts, tokens), whole),
        ],
        out_specs=[
            pl.BlockSpec((tokens, width), whole),
            pl.BlockSpec((tokens, width), whole),
            pl.BlockSpec((step, 2 * (MAIN + TAIL), width // 2), lambda i: (i, 0, 0)),
        ],
        out_shape=[
            jax.ShapeDtypeStruct((tokens, width), jnp.bfloat16),
            jax.ShapeDtypeStruct((tokens, width), jnp.bfloat16),
            jax.ShapeDtypeStruct((experts, 2 * (MAIN + TAIL), width // 2), jnp.bfloat16),
        ],
        scratch_shapes=[pltpu.VMEM((tokens, 8 * HEAD_DIM), jnp.bfloat16)],
        compiler_params=pltpu.CompilerParams(vmem_limit_bytes=32 * 2**20),
        cost_estimate=pl.CostEstimate(flops=10**9, bytes_accessed=10**7, transcendentals=0),
        name="dispatch",
    )(attended, residual, out_weight, gain, ranks)


PASS = 16


def expert_kernel(
    rows_ref,
    gate0_ref,
    up0_ref,
    gate1_ref,
    up1_ref,
    down0_ref,
    down1_ref,
    shared_gate_ref,
    shared_up_ref,
    shared_down_ref,
    mixed_ref,
    normed_ref,
    out_ref,
    base_ref,
    spread_ref,
    rows2_ref,
):
    total, _, half = rows_ref.shape
    tails, mains = PASS * TAIL, PASS * MAIN
    row = lax.broadcasted_iota(jnp.int32, (2 * tails, 2 * tails), 0)
    col = lax.broadcasted_iota(jnp.int32, (2 * tails, 2 * tails), 1)
    slot = row % tails
    home = slot // TAIL * (2 * TAIL) + row // tails * TAIL + slot % TAIL
    spread_ref[...] = (home == col).astype(jnp.bfloat16)

    def hidden(rows, gate_matrix, up_matrix):
        gate = jnp.dot(rows, gate_matrix, preferred_element_type=jnp.float32)
        upward = jnp.dot(rows, up_matrix, preferred_element_type=jnp.float32)
        return (jax.nn.silu(gate) * upward).astype(jnp.bfloat16)

    @pl.loop(0, total // PASS)
    def _(turn):
        part = pl.ds(turn * PASS, PASS)
        spread = spread_ref[...]
        rows2_ref[:mains, :half] = rows_ref[part, 0:MAIN, :].reshape(mains, half)
        rows2_ref[:mains, half:] = rows_ref[part, MAIN : 2 * MAIN, :].reshape(mains, half)
        ends = jnp.dot(
            spread, rows_ref[part, 2 * MAIN :, :].reshape(2 * tails, half), preferred_element_type=jnp.float32
        ).astype(jnp.bfloat16)
        rows2_ref[mains:, :half] = ends[:tails]
        rows2_ref[mains:, half:] = ends[tails:]
        act0 = hidden(rows2_ref[...], gate0_ref[0], up0_ref[0])
        act1 = hidden(rows2_ref[...], gate1_ref[0], up1_ref[0])
        ends = []
        for side in range(2):
            span = slice(side * half, (side + 1) * half)
            result = jnp.dot(act0, down0_ref[0, :, span], preferred_element_type=jnp.float32) + jnp.dot(
                act1, down1_ref[0, :, span], preferred_element_type=jnp.float32
            )
            result = result.astype(jnp.bfloat16)
            out_ref[part, side * MAIN : (side + 1) * MAIN, :] = result[:mains].reshape(PASS, MAIN, half)
            ends.append(result[mains:])
        ends = lax.dot_general(
            spread, jnp.concatenate(ends, axis=0), (((0,), (0,)), ((), ())), preferred_element_type=jnp.float32
        )
        out_ref[part, 2 * MAIN :, :] = ends.astype(jnp.bfloat16).reshape(PASS, 2 * TAIL, half)

    act = hidden(normed_ref[...], shared_gate_ref[...], shared_up_ref[...])
    base_ref[...] = mixed_ref[...].astype(jnp.float32) + jnp.dot(
        act, shared_down_ref[...], preferred_element_type=jnp.float32
    )


def expert(rows, weights, mixed, normed):
    return pl.pallas_call(
        expert_kernel,
        in_specs=[pl.BlockSpec(memory_space=pltpu.VMEM)] * (3 + len(weights)),
        out_specs=[pl.BlockSpec(memory_space=pltpu.VMEM)] * 2,
        out_shape=[
            jax.ShapeDtypeStruct(rows.shape, jnp.bfloat16),
            jax.ShapeDtypeStruct(mixed.shape, jnp.float32),
        ],
        scratch_shapes=[
            pltpu.VMEM((PASS * 2 * TAIL, PASS * 2 * TAIL), jnp.bfloat16),
            pltpu.VMEM((PASS * (MAIN + TAIL), 2 * rows.shape[2]), jnp.bfloat16),
        ],
        compiler_params=pltpu.CompilerParams(vmem_limit_bytes=24 * 2**20),
        cost_estimate=pl.CostEstimate(flops=8 * 10**9, bytes_accessed=17 * 10**6, transcendentals=10**6),
        name="expert",
    )(rows, *weights, mixed, normed)


HALF = 32


def combine_kernel(rows_ref, ranks_ref, base_ref, out_ref, acc_ref):
    total, _, half = rows_ref.shape
    tokens = base_ref.shape[0]
    experts = ranks_ref.shape[0] // 3
    acc_ref[...] = base_ref[...]

    @pl.loop(0, total // HALF)
    def _(turn):
        def weights(slots, wanted):
            chosen = expand(HALF, slots, experts, turn * HALF)
            rank, high, low = [
                jnp.dot(chosen, ranks_ref[i * experts : (i + 1) * experts], preferred_element_type=jnp.float32)
                for i in range(3)
            ]
            slot = wanted(lax.broadcasted_iota(jnp.int32, rank.shape, 0) % slots).astype(jnp.float32)
            here = rank == slot
            parts = [jnp.where(here, part, 0.0) for part in (high, low)]
            return jnp.concatenate(parts, axis=1).T.astype(jnp.bfloat16)

        part = pl.ds(turn * HALF, HALF)
        main = weights(MAIN, lambda slot: slot)
        ends = rows_ref[part, 2 * MAIN :, :].reshape(HALF * 2 * TAIL, half)
        for side in range(2):
            tail = weights(2 * TAIL, lambda slot: jnp.where(slot // TAIL == side, MAIN + slot % TAIL, -2))
            rows = rows_ref[part, side * MAIN : (side + 1) * MAIN, :].reshape(HALF * MAIN, half)
            sums = jnp.dot(main, rows, preferred_element_type=jnp.float32) + jnp.dot(
                tail, ends, preferred_element_type=jnp.float32
            )
            span = pl.ds(side * half, half)
            acc_ref[:, span] += sums[:tokens] + sums[tokens:]

    out_ref[...] = acc_ref[...].astype(jnp.bfloat16)


def combine(rows, ranks, base):
    return pl.pallas_call(
        combine_kernel,
        in_specs=[pl.BlockSpec(memory_space=pltpu.VMEM)] * 3,
        out_specs=pl.BlockSpec(memory_space=pltpu.VMEM),
        out_shape=jax.ShapeDtypeStruct(base.shape, jnp.bfloat16),
        scratch_shapes=[pltpu.VMEM(base.shape, jnp.float32)],
        compiler_params=pltpu.CompilerParams(vmem_limit_bytes=24 * 2**20),
        cost_estimate=pl.CostEstimate(flops=10**9, bytes_accessed=10**7, transcendentals=0),
        name="combine",
    )(rows, ranks, base)


def local(
    queries,
    key_rows,
    value_rows,
    residual,
    out_weight,
    norm_gain,
    routes,
    route_weight,
    expert_gate,
    expert_up,
    expert_down,
    shared_gate,
    shared_up,
    shared_down,
):
    core = lax.axis_index("tp")
    offset = 128 * core + 16 * (lax.axis_index("sp") % 8)
    swap = [(0, 1), (1, 0)]
    cores = core[None].astype(jnp.int32)
    keep, send = pack(cores, queries, key_rows, value_rows)
    taken = lax.ppermute(send, "tp", swap)
    mine = lax.all_to_all(spread(cores, keep, taken), "sp", 0, 0, tiled=True)
    peer = lax.ppermute(mine, "tp", swap)
    mine, routes, route_weight = lax.optimization_barrier((mine, routes, route_weight))
    ranks = route(routes.T, route_weight.T, 64)
    peer, ranks, expert_gate_, expert_up_, expert_down_ = lax.optimization_barrier(
        (peer, ranks, expert_gate, expert_up, expert_down)
    )
    attended = attention(jnp.stack([core, offset]).astype(jnp.int32), mine, peer)
    gate_other = lax.ppermute(expert_gate_, "tp", swap)
    up_other = lax.ppermute(expert_up_, "tp", swap)
    down_other = lax.ppermute(expert_down_, "tp", swap)
    attended, gate_other, up_other, down_other = lax.optimization_barrier(
        (attended, gate_other, up_other, down_other)
    )
    attended = lax.all_to_all(attended, "sp", 0, 0, tiled=True)
    experts = lax.axis_size("sp")
    mixed, normed, outgoing = dispatch(
        attended, residual, out_weight, norm_gain[None, :], ranks, experts
    )
    incoming = lax.all_to_all(outgoing, "sp", 0, 0, tiled=True)
    result, base = expert(
        incoming,
        (
            expert_gate,
            expert_up,
            gate_other,
            up_other,
            expert_down,
            down_other,
            shared_gate,
            shared_up,
            shared_down,
        ),
        mixed,
        normed,
    )
    returned = lax.all_to_all(result, "sp", 0, 0, tiled=True)
    return combine(returned, ranks, base)


def solution(mesh):
    return jax.shard_map(
        local,
        mesh=mesh,
        in_specs=(
            P("sp", "tp"),
            P("sp", "tp"),
            P("sp", "tp"),
            P(("sp", "tp"), None),
            P(),
            P(),
            P(("sp", "tp"), None),
            P(("sp", "tp"), None),
            P("sp", None, "tp"),
            P("sp", None, "tp"),
            P("sp", "tp", None),
            P(),
            P(),
            P(),
        ),
        out_specs=P(("sp", "tp"), None),
        check_vma=False,
    )
```

```python
import jax
import jax.numpy as jnp
from jax import lax
from jax.experimental import pallas as pl
from jax.experimental.pallas import tpu as pltpu
from jax.sharding import PartitionSpec as P

HEAD_DIM = 64
LANES = 128
TOPK = 8
LOG2E = 1.4426950408889634
norm_eps = 1e-06


VMEM_BYTES = 67043328


def pack_kernel(core_ref, query_ref, key_ref, value_ref, keep_out, send_out):
    heads, rows = keep_out.shape[0], query_ref.shape[0] // 2
    core = core_ref[0]
    for out, half in ((keep_out, core), (send_out, 1 - core)):
        own = pl.ds(half * rows, rows)
        for head in range(heads):
            span = slice(head * HEAD_DIM, (head + 1) * HEAD_DIM)
            out[head, :rows] = jnp.concatenate([key_ref[own, span], value_ref[own, span]], axis=1)
            query = query_ref[own, span].reshape(rows // 16, 16, HEAD_DIM)
            query = jnp.concatenate([query[:, :8], query[:, 8:]], axis=2)
            out[head, rows:] = query.reshape(rows // 2, LANES)


def pack(core, queries, key_rows, value_rows):
    side, width = key_rows.shape
    half = jax.ShapeDtypeStruct((width // HEAD_DIM, side // 2 + side // 4, LANES), jnp.bfloat16)
    return pl.pallas_call(
        pack_kernel,
        in_specs=[pl.BlockSpec(memory_space=pltpu.SMEM)] + [pl.BlockSpec(memory_space=pltpu.VMEM)] * 3,
        out_specs=[pl.BlockSpec(memory_space=pltpu.VMEM)] * 2,
        out_shape=[half, half],
        compiler_params=pltpu.CompilerParams(vmem_limit_bytes=8 * 2**20),
        name="pack",
    )(core, queries, key_rows, value_rows)


def spread_kernel(core_ref, keep_ref, taken_ref, out_ref):
    chips, depth, _ = out_ref.shape
    rows = depth - 8
    for head in range(chips // 8):
        mine = head // 4 == core_ref[0]
        held = jnp.where(mine, keep_ref[head % 4], taken_ref[head % 4])
        for chip in range(8):
            out_ref[8 * head + chip, :rows] = held[:rows]
            out_ref[8 * head + chip, rows:] = held[rows + 8 * chip : rows + 8 * chip + 8]


def spread(core, keep, taken):
    shape = (64, keep.shape[1] * 2 // 3 + 8, LANES)
    return pl.pallas_call(
        spread_kernel,
        in_specs=[pl.BlockSpec(memory_space=pltpu.SMEM)] + [pl.BlockSpec(memory_space=pltpu.VMEM)] * 2,
        out_specs=pl.BlockSpec(memory_space=pltpu.VMEM),
        out_shape=jax.ShapeDtypeStruct(shape, jnp.bfloat16),
        compiler_params=pltpu.CompilerParams(vmem_limit_bytes=16 * 2**20),
        name="spread",
    )(core, keep, taken)


def route_kernel(routes_ref, weight_ref, out_ref):
    tokens, experts = routes_ref.shape[1], out_ref.shape[0] // 3
    names = lax.broadcasted_iota(jnp.int32, (experts, tokens), 0)
    pick = jnp.zeros((experts, tokens), jnp.float32)
    share = jnp.zeros((experts, tokens), jnp.float32)
    for k in range(TOPK):
        named = routes_ref[k : k + 1, :] == names
        pick = jnp.where(named, 1.0, pick)
        share = jnp.where(named, weight_ref[k : k + 1, :], share)
    row = lax.broadcasted_iota(jnp.int32, (tokens, tokens), 0)
    col = lax.broadcasted_iota(jnp.int32, (tokens, tokens), 1)
    above = (row < col).astype(jnp.bfloat16)
    rank = jnp.dot(pick.astype(jnp.bfloat16), above, preferred_element_type=jnp.float32)
    out_ref[0:experts] = jnp.where(pick > 0.0, rank, -1.0).astype(jnp.bfloat16)
    high = share.astype(jnp.bfloat16)
    out_ref[experts : 2 * experts] = high
    out_ref[2 * experts :] = (share - high.astype(jnp.float32)).astype(jnp.bfloat16)


def route(routes, route_weight, experts):
    return pl.pallas_call(
        route_kernel,
        out_shape=jax.ShapeDtypeStruct((3 * experts, routes.shape[1]), jnp.bfloat16),
        in_specs=[pl.BlockSpec(memory_space=pltpu.VMEM)] * 2,
        out_specs=pl.BlockSpec(memory_space=pltpu.VMEM),
        name="route",
    )(routes, route_weight)


GROUP = 2
FULL = 8


def attention_kernel(meta_ref, mine_ref, peer, out_ref, kv_ref, tri_ref, query_ref, acc_ref, sems):
    core, offset = meta_ref[0], meta_ref[1]
    side = tri_ref.shape[0]
    rows = side // 2
    first_rows = pl.ds(pl.multiple_of(core * rows, rows), rows)
    other_rows = pl.ds(pl.multiple_of((1 - core) * rows, rows), rows)
    span = kv_ref.shape[0] // 4
    loads = []
    for piece in range(4):
        chips = pl.ds(piece * span, span)
        loads.append(
            pltpu.make_async_copy(peer.at[chips, pl.ds(0, rows)], kv_ref.at[chips, other_rows], sems.at[piece])
        )
        loads[-1].start()
    row = lax.broadcasted_iota(jnp.int32, (side, side), 0)
    col = lax.broadcasted_iota(jnp.int32, (side, side), 1)
    tri_ref[...] = (row > col).astype(jnp.float32)
    raw = mine_ref[:, rows:]
    none = jnp.zeros(raw.shape[:2] + (HEAD_DIM,), jnp.bfloat16)
    early = jnp.concatenate([raw[:, :, :HEAD_DIM], none], axis=2)
    late = jnp.concatenate([raw[:, :, HEAD_DIM:], none], axis=2)
    query_ref[...] = jnp.concatenate([early, late], axis=1).reshape(query_ref.shape)

    @pl.loop(0, kv_ref.shape[0] // 4)
    def _(turn):
        for i in range(4):
            kv_ref[4 * turn + i, first_rows] = mine_ref[4 * turn + i, :rows]

    for load in loads:
        load.wait()

    tiles, depth = query_ref.shape[:2]
    blocks = depth // 16

    def advance(jobs, skip, diagonal, count):
        chains = [(tile, first + i, i) for tile, first in jobs for i in range(count)]
        queries = {tile: query_ref[tile, skip:] for tile, _ in jobs}
        keys = [kv_ref[block] for _, block, _ in chains]
        scores = [
            lax.dot_general(
                queries[tile], kv, (((1,), (1,)), ((), ())), preferred_element_type=jnp.float32
            )
            * (HEAD_DIM**-0.5 * LOG2E)
            for (tile, _, _), kv in zip(chains, keys)
        ]
        costs = [jnp.maximum(s, jnp.log2(1.0 + jnp.exp2(jnp.minimum(s, 126.0)))) for s in scores]
        slacks = [s - c for s, c in zip(scores, costs)]
        if diagonal:
            edge = 16 * count
            shape = (edge, side)
            place = lax.broadcasted_iota(jnp.int32, shape, 0)
            place = place // 16 * side + place % 16 + offset - lax.broadcasted_iota(jnp.int32, shape, 1)
            live = [place > i * side for i in range(count)]

            def masked(i, value):
                top = jnp.where(live[i], value[:edge], 0.0)
                return top if value.shape[0] == edge else jnp.concatenate([top, value[edge:]], axis=0)

            costs = [masked(i, c) for (_, _, i), c in zip(chains, costs)]
        tri = tri_ref[...]
        insides = [jnp.dot(c, tri, preferred_element_type=jnp.float32) for c in costs]
        accs = {tile: acc_ref[tile, skip:] for tile, _ in jobs}
        for (tile, _, i), kv, cost, slack, inside in zip(chains, keys, costs, slacks, insides):
            weight = jnp.exp2(slack - inside)
            if diagonal:
                weight = masked(i, weight)
            part = jnp.dot(weight.astype(jnp.bfloat16), kv, preferred_element_type=jnp.float32)
            accs[tile] = accs[tile] * jnp.exp2(-jnp.sum(cost, axis=1, keepdims=True)) + part
        for tile, acc in accs.items():
            acc_ref[tile, skip:] = acc

    acc_ref[...] = jnp.zeros_like(acc_ref)

    @pl.loop(0, blocks // FULL)
    def _(step):
        advance([(1, step * FULL)], 0, False, FULL)

    for step in range(blocks // GROUP):
        advance([(tile, blocks * tile + step * GROUP) for tile in range(tiles)], step * GROUP * 16, True, GROUP)
    done = acc_ref[:, :, HEAD_DIM:].reshape(tiles * blocks, 16, HEAD_DIM)
    out_ref[...] = jnp.concatenate([done[:, :8], done[:, 8:]], axis=2).astype(jnp.bfloat16)


def attention(meta, mine, peer):
    chips, depth, _ = mine.shape
    side = 2 * (depth - 8)
    pairs = 136 * side * side
    return pl.pallas_call(
        attention_kernel,
        out_shape=jax.ShapeDtypeStruct((chips, 8, LANES), jnp.bfloat16),
        in_specs=[
            pl.BlockSpec(memory_space=pltpu.SMEM),
            pl.BlockSpec(memory_space=pltpu.VMEM),
            pl.BlockSpec(memory_space=pl.ANY),
        ],
        out_specs=pl.BlockSpec(memory_space=pltpu.VMEM),
        scratch_shapes=[
            pltpu.VMEM((chips, side, LANES), jnp.bfloat16),
            pltpu.VMEM((side, side), jnp.float32),
            pltpu.VMEM((2, 2 * side, LANES), jnp.bfloat16),
            pltpu.VMEM((2, 2 * side, LANES), jnp.float32),
            pltpu.SemaphoreType.DMA((4,)),
        ],
        compiler_params=pltpu.CompilerParams(vmem_limit_bytes=40 * 2**20),
        cost_estimate=pl.CostEstimate(
            flops=pairs * 2 * 768, bytes_accessed=6 * 2**20, transcendentals=pairs * 3
        ),
        name="attend",
    )(meta, mine, peer)


MAIN = 16
TAIL = 4


def expand(count, slots, experts, first):
    row = lax.broadcasted_iota(jnp.int32, (count * slots, experts), 0)
    col = lax.broadcasted_iota(jnp.int32, (count * slots, experts), 1)
    return (col == first + row // slots).astype(jnp.bfloat16)


STEP = 16


def copy_group(source, target, sems, start, count, parts):
    each = count // parts
    return [
        pltpu.make_async_copy(
            source.at[pl.ds(start + i * each, each)],
            target.at[pl.ds(start + i * each, each)],
            sems.at[start // each + i],
        )
        for i in range(parts)
    ]


def dispatch_kernel(
    attended_ref,
    residual_ref,
    weight_ref,
    gain_ref,
    rank_ref,
    mixed_ref,
    normed_ref,
    out_ref,
    heads_ref,
):
    count, _, half = out_ref.shape
    experts, tokens = rank_ref.shape

    @pl.when(pl.program_id(0) == 0)
    def _():
        for head in range(8):
            rows = attended_ref[8 * head : 8 * head + 8]
            rows = jnp.concatenate([rows[:, :, :HEAD_DIM], rows[:, :, HEAD_DIM:]], axis=1)
            heads_ref[:, head * HEAD_DIM : (head + 1) * HEAD_DIM] = rows.reshape(tokens, HEAD_DIM)
        projected = jnp.dot(heads_ref[...], weight_ref[...], preferred_element_type=jnp.float32)
        mixed = (residual_ref[...].astype(jnp.float32) + projected).astype(jnp.bfloat16)
        mixed_ref[...] = mixed
        mixed = mixed.astype(jnp.float32)
        inverse = lax.rsqrt(jnp.mean(mixed * mixed, axis=1, keepdims=True) + norm_eps)
        normed_ref[...] = (mixed * inverse * gain_ref[...]).astype(jnp.bfloat16)

    left, right = normed_ref[:, :half], normed_ref[:, half:]
    first = pl.program_id(0) * count

    def chosen(slots, lowest):
        rank = jnp.dot(
            expand(count, slots, experts, first), rank_ref[...], preferred_element_type=jnp.float32
        )
        slot = lowest + lax.broadcasted_iota(jnp.int32, rank.shape, 0) % (slots if lowest == 0 else TAIL)
        return (rank == slot.astype(jnp.float32)).astype(jnp.bfloat16)

    def pick(rows, side):
        return jnp.dot(rows, side, preferred_element_type=jnp.float32)

    main, tail = chosen(MAIN, 0), chosen(2 * TAIL, MAIN)
    out_ref[:, 0:MAIN, :] = pick(main, left).astype(jnp.bfloat16).reshape(count, MAIN, half)
    out_ref[:, MAIN : 2 * MAIN, :] = pick(main, right).astype(jnp.bfloat16).reshape(count, MAIN, half)
    early = lax.broadcasted_iota(jnp.int32, (tail.shape[0], half), 0) % (2 * TAIL) < TAIL
    both = jnp.where(early, pick(tail, left), pick(tail, right))
    out_ref[:, 2 * MAIN :, :] = both.astype(jnp.bfloat16).reshape(count, 2 * TAIL, half)


def dispatch(attended, residual, out_weight, gain, ranks, experts):
    tokens, width = residual.shape
    step = 32
    whole = lambda i: (0, 0)
    return pl.pallas_call(
        dispatch_kernel,
        grid=(experts // step,),
        in_specs=[
            pl.BlockSpec(attended.shape, lambda i: (0, 0, 0)),
            pl.BlockSpec(residual.shape, whole),
            pl.BlockSpec(out_weight.shape, whole),
            pl.BlockSpec(gain.shape, whole),
            pl.BlockSpec((experts, tokens), whole),
        ],
        out_specs=[
            pl.BlockSpec((tokens, width), whole),
            pl.BlockSpec((tokens, width), whole),
            pl.BlockSpec((step, 2 * (MAIN + TAIL), width // 2), lambda i: (i, 0, 0)),
        ],
        out_shape=[
            jax.ShapeDtypeStruct((tokens, width), jnp.bfloat16),
            jax.ShapeDtypeStruct((tokens, width), jnp.bfloat16),
            jax.ShapeDtypeStruct((experts, 2 * (MAIN + TAIL), width // 2), jnp.bfloat16),
        ],
        scratch_shapes=[pltpu.VMEM((tokens, 8 * HEAD_DIM), jnp.bfloat16)],
        compiler_params=pltpu.CompilerParams(vmem_limit_bytes=32 * 2**20),
        cost_estimate=pl.CostEstimate(flops=10**9, bytes_accessed=10**7, transcendentals=0),
        name="dispatch",
    )(attended, residual, out_weight, gain, ranks)


PASS = 32


def expert_kernel(
    rows_ref,
    gate0_ref,
    up0_ref,
    gate1_ref,
    up1_ref,
    down0_ref,
    down1_ref,
    shared_gate_ref,
    shared_up_ref,
    shared_down_ref,
    mixed_ref,
    normed_ref,
    out_ref,
    base_ref,
    spread_ref,
    rows2_ref,
):
    total, _, half = rows_ref.shape
    tails, mains = PASS * TAIL, PASS * MAIN
    row = lax.broadcasted_iota(jnp.int32, (2 * tails, 2 * tails), 0)
    col = lax.broadcasted_iota(jnp.int32, (2 * tails, 2 * tails), 1)
    slot = row % tails
    home = slot // TAIL * (2 * TAIL) + row // tails * TAIL + slot % TAIL
    spread_ref[...] = (home == col).astype(jnp.bfloat16)

    def hidden(rows, gate_matrix, up_matrix):
        gate = jnp.dot(rows, gate_matrix, preferred_element_type=jnp.float32)
        upward = jnp.dot(rows, up_matrix, preferred_element_type=jnp.float32)
        return (jax.nn.silu(gate) * upward).astype(jnp.bfloat16)

    @pl.loop(0, total // PASS)
    def _(turn):
        part = pl.ds(turn * PASS, PASS)
        spread = spread_ref[...]
        rows2_ref[:mains, :half] = rows_ref[part, 0:MAIN, :].reshape(mains, half)
        rows2_ref[:mains, half:] = rows_ref[part, MAIN : 2 * MAIN, :].reshape(mains, half)
        ends = jnp.dot(
            spread, rows_ref[part, 2 * MAIN :, :].reshape(2 * tails, half), preferred_element_type=jnp.float32
        ).astype(jnp.bfloat16)
        rows2_ref[mains:, :half] = ends[:tails]
        rows2_ref[mains:, half:] = ends[tails:]
        act0 = hidden(rows2_ref[...], gate0_ref[0], up0_ref[0])
        act1 = hidden(rows2_ref[...], gate1_ref[0], up1_ref[0])
        ends = []
        for side in range(2):
            span = slice(side * half, (side + 1) * half)
            result = jnp.dot(act0, down0_ref[0, :, span], preferred_element_type=jnp.float32) + jnp.dot(
                act1, down1_ref[0, :, span], preferred_element_type=jnp.float32
            )
            result = result.astype(jnp.bfloat16)
            out_ref[part, side * MAIN : (side + 1) * MAIN, :] = result[:mains].reshape(PASS, MAIN, half)
            ends.append(result[mains:])
        ends = lax.dot_general(
            spread, jnp.concatenate(ends, axis=0), (((0,), (0,)), ((), ())), preferred_element_type=jnp.float32
        )
        out_ref[part, 2 * MAIN :, :] = ends.astype(jnp.bfloat16).reshape(PASS, 2 * TAIL, half)

    act = hidden(normed_ref[...], shared_gate_ref[...], shared_up_ref[...])
    base_ref[...] = mixed_ref[...].astype(jnp.float32) + jnp.dot(
        act, shared_down_ref[...], preferred_element_type=jnp.float32
    )


def expert(rows, weights, mixed, normed):
    return pl.pallas_call(
        expert_kernel,
        in_specs=[pl.BlockSpec(memory_space=pltpu.VMEM)] * (3 + len(weights)),
        out_specs=[pl.BlockSpec(memory_space=pltpu.VMEM)] * 2,
        out_shape=[
            jax.ShapeDtypeStruct(rows.shape, jnp.bfloat16),
            jax.ShapeDtypeStruct(mixed.shape, jnp.float32),
        ],
        scratch_shapes=[
            pltpu.VMEM((PASS * 2 * TAIL, PASS * 2 * TAIL), jnp.bfloat16),
            pltpu.VMEM((PASS * (MAIN + TAIL), 2 * rows.shape[2]), jnp.bfloat16),
        ],
        compiler_params=pltpu.CompilerParams(vmem_limit_bytes=24 * 2**20),
        cost_estimate=pl.CostEstimate(flops=8 * 10**9, bytes_accessed=17 * 10**6, transcendentals=10**6),
        name="expert",
    )(rows, *weights, mixed, normed)


HALF = 64


def combine_kernel(rows_ref, ranks_ref, base_ref, out_ref, acc_ref):
    total, _, half = rows_ref.shape
    tokens = base_ref.shape[0]
    experts = ranks_ref.shape[0] // 3
    acc_ref[...] = base_ref[...]

    @pl.loop(0, total // HALF)
    def _(turn):
        def weights(slots, wanted):
            chosen = expand(HALF, slots, experts, turn * HALF)
            rank, high, low = [
                jnp.dot(chosen, ranks_ref[i * experts : (i + 1) * experts], preferred_element_type=jnp.float32)
                for i in range(3)
            ]
            slot = wanted(lax.broadcasted_iota(jnp.int32, rank.shape, 0) % slots).astype(jnp.float32)
            here = rank == slot
            parts = [jnp.where(here, part, 0.0) for part in (high, low)]
            return jnp.concatenate(parts, axis=1).T.astype(jnp.bfloat16)

        part = pl.ds(turn * HALF, HALF)
        main = weights(MAIN, lambda slot: slot)
        ends = rows_ref[part, 2 * MAIN :, :].reshape(HALF * 2 * TAIL, half)
        for side in range(2):
            tail = weights(2 * TAIL, lambda slot: jnp.where(slot // TAIL == side, MAIN + slot % TAIL, -2))
            rows = rows_ref[part, side * MAIN : (side + 1) * MAIN, :].reshape(HALF * MAIN, half)
            sums = jnp.dot(main, rows, preferred_element_type=jnp.float32) + jnp.dot(
                tail, ends, preferred_element_type=jnp.float32
            )
            span = pl.ds(side * half, half)
            acc_ref[:, span] += sums[:tokens] + sums[tokens:]

    out_ref[...] = acc_ref[...].astype(jnp.bfloat16)


def combine(rows, ranks, base):
    return pl.pallas_call(
        combine_kernel,
        in_specs=[pl.BlockSpec(memory_space=pltpu.VMEM)] * 3,
        out_specs=pl.BlockSpec(memory_space=pltpu.VMEM),
        out_shape=jax.ShapeDtypeStruct(base.shape, jnp.bfloat16),
        scratch_shapes=[pltpu.VMEM(base.shape, jnp.float32)],
        compiler_params=pltpu.CompilerParams(vmem_limit_bytes=24 * 2**20),
        cost_estimate=pl.CostEstimate(flops=10**9, bytes_accessed=10**7, transcendentals=0),
        name="combine",
    )(rows, ranks, base)


def local(
    queries,
    key_rows,
    value_rows,
    residual,
    out_weight,
    norm_gain,
    routes,
    route_weight,
    expert_gate,
    expert_up,
    expert_down,
    shared_gate,
    shared_up,
    shared_down,
):
    core = lax.axis_index("tp")
    offset = 128 * core + 16 * (lax.axis_index("sp") % 8)
    swap = [(0, 1), (1, 0)]
    cores = core[None].astype(jnp.int32)
    keep, send = pack(cores, queries, key_rows, value_rows)
    taken = lax.ppermute(send, "tp", swap)
    mine = lax.all_to_all(spread(cores, keep, taken), "sp", 0, 0, tiled=True)
    peer = lax.ppermute(mine, "tp", swap)
    mine, routes, route_weight = lax.optimization_barrier((mine, routes, route_weight))
    ranks = route(routes.T, route_weight.T, 64)
    peer, ranks, expert_gate_, expert_up_, expert_down_ = lax.optimization_barrier(
        (peer, ranks, expert_gate, expert_up, expert_down)
    )
    attended = attention(jnp.stack([core, offset]).astype(jnp.int32), mine, peer)
    gate_other = lax.ppermute(expert_gate_, "tp", swap)
    up_other = lax.ppermute(expert_up_, "tp", swap)
    down_other = lax.ppermute(expert_down_, "tp", swap)
    attended, gate_other, up_other, down_other = lax.optimization_barrier(
        (attended, gate_other, up_other, down_other)
    )
    attended = lax.all_to_all(attended, "sp", 0, 0, tiled=True)
    experts = lax.axis_size("sp")
    mixed, normed, outgoing = dispatch(
        attended, residual, out_weight, norm_gain[None, :], ranks, experts
    )
    incoming = lax.all_to_all(outgoing, "sp", 0, 0, tiled=True)
    result, base = expert(
        incoming,
        (
            expert_gate,
            expert_up,
            gate_other,
            up_other,
            expert_down,
            down_other,
            shared_gate,
            shared_up,
            shared_down,
        ),
        mixed,
        normed,
    )
    returned = lax.all_to_all(result, "sp", 0, 0, tiled=True)
    return combine(returned, ranks, base)


def solution(mesh):
    return jax.shard_map(
        local,
        mesh=mesh,
        in_specs=(
            P("sp", "tp"),
            P("sp", "tp"),
            P("sp", "tp"),
            P(("sp", "tp"), None),
            P(),
            P(),
            P(("sp", "tp"), None),
            P(("sp", "tp"), None),
            P("sp", None, "tp"),
            P("sp", None, "tp"),
            P("sp", "tp", None),
            P(),
            P(),
            P(),
        ),
        out_specs=P(("sp", "tp"), None),
        check_vma=False,
    )
```

```python
import jax
import jax.numpy as jnp
from jax import lax
from jax.experimental import pallas as pl
from jax.experimental.pallas import tpu as pltpu
from jax.sharding import PartitionSpec as P

HEAD_DIM = 64
LANES = 128
TOPK = 8
LOG2E = 1.4426950408889634
norm_eps = 1e-06


VMEM_BYTES = 67043328


def pack_kernel(core_ref, rows_ref, keep_out, send_out):
    heads, rows = keep_out.shape[0], rows_ref.shape[1] // 2
    core = core_ref[0]
    for out, half in ((send_out, 1 - core), (keep_out, core)):
        own = pl.ds(half * rows, rows)
        for head in range(heads):
            span = slice(head * HEAD_DIM, (head + 1) * HEAD_DIM)
            out[head, :rows] = jnp.concatenate([rows_ref[1, own, span], rows_ref[2, own, span]], axis=1)
            query = rows_ref[0, own, span].reshape(rows // 16, 16, HEAD_DIM)
            query = jnp.concatenate([query[:, :8], query[:, 8:]], axis=2)
            out[head, rows:] = query.reshape(rows // 2, LANES)


def pack(core, queries, key_rows, value_rows):
    side, width = key_rows.shape
    half = jax.ShapeDtypeStruct((width // HEAD_DIM, side // 2 + side // 4, LANES), jnp.bfloat16)
    return pl.pallas_call(
        pack_kernel,
        in_specs=[pl.BlockSpec(memory_space=pltpu.SMEM), pl.BlockSpec(memory_space=pltpu.VMEM)],
        out_specs=[pl.BlockSpec(memory_space=pltpu.VMEM)] * 2,
        out_shape=[half, half],
        compiler_params=pltpu.CompilerParams(vmem_limit_bytes=8 * 2**20),
        name="pack",
    )(core, jnp.stack([queries, key_rows, value_rows]))


def spread_kernel(core_ref, keep_ref, taken_ref, out_ref):
    chips, depth, _ = out_ref.shape
    rows = depth - 8
    for head in range(chips // 8):
        mine = head // 4 == core_ref[0]
        held = jnp.where(mine, keep_ref[head % 4], taken_ref[head % 4])
        for chip in range(8):
            out_ref[8 * head + chip, :rows] = held[:rows]
            out_ref[8 * head + chip, rows:] = held[rows + 8 * chip : rows + 8 * chip + 8]


def spread(core, keep, taken):
    shape = (64, keep.shape[1] * 2 // 3 + 8, LANES)
    return pl.pallas_call(
        spread_kernel,
        in_specs=[pl.BlockSpec(memory_space=pltpu.SMEM)] + [pl.BlockSpec(memory_space=pltpu.VMEM)] * 2,
        out_specs=pl.BlockSpec(memory_space=pltpu.VMEM),
        out_shape=jax.ShapeDtypeStruct(shape, jnp.bfloat16),
        compiler_params=pltpu.CompilerParams(vmem_limit_bytes=16 * 2**20),
        name="spread",
    )(core, keep, taken)


def route_kernel(routes_ref, weight_ref, out_ref):
    tokens, experts = routes_ref.shape[1], out_ref.shape[0] // 3
    names = lax.broadcasted_iota(jnp.int32, (experts, tokens), 0)
    pick = jnp.zeros((experts, tokens), jnp.float32)
    share = jnp.zeros((experts, tokens), jnp.float32)
    for k in range(TOPK):
        named = routes_ref[k : k + 1, :] == names
        pick = jnp.where(named, 1.0, pick)
        share = jnp.where(named, weight_ref[k : k + 1, :], share)
    row = lax.broadcasted_iota(jnp.int32, (tokens, tokens), 0)
    col = lax.broadcasted_iota(jnp.int32, (tokens, tokens), 1)
    above = (row < col).astype(jnp.bfloat16)
    rank = jnp.dot(pick.astype(jnp.bfloat16), above, preferred_element_type=jnp.float32)
    out_ref[0:experts] = jnp.where(pick > 0.0, rank, -1.0).astype(jnp.bfloat16)
    high = share.astype(jnp.bfloat16)
    out_ref[experts : 2 * experts] = high
    out_ref[2 * experts :] = (share - high.astype(jnp.float32)).astype(jnp.bfloat16)


def route(routes, route_weight, experts):
    return pl.pallas_call(
        route_kernel,
        out_shape=jax.ShapeDtypeStruct((3 * experts, routes.shape[1]), jnp.bfloat16),
        in_specs=[pl.BlockSpec(memory_space=pltpu.VMEM)] * 2,
        out_specs=pl.BlockSpec(memory_space=pltpu.VMEM),
        name="route",
    )(routes, route_weight)


GROUP = 2
FULL = 8


def attention_kernel(meta_ref, mine_ref, peer, out_ref, kv_ref, tri_ref, query_ref, acc_ref, sems):
    core, offset = meta_ref[0], meta_ref[1]
    side = tri_ref.shape[0]
    rows = side // 2
    first_rows = pl.ds(pl.multiple_of(core * rows, rows), rows)
    other_rows = pl.ds(pl.multiple_of((1 - core) * rows, rows), rows)
    span = kv_ref.shape[0] // 4
    loads = []
    for piece in range(4):
        chips = pl.ds(piece * span, span)
        loads.append(
            pltpu.make_async_copy(peer.at[chips, pl.ds(0, rows)], kv_ref.at[chips, other_rows], sems.at[piece])
        )
        loads[-1].start()
    row = lax.broadcasted_iota(jnp.int32, (side, side), 0)
    col = lax.broadcasted_iota(jnp.int32, (side, side), 1)
    tri_ref[...] = (row > col).astype(jnp.float32)
    raw = mine_ref[:, rows:]
    none = jnp.zeros(raw.shape[:2] + (HEAD_DIM,), jnp.bfloat16)
    early = jnp.concatenate([raw[:, :, :HEAD_DIM], none], axis=2)
    late = jnp.concatenate([raw[:, :, HEAD_DIM:], none], axis=2)
    query_ref[...] = jnp.concatenate([early, late], axis=1).reshape(query_ref.shape)

    @pl.loop(0, kv_ref.shape[0] // 4)
    def _(turn):
        for i in range(4):
            kv_ref[4 * turn + i, first_rows] = mine_ref[4 * turn + i, :rows]

    for load in loads:
        load.wait()

    tiles, depth = query_ref.shape[:2]
    blocks = depth // 16

    def advance(jobs, skip, diagonal, count):
        chains = [(tile, first + i, i) for tile, first in jobs for i in range(count)]
        queries = {tile: query_ref[tile, skip:] for tile, _ in jobs}
        keys = [kv_ref[block] for _, block, _ in chains]
        scores = [
            lax.dot_general(
                queries[tile], kv, (((1,), (1,)), ((), ())), preferred_element_type=jnp.float32
            )
            * (HEAD_DIM**-0.5 * LOG2E)
            for (tile, _, _), kv in zip(chains, keys)
        ]
        costs = [jnp.maximum(s, jnp.log2(1.0 + jnp.exp2(jnp.minimum(s, 126.0)))) for s in scores]
        slacks = [s - c for s, c in zip(scores, costs)]
        if diagonal:
            edge = 16 * count
            shape = (edge, side)
            place = lax.broadcasted_iota(jnp.int32, shape, 0)
            place = place // 16 * side + place % 16 + offset - lax.broadcasted_iota(jnp.int32, shape, 1)
            live = [place > i * side for i in range(count)]

            def masked(i, value):
                top = jnp.where(live[i], value[:edge], 0.0)
                return top if value.shape[0] == edge else jnp.concatenate([top, value[edge:]], axis=0)

            costs = [masked(i, c) for (_, _, i), c in zip(chains, costs)]
        tri = tri_ref[...]
        insides = [jnp.dot(c, tri, preferred_element_type=jnp.float32) for c in costs]
        accs = {tile: acc_ref[tile, skip:] for tile, _ in jobs}
        for (tile, _, i), kv, cost, slack, inside in zip(chains, keys, costs, slacks, insides):
            weight = jnp.exp2(slack - inside)
            if diagonal:
                weight = masked(i, weight)
            part = jnp.dot(weight.astype(jnp.bfloat16), kv, preferred_element_type=jnp.float32)
            accs[tile] = accs[tile] * jnp.exp2(-jnp.sum(cost, axis=1, keepdims=True)) + part
        for tile, acc in accs.items():
            acc_ref[tile, skip:] = acc

    acc_ref[...] = jnp.zeros_like(acc_ref)

    @pl.loop(0, blocks // FULL)
    def _(step):
        advance([(1, step * FULL)], 0, False, FULL)

    for step in range(blocks // GROUP):
        advance([(tile, blocks * tile + step * GROUP) for tile in range(tiles)], step * GROUP * 16, True, GROUP)
    done = acc_ref[:, :, HEAD_DIM:].reshape(tiles * blocks, 16, HEAD_DIM)
    out_ref[...] = jnp.concatenate([done[:, :8], done[:, 8:]], axis=2).astype(jnp.bfloat16)


def attention(meta, mine, peer):
    chips, depth, _ = mine.shape
    side = 2 * (depth - 8)
    pairs = 136 * side * side
    return pl.pallas_call(
        attention_kernel,
        out_shape=jax.ShapeDtypeStruct((chips, 8, LANES), jnp.bfloat16),
        in_specs=[
            pl.BlockSpec(memory_space=pltpu.SMEM),
            pl.BlockSpec(memory_space=pltpu.VMEM),
            pl.BlockSpec(memory_space=pl.ANY),
        ],
        out_specs=pl.BlockSpec(memory_space=pltpu.VMEM),
        scratch_shapes=[
            pltpu.VMEM((chips, side, LANES), jnp.bfloat16),
            pltpu.VMEM((side, side), jnp.float32),
            pltpu.VMEM((2, 2 * side, LANES), jnp.bfloat16),
            pltpu.VMEM((2, 2 * side, LANES), jnp.float32),
            pltpu.SemaphoreType.DMA((4,)),
        ],
        compiler_params=pltpu.CompilerParams(vmem_limit_bytes=40 * 2**20),
        cost_estimate=pl.CostEstimate(
            flops=pairs * 2 * 768, bytes_accessed=6 * 2**20, transcendentals=pairs * 3
        ),
        name="attend",
    )(meta, mine, peer)


MAIN = 16
TAIL = 4


def expand(count, slots, experts, first):
    row = lax.broadcasted_iota(jnp.int32, (count * slots, experts), 0)
    col = lax.broadcasted_iota(jnp.int32, (count * slots, experts), 1)
    return (col == first + row // slots).astype(jnp.bfloat16)


STEP = 16


def copy_group(source, target, sems, start, count, parts):
    each = count // parts
    return [
        pltpu.make_async_copy(
            source.at[pl.ds(start + i * each, each)],
            target.at[pl.ds(start + i * each, each)],
            sems.at[start // each + i],
        )
        for i in range(parts)
    ]


def dispatch_kernel(
    attended_ref,
    residual_ref,
    weight_ref,
    gain_ref,
    rank_ref,
    mixed_ref,
    normed_ref,
    out_ref,
    heads_ref,
):
    count, _, half = out_ref.shape
    experts, tokens = rank_ref.shape

    @pl.when(pl.program_id(0) == 0)
    def _():
        for head in range(8):
            rows = attended_ref[8 * head : 8 * head + 8]
            rows = jnp.concatenate([rows[:, :, :HEAD_DIM], rows[:, :, HEAD_DIM:]], axis=1)
            heads_ref[:, head * HEAD_DIM : (head + 1) * HEAD_DIM] = rows.reshape(tokens, HEAD_DIM)
        projected = jnp.dot(heads_ref[...], weight_ref[...], preferred_element_type=jnp.float32)
        mixed = (residual_ref[...].astype(jnp.float32) + projected).astype(jnp.bfloat16)
        mixed_ref[...] = mixed
        mixed = mixed.astype(jnp.float32)
        inverse = lax.rsqrt(jnp.mean(mixed * mixed, axis=1, keepdims=True) + norm_eps)
        normed_ref[...] = (mixed * inverse * gain_ref[...]).astype(jnp.bfloat16)

    left, right = normed_ref[:, :half], normed_ref[:, half:]
    first = pl.program_id(0) * count

    def chosen(slots, lowest):
        rank = jnp.dot(
            expand(count, slots, experts, first), rank_ref[...], preferred_element_type=jnp.float32
        )
        slot = lowest + lax.broadcasted_iota(jnp.int32, rank.shape, 0) % (slots if lowest == 0 else TAIL)
        return (rank == slot.astype(jnp.float32)).astype(jnp.bfloat16)

    def pick(rows, side):
        return jnp.dot(rows, side, preferred_element_type=jnp.float32)

    main, tail = chosen(MAIN, 0), chosen(2 * TAIL, MAIN)
    out_ref[:, 0:MAIN, :] = pick(main, left).astype(jnp.bfloat16).reshape(count, MAIN, half)
    out_ref[:, MAIN : 2 * MAIN, :] = pick(main, right).astype(jnp.bfloat16).reshape(count, MAIN, half)
    early = lax.broadcasted_iota(jnp.int32, (tail.shape[0], half), 0) % (2 * TAIL) < TAIL
    both = jnp.where(early, pick(tail, left), pick(tail, right))
    out_ref[:, 2 * MAIN :, :] = both.astype(jnp.bfloat16).reshape(count, 2 * TAIL, half)


def dispatch(attended, residual, out_weight, gain, ranks, experts):
    tokens, width = residual.shape
    step = 32
    whole = lambda i: (0, 0)
    return pl.pallas_call(
        dispatch_kernel,
        grid=(experts // step,),
        in_specs=[
            pl.BlockSpec(attended.shape, lambda i: (0, 0, 0)),
            pl.BlockSpec(residual.shape, whole),
            pl.BlockSpec(out_weight.shape, whole),
            pl.BlockSpec(gain.shape, whole),
            pl.BlockSpec((experts, tokens), whole),
        ],
        out_specs=[
            pl.BlockSpec((tokens, width), whole),
            pl.BlockSpec((tokens, width), whole),
            pl.BlockSpec((step, 2 * (MAIN + TAIL), width // 2), lambda i: (i, 0, 0)),
        ],
        out_shape=[
            jax.ShapeDtypeStruct((tokens, width), jnp.bfloat16),
            jax.ShapeDtypeStruct((tokens, width), jnp.bfloat16),
            jax.ShapeDtypeStruct((experts, 2 * (MAIN + TAIL), width // 2), jnp.bfloat16),
        ],
        scratch_shapes=[pltpu.VMEM((tokens, 8 * HEAD_DIM), jnp.bfloat16)],
        compiler_params=pltpu.CompilerParams(vmem_limit_bytes=32 * 2**20),
        cost_estimate=pl.CostEstimate(flops=10**9, bytes_accessed=10**7, transcendentals=0),
        name="dispatch",
    )(attended, residual, out_weight, gain, ranks)


PASS = 32


def expert_kernel(
    rows_ref,
    gate0_ref,
    up0_ref,
    gate1_ref,
    up1_ref,
    down0_ref,
    down1_ref,
    shared_gate_ref,
    shared_up_ref,
    shared_down_ref,
    mixed_ref,
    normed_ref,
    out_ref,
    base_ref,
    spread_ref,
    rows2_ref,
):
    total, _, half = rows_ref.shape
    tails, mains = PASS * TAIL, PASS * MAIN
    row = lax.broadcasted_iota(jnp.int32, (2 * tails, 2 * tails), 0)
    col = lax.broadcasted_iota(jnp.int32, (2 * tails, 2 * tails), 1)
    slot = row % tails
    home = slot // TAIL * (2 * TAIL) + row // tails * TAIL + slot % TAIL
    spread_ref[...] = (home == col).astype(jnp.bfloat16)

    def hidden(rows, gate_matrix, up_matrix):
        gate = jnp.dot(rows, gate_matrix, preferred_element_type=jnp.float32)
        upward = jnp.dot(rows, up_matrix, preferred_element_type=jnp.float32)
        return (jax.nn.silu(gate) * upward).astype(jnp.bfloat16)

    @pl.loop(0, total // PASS)
    def _(turn):
        part = pl.ds(turn * PASS, PASS)
        spread = spread_ref[...]
        rows2_ref[:mains, :half] = rows_ref[part, 0:MAIN, :].reshape(mains, half)
        rows2_ref[:mains, half:] = rows_ref[part, MAIN : 2 * MAIN, :].reshape(mains, half)
        ends = jnp.dot(
            spread, rows_ref[part, 2 * MAIN :, :].reshape(2 * tails, half), preferred_element_type=jnp.float32
        ).astype(jnp.bfloat16)
        rows2_ref[mains:, :half] = ends[:tails]
        rows2_ref[mains:, half:] = ends[tails:]
        act0 = hidden(rows2_ref[...], gate0_ref[0], up0_ref[0])
        act1 = hidden(rows2_ref[...], gate1_ref[0], up1_ref[0])
        ends = []
        for side in range(2):
            span = slice(side * half, (side + 1) * half)
            result = jnp.dot(act0, down0_ref[0, :, span], preferred_element_type=jnp.float32) + jnp.dot(
                act1, down1_ref[0, :, span], preferred_element_type=jnp.float32
            )
            result = result.astype(jnp.bfloat16)
            out_ref[part, side * MAIN : (side + 1) * MAIN, :] = result[:mains].reshape(PASS, MAIN, half)
            ends.append(result[mains:])
        ends = lax.dot_general(
            spread, jnp.concatenate(ends, axis=0), (((0,), (0,)), ((), ())), preferred_element_type=jnp.float32
        )
        out_ref[part, 2 * MAIN :, :] = ends.astype(jnp.bfloat16).reshape(PASS, 2 * TAIL, half)

    act = hidden(normed_ref[...], shared_gate_ref[...], shared_up_ref[...])
    base_ref[...] = mixed_ref[...].astype(jnp.float32) + jnp.dot(
        act, shared_down_ref[...], preferred_element_type=jnp.float32
    )


def expert(rows, weights, mixed, normed):
    return pl.pallas_call(
        expert_kernel,
        in_specs=[pl.BlockSpec(memory_space=pltpu.VMEM)] * (3 + len(weights)),
        out_specs=[pl.BlockSpec(memory_space=pltpu.VMEM)] * 2,
        out_shape=[
            jax.ShapeDtypeStruct(rows.shape, jnp.bfloat16),
            jax.ShapeDtypeStruct(mixed.shape, jnp.float32),
        ],
        scratch_shapes=[
            pltpu.VMEM((PASS * 2 * TAIL, PASS * 2 * TAIL), jnp.bfloat16),
            pltpu.VMEM((PASS * (MAIN + TAIL), 2 * rows.shape[2]), jnp.bfloat16),
        ],
        compiler_params=pltpu.CompilerParams(vmem_limit_bytes=24 * 2**20),
        cost_estimate=pl.CostEstimate(flops=8 * 10**9, bytes_accessed=17 * 10**6, transcendentals=10**6),
        name="expert",
    )(rows, *weights, mixed, normed)


HALF = 64


def combine_kernel(rows_ref, ranks_ref, base_ref, out_ref, acc_ref):
    total, _, half = rows_ref.shape
    tokens = base_ref.shape[0]
    experts = ranks_ref.shape[0] // 3
    acc_ref[...] = base_ref[...]

    @pl.loop(0, total // HALF)
    def _(turn):
        def weights(slots, wanted):
            chosen = expand(HALF, slots, experts, turn * HALF)
            rank, high, low = [
                jnp.dot(chosen, ranks_ref[i * experts : (i + 1) * experts], preferred_element_type=jnp.float32)
                for i in range(3)
            ]
            slot = wanted(lax.broadcasted_iota(jnp.int32, rank.shape, 0) % slots).astype(jnp.float32)
            here = rank == slot
            parts = [jnp.where(here, part, 0.0) for part in (high, low)]
            return jnp.concatenate(parts, axis=1).T.astype(jnp.bfloat16)

        part = pl.ds(turn * HALF, HALF)
        main = weights(MAIN, lambda slot: slot)
        ends = rows_ref[part, 2 * MAIN :, :].reshape(HALF * 2 * TAIL, half)
        for side in range(2):
            tail = weights(2 * TAIL, lambda slot: jnp.where(slot // TAIL == side, MAIN + slot % TAIL, -2))
            rows = rows_ref[part, side * MAIN : (side + 1) * MAIN, :].reshape(HALF * MAIN, half)
            sums = jnp.dot(main, rows, preferred_element_type=jnp.float32) + jnp.dot(
                tail, ends, preferred_element_type=jnp.float32
            )
            span = pl.ds(side * half, half)
            acc_ref[:, span] += sums[:tokens] + sums[tokens:]

    out_ref[...] = acc_ref[...].astype(jnp.bfloat16)


def combine(rows, ranks, base):
    return pl.pallas_call(
        combine_kernel,
        in_specs=[pl.BlockSpec(memory_space=pltpu.VMEM)] * 3,
        out_specs=pl.BlockSpec(memory_space=pltpu.VMEM),
        out_shape=jax.ShapeDtypeStruct(base.shape, jnp.bfloat16),
        scratch_shapes=[pltpu.VMEM(base.shape, jnp.float32)],
        compiler_params=pltpu.CompilerParams(vmem_limit_bytes=24 * 2**20),
        cost_estimate=pl.CostEstimate(flops=10**9, bytes_accessed=10**7, transcendentals=0),
        name="combine",
    )(rows, ranks, base)


def local(
    queries,
    key_rows,
    value_rows,
    residual,
    out_weight,
    norm_gain,
    routes,
    route_weight,
    expert_gate,
    expert_up,
    expert_down,
    shared_gate,
    shared_up,
    shared_down,
):
    core = lax.axis_index("tp")
    offset = 128 * core + 16 * (lax.axis_index("sp") % 8)
    swap = [(0, 1), (1, 0)]
    cores = core[None].astype(jnp.int32)
    keep, send = pack(cores, queries, key_rows, value_rows)
    taken = lax.ppermute(send, "tp", swap)
    mine = lax.all_to_all(spread(cores, keep, taken), "sp", 0, 0, tiled=True)
    peer = lax.ppermute(mine, "tp", swap)
    mine, routes, route_weight = lax.optimization_barrier((mine, routes, route_weight))
    ranks = route(routes.T, route_weight.T, 64)
    peer, ranks, expert_gate_, expert_up_, expert_down_ = lax.optimization_barrier(
        (peer, ranks, expert_gate, expert_up, expert_down)
    )
    attended = attention(jnp.stack([core, offset]).astype(jnp.int32), mine, peer)
    gate_other = lax.ppermute(expert_gate_, "tp", swap)
    up_other = lax.ppermute(expert_up_, "tp", swap)
    down_other = lax.ppermute(expert_down_, "tp", swap)
    attended, gate_other, up_other, down_other = lax.optimization_barrier(
        (attended, gate_other, up_other, down_other)
    )
    attended = lax.all_to_all(attended, "sp", 0, 0, tiled=True)
    experts = lax.axis_size("sp")
    mixed, normed, outgoing = dispatch(
        attended, residual, out_weight, norm_gain[None, :], ranks, experts
    )
    incoming = lax.all_to_all(outgoing, "sp", 0, 0, tiled=True)
    result, base = expert(
        incoming,
        (
            expert_gate,
            expert_up,
            gate_other,
            up_other,
            expert_down,
            down_other,
            shared_gate,
            shared_up,
            shared_down,
        ),
        mixed,
        normed,
    )
    returned = lax.all_to_all(result, "sp", 0, 0, tiled=True)
    return combine(returned, ranks, base)


def solution(mesh):
    return jax.shard_map(
        local,
        mesh=mesh,
        in_specs=(
            P("sp", "tp"),
            P("sp", "tp"),
            P("sp", "tp"),
            P(("sp", "tp"), None),
            P(),
            P(),
            P(("sp", "tp"), None),
            P(("sp", "tp"), None),
            P("sp", None, "tp"),
            P("sp", None, "tp"),
            P("sp", "tp", None),
            P(),
            P(),
            P(),
        ),
        out_specs=P(("sp", "tp"), None),
        check_vma=False,
    )
```

```python
import jax
import jax.numpy as jnp
from jax import lax
from jax.experimental import pallas as pl
from jax.experimental.pallas import tpu as pltpu
from jax.sharding import PartitionSpec as P

HEAD_DIM = 64
LANES = 128
TOPK = 8
LOG2E = 1.4426950408889634
norm_eps = 1e-06


VMEM_BYTES = 67043328


def pack_kernel(core_ref, rows_ref, keep_out, send_out):
    heads, rows = keep_out.shape[0], rows_ref.shape[1] // 2
    core = core_ref[0]
    for out, half in ((send_out, 1 - core), (keep_out, core)):
        own = pl.ds(half * rows, rows)
        for head in range(heads):
            span = slice(head * HEAD_DIM, (head + 1) * HEAD_DIM)
            out[head, :rows] = jnp.concatenate([rows_ref[1, own, span], rows_ref[2, own, span]], axis=1)
            query = rows_ref[0, own, span].reshape(rows // 16, 16, HEAD_DIM)
            query = jnp.concatenate([query[:, :8], query[:, 8:]], axis=2)
            out[head, rows:] = query.reshape(rows // 2, LANES)


def pack(core, queries, key_rows, value_rows):
    side, width = key_rows.shape
    half = jax.ShapeDtypeStruct((width // HEAD_DIM, side // 2 + side // 4, LANES), jnp.bfloat16)
    return pl.pallas_call(
        pack_kernel,
        in_specs=[pl.BlockSpec(memory_space=pltpu.SMEM), pl.BlockSpec(memory_space=pltpu.VMEM)],
        out_specs=[pl.BlockSpec(memory_space=pltpu.VMEM)] * 2,
        out_shape=[half, half],
        compiler_params=pltpu.CompilerParams(vmem_limit_bytes=8 * 2**20),
        name="pack",
    )(core, jnp.stack([queries, key_rows, value_rows]))


def spread_kernel(core_ref, keep_ref, taken_ref, out_ref):
    chips, depth, _ = out_ref.shape
    rows = depth - 8
    for head in range(chips // 8):
        mine = head // 4 == core_ref[0]
        held = jnp.where(mine, keep_ref[head % 4], taken_ref[head % 4])
        for chip in range(8):
            out_ref[8 * head + chip, :rows] = held[:rows]
            out_ref[8 * head + chip, rows:] = held[rows + 8 * chip : rows + 8 * chip + 8]


def spread(core, keep, taken):
    shape = (64, keep.shape[1] * 2 // 3 + 8, LANES)
    return pl.pallas_call(
        spread_kernel,
        in_specs=[pl.BlockSpec(memory_space=pltpu.SMEM)] + [pl.BlockSpec(memory_space=pltpu.VMEM)] * 2,
        out_specs=pl.BlockSpec(memory_space=pltpu.VMEM),
        out_shape=jax.ShapeDtypeStruct(shape, jnp.bfloat16),
        compiler_params=pltpu.CompilerParams(vmem_limit_bytes=16 * 2**20),
        name="spread",
    )(core, keep, taken)


def route_kernel(routes_ref, weight_ref, out_ref):
    tokens, experts = routes_ref.shape[1], out_ref.shape[0] // 3
    names = lax.broadcasted_iota(jnp.int32, (experts, tokens), 0)
    pick = jnp.zeros((experts, tokens), jnp.float32)
    share = jnp.zeros((experts, tokens), jnp.float32)
    for k in range(TOPK):
        named = routes_ref[k : k + 1, :] == names
        pick = jnp.where(named, 1.0, pick)
        share = jnp.where(named, weight_ref[k : k + 1, :], share)
    row = lax.broadcasted_iota(jnp.int32, (tokens, tokens), 0)
    col = lax.broadcasted_iota(jnp.int32, (tokens, tokens), 1)
    above = (row < col).astype(jnp.bfloat16)
    rank = jnp.dot(pick.astype(jnp.bfloat16), above, preferred_element_type=jnp.float32)
    out_ref[0:experts] = jnp.where(pick > 0.0, rank, -1.0).astype(jnp.bfloat16)
    high = share.astype(jnp.bfloat16)
    out_ref[experts : 2 * experts] = high
    out_ref[2 * experts :] = (share - high.astype(jnp.float32)).astype(jnp.bfloat16)


def route(routes, route_weight, experts):
    return pl.pallas_call(
        route_kernel,
        out_shape=jax.ShapeDtypeStruct((3 * experts, routes.shape[1]), jnp.bfloat16),
        in_specs=[pl.BlockSpec(memory_space=pltpu.VMEM)] * 2,
        out_specs=pl.BlockSpec(memory_space=pltpu.VMEM),
        name="route",
    )(routes, route_weight)


GROUP = 2
FULL = 8


def attention_kernel(meta_ref, mine_ref, peer, out_ref, kv_ref, tri_ref, query_ref, acc_ref, sems):
    core, offset = meta_ref[0], meta_ref[1]
    side = tri_ref.shape[0]
    rows = side // 2
    first_rows = pl.ds(pl.multiple_of(core * rows, rows), rows)
    other_rows = pl.ds(pl.multiple_of((1 - core) * rows, rows), rows)
    span = kv_ref.shape[0] // 4
    loads = []
    for piece in range(4):
        chips = pl.ds(piece * span, span)
        loads.append(
            pltpu.make_async_copy(peer.at[chips, pl.ds(0, rows)], kv_ref.at[chips, other_rows], sems.at[piece])
        )
        loads[-1].start()
    row = lax.broadcasted_iota(jnp.int32, (side, side), 0)
    col = lax.broadcasted_iota(jnp.int32, (side, side), 1)
    tri_ref[...] = (row > col).astype(jnp.float32)
    raw = mine_ref[:, rows:]
    none = jnp.zeros(raw.shape[:2] + (HEAD_DIM,), jnp.bfloat16)
    early = jnp.concatenate([raw[:, :, :HEAD_DIM], none], axis=2)
    late = jnp.concatenate([raw[:, :, HEAD_DIM:], none], axis=2)
    query_ref[...] = jnp.concatenate([early, late], axis=1).reshape(query_ref.shape)

    @pl.loop(0, kv_ref.shape[0] // 4)
    def _(turn):
        for i in range(4):
            kv_ref[4 * turn + i, first_rows] = mine_ref[4 * turn + i, :rows]

    for load in loads:
        load.wait()

    tiles, depth = query_ref.shape[:2]
    blocks = depth // 16

    def advance(jobs, skip, diagonal, count):
        chains = [(tile, first + i, i) for tile, first in jobs for i in range(count)]
        queries = {tile: query_ref[tile, skip:] for tile, _ in jobs}
        keys = [kv_ref[block] for _, block, _ in chains]
        scores = [
            lax.dot_general(
                queries[tile], kv, (((1,), (1,)), ((), ())), preferred_element_type=jnp.float32
            )
            * (HEAD_DIM**-0.5 * LOG2E)
            for (tile, _, _), kv in zip(chains, keys)
        ]
        costs = [jnp.maximum(s, jnp.log2(1.0 + jnp.exp2(jnp.minimum(s, 126.0)))) for s in scores]
        slacks = [s - c for s, c in zip(scores, costs)]
        if diagonal:
            edge = 16 * count
            shape = (edge, side)
            place = lax.broadcasted_iota(jnp.int32, shape, 0)
            place = place // 16 * side + place % 16 + offset - lax.broadcasted_iota(jnp.int32, shape, 1)
            live = [place > i * side for i in range(count)]

            def masked(i, value):
                top = jnp.where(live[i], value[:edge], 0.0)
                return top if value.shape[0] == edge else jnp.concatenate([top, value[edge:]], axis=0)

            costs = [masked(i, c) for (_, _, i), c in zip(chains, costs)]
        tri = tri_ref[...]
        insides = [jnp.dot(c, tri, preferred_element_type=jnp.float32) for c in costs]
        for job, (tile, _) in enumerate(jobs):
            weights, later = [None] * count, None
            for i in reversed(range(count)):
                chain = job * count + i
                left = slacks[chain] if later is None else slacks[chain] - later
                weight = jnp.exp2(left - insides[chain])
                if diagonal:
                    weight = masked(i, weight)
                weights[i] = weight.astype(jnp.bfloat16)
                total = jnp.sum(costs[chain], axis=1, keepdims=True)
                later = total if later is None else later + total
            part = jnp.dot(
                jnp.concatenate(weights, axis=1),
                jnp.concatenate(keys[job * count : (job + 1) * count], axis=0),
                preferred_element_type=jnp.float32,
            )
            acc_ref[tile, skip:] = acc_ref[tile, skip:] * jnp.exp2(-later) + part

    acc_ref[...] = jnp.zeros_like(acc_ref)

    @pl.loop(0, blocks // FULL)
    def _(step):
        advance([(1, step * FULL)], 0, False, FULL)

    for step in range(blocks // GROUP):
        advance([(tile, blocks * tile + step * GROUP) for tile in range(tiles)], step * GROUP * 16, True, GROUP)
    done = acc_ref[:, :, HEAD_DIM:].reshape(tiles * blocks, 16, HEAD_DIM)
    out_ref[...] = jnp.concatenate([done[:, :8], done[:, 8:]], axis=2).astype(jnp.bfloat16)


def attention(meta, mine, peer):
    chips, depth, _ = mine.shape
    side = 2 * (depth - 8)
    pairs = 136 * side * side
    return pl.pallas_call(
        attention_kernel,
        out_shape=jax.ShapeDtypeStruct((chips, 8, LANES), jnp.bfloat16),
        in_specs=[
            pl.BlockSpec(memory_space=pltpu.SMEM),
            pl.BlockSpec(memory_space=pltpu.VMEM),
            pl.BlockSpec(memory_space=pl.ANY),
        ],
        out_specs=pl.BlockSpec(memory_space=pltpu.VMEM),
        scratch_shapes=[
            pltpu.VMEM((chips, side, LANES), jnp.bfloat16),
            pltpu.VMEM((side, side), jnp.float32),
            pltpu.VMEM((2, 2 * side, LANES), jnp.bfloat16),
            pltpu.VMEM((2, 2 * side, LANES), jnp.float32),
            pltpu.SemaphoreType.DMA((4,)),
        ],
        compiler_params=pltpu.CompilerParams(vmem_limit_bytes=40 * 2**20),
        cost_estimate=pl.CostEstimate(
            flops=pairs * 2 * 768, bytes_accessed=6 * 2**20, transcendentals=pairs * 3
        ),
        name="attend",
    )(meta, mine, peer)


MAIN = 16
TAIL = 4


def expand(count, slots, experts, first):
    row = lax.broadcasted_iota(jnp.int32, (count * slots, experts), 0)
    col = lax.broadcasted_iota(jnp.int32, (count * slots, experts), 1)
    return (col == first + row // slots).astype(jnp.bfloat16)


STEP = 16


def copy_group(source, target, sems, start, count, parts):
    each = count // parts
    return [
        pltpu.make_async_copy(
            source.at[pl.ds(start + i * each, each)],
            target.at[pl.ds(start + i * each, each)],
            sems.at[start // each + i],
        )
        for i in range(parts)
    ]


def dispatch_kernel(
    attended_ref,
    residual_ref,
    weight_ref,
    gain_ref,
    rank_ref,
    mixed_ref,
    normed_ref,
    out_ref,
    heads_ref,
):
    count, _, half = out_ref.shape
    experts, tokens = rank_ref.shape

    @pl.when(pl.program_id(0) == 0)
    def _():
        for head in range(8):
            rows = attended_ref[8 * head : 8 * head + 8]
            rows = jnp.concatenate([rows[:, :, :HEAD_DIM], rows[:, :, HEAD_DIM:]], axis=1)
            heads_ref[:, head * HEAD_DIM : (head + 1) * HEAD_DIM] = rows.reshape(tokens, HEAD_DIM)
        projected = jnp.dot(heads_ref[...], weight_ref[...], preferred_element_type=jnp.float32)
        mixed = (residual_ref[...].astype(jnp.float32) + projected).astype(jnp.bfloat16)
        mixed_ref[...] = mixed
        mixed = mixed.astype(jnp.float32)
        inverse = lax.rsqrt(jnp.mean(mixed * mixed, axis=1, keepdims=True) + norm_eps)
        normed_ref[...] = (mixed * inverse * gain_ref[...]).astype(jnp.bfloat16)

    left, right = normed_ref[:, :half], normed_ref[:, half:]
    first = pl.program_id(0) * count

    def chosen(slots, lowest):
        rank = jnp.dot(
            expand(count, slots, experts, first), rank_ref[...], preferred_element_type=jnp.float32
        )
        slot = lowest + lax.broadcasted_iota(jnp.int32, rank.shape, 0) % (slots if lowest == 0 else TAIL)
        return (rank == slot.astype(jnp.float32)).astype(jnp.bfloat16)

    def pick(rows, side):
        return jnp.dot(rows, side, preferred_element_type=jnp.float32)

    main, tail = chosen(MAIN, 0), chosen(2 * TAIL, MAIN)
    out_ref[:, 0:MAIN, :] = pick(main, left).astype(jnp.bfloat16).reshape(count, MAIN, half)
    out_ref[:, MAIN : 2 * MAIN, :] = pick(main, right).astype(jnp.bfloat16).reshape(count, MAIN, half)
    early = lax.broadcasted_iota(jnp.int32, (tail.shape[0], half), 0) % (2 * TAIL) < TAIL
    both = jnp.where(early, pick(tail, left), pick(tail, right))
    out_ref[:, 2 * MAIN :, :] = both.astype(jnp.bfloat16).reshape(count, 2 * TAIL, half)


def dispatch(attended, residual, out_weight, gain, ranks, experts):
    tokens, width = residual.shape
    step = 32
    whole = lambda i: (0, 0)
    return pl.pallas_call(
        dispatch_kernel,
        grid=(experts // step,),
        in_specs=[
            pl.BlockSpec(attended.shape, lambda i: (0, 0, 0)),
            pl.BlockSpec(residual.shape, whole),
            pl.BlockSpec(out_weight.shape, whole),
            pl.BlockSpec(gain.shape, whole),
            pl.BlockSpec((experts, tokens), whole),
        ],
        out_specs=[
            pl.BlockSpec((tokens, width), whole),
            pl.BlockSpec((tokens, width), whole),
            pl.BlockSpec((step, 2 * (MAIN + TAIL), width // 2), lambda i: (i, 0, 0)),
        ],
        out_shape=[
            jax.ShapeDtypeStruct((tokens, width), jnp.bfloat16),
            jax.ShapeDtypeStruct((tokens, width), jnp.bfloat16),
            jax.ShapeDtypeStruct((experts, 2 * (MAIN + TAIL), width // 2), jnp.bfloat16),
        ],
        scratch_shapes=[pltpu.VMEM((tokens, 8 * HEAD_DIM), jnp.bfloat16)],
        compiler_params=pltpu.CompilerParams(vmem_limit_bytes=32 * 2**20),
        cost_estimate=pl.CostEstimate(flops=10**9, bytes_accessed=10**7, transcendentals=0),
        name="dispatch",
    )(attended, residual, out_weight, gain, ranks)


PASS = 32


def expert_kernel(
    rows_ref,
    gate0_ref,
    up0_ref,
    gate1_ref,
    up1_ref,
    down0_ref,
    down1_ref,
    shared_gate_ref,
    shared_up_ref,
    shared_down_ref,
    mixed_ref,
    normed_ref,
    out_ref,
    base_ref,
    spread_ref,
    rows2_ref,
):
    total, _, half = rows_ref.shape
    tails, mains = PASS * TAIL, PASS * MAIN
    row = lax.broadcasted_iota(jnp.int32, (2 * tails, 2 * tails), 0)
    col = lax.broadcasted_iota(jnp.int32, (2 * tails, 2 * tails), 1)
    slot = row % tails
    home = slot // TAIL * (2 * TAIL) + row // tails * TAIL + slot % TAIL
    spread_ref[...] = (home == col).astype(jnp.bfloat16)

    def hidden(rows, gate_matrix, up_matrix):
        gate = jnp.dot(rows, gate_matrix, preferred_element_type=jnp.float32)
        upward = jnp.dot(rows, up_matrix, preferred_element_type=jnp.float32)
        return (jax.nn.silu(gate) * upward).astype(jnp.bfloat16)

    @pl.loop(0, total // PASS)
    def _(turn):
        part = pl.ds(turn * PASS, PASS)
        spread = spread_ref[...]
        rows2_ref[:mains, :half] = rows_ref[part, 0:MAIN, :].reshape(mains, half)
        rows2_ref[:mains, half:] = rows_ref[part, MAIN : 2 * MAIN, :].reshape(mains, half)
        ends = jnp.dot(
            spread, rows_ref[part, 2 * MAIN :, :].reshape(2 * tails, half), preferred_element_type=jnp.float32
        ).astype(jnp.bfloat16)
        rows2_ref[mains:, :half] = ends[:tails]
        rows2_ref[mains:, half:] = ends[tails:]
        act0 = hidden(rows2_ref[...], gate0_ref[0], up0_ref[0])
        act1 = hidden(rows2_ref[...], gate1_ref[0], up1_ref[0])
        ends = []
        for side in range(2):
            span = slice(side * half, (side + 1) * half)
            result = jnp.dot(act0, down0_ref[0, :, span], preferred_element_type=jnp.float32) + jnp.dot(
                act1, down1_ref[0, :, span], preferred_element_type=jnp.float32
            )
            result = result.astype(jnp.bfloat16)
            out_ref[part, side * MAIN : (side + 1) * MAIN, :] = result[:mains].reshape(PASS, MAIN, half)
            ends.append(result[mains:])
        ends = lax.dot_general(
            spread, jnp.concatenate(ends, axis=0), (((0,), (0,)), ((), ())), preferred_element_type=jnp.float32
        )
        out_ref[part, 2 * MAIN :, :] = ends.astype(jnp.bfloat16).reshape(PASS, 2 * TAIL, half)

    act = hidden(normed_ref[...], shared_gate_ref[...], shared_up_ref[...])
    base_ref[...] = mixed_ref[...].astype(jnp.float32) + jnp.dot(
        act, shared_down_ref[...], preferred_element_type=jnp.float32
    )


def expert(rows, weights, mixed, normed):
    return pl.pallas_call(
        expert_kernel,
        in_specs=[pl.BlockSpec(memory_space=pltpu.VMEM)] * (3 + len(weights)),
        out_specs=[pl.BlockSpec(memory_space=pltpu.VMEM)] * 2,
        out_shape=[
            jax.ShapeDtypeStruct(rows.shape, jnp.bfloat16),
            jax.ShapeDtypeStruct(mixed.shape, jnp.float32),
        ],
        scratch_shapes=[
            pltpu.VMEM((PASS * 2 * TAIL, PASS * 2 * TAIL), jnp.bfloat16),
            pltpu.VMEM((PASS * (MAIN + TAIL), 2 * rows.shape[2]), jnp.bfloat16),
        ],
        compiler_params=pltpu.CompilerParams(vmem_limit_bytes=24 * 2**20),
        cost_estimate=pl.CostEstimate(flops=8 * 10**9, bytes_accessed=17 * 10**6, transcendentals=10**6),
        name="expert",
    )(rows, *weights, mixed, normed)


HALF = 64


def combine_kernel(rows_ref, ranks_ref, base_ref, out_ref, acc_ref):
    total, _, half = rows_ref.shape
    tokens = base_ref.shape[0]
    experts = ranks_ref.shape[0] // 3
    acc_ref[...] = base_ref[...]

    @pl.loop(0, total // HALF)
    def _(turn):
        def weights(slots, wanted):
            chosen = expand(HALF, slots, experts, turn * HALF)
            rank, high, low = [
                jnp.dot(chosen, ranks_ref[i * experts : (i + 1) * experts], preferred_element_type=jnp.float32)
                for i in range(3)
            ]
            slot = wanted(lax.broadcasted_iota(jnp.int32, rank.shape, 0) % slots).astype(jnp.float32)
            here = rank == slot
            parts = [jnp.where(here, part, 0.0) for part in (high, low)]
            return jnp.concatenate(parts, axis=1).T.astype(jnp.bfloat16)

        part = pl.ds(turn * HALF, HALF)
        main = weights(MAIN, lambda slot: slot)
        ends = rows_ref[part, 2 * MAIN :, :].reshape(HALF * 2 * TAIL, half)
        for side in range(2):
            tail = weights(2 * TAIL, lambda slot: jnp.where(slot // TAIL == side, MAIN + slot % TAIL, -2))
            rows = rows_ref[part, side * MAIN : (side + 1) * MAIN, :].reshape(HALF * MAIN, half)
            sums = jnp.dot(main, rows, preferred_element_type=jnp.float32) + jnp.dot(
                tail, ends, preferred_element_type=jnp.float32
            )
            span = pl.ds(side * half, half)
            acc_ref[:, span] += sums[:tokens] + sums[tokens:]

    out_ref[...] = acc_ref[...].astype(jnp.bfloat16)


def combine(rows, ranks, base):
    return pl.pallas_call(
        combine_kernel,
        in_specs=[pl.BlockSpec(memory_space=pltpu.VMEM)] * 3,
        out_specs=pl.BlockSpec(memory_space=pltpu.VMEM),
        out_shape=jax.ShapeDtypeStruct(base.shape, jnp.bfloat16),
        scratch_shapes=[pltpu.VMEM(base.shape, jnp.float32)],
        compiler_params=pltpu.CompilerParams(vmem_limit_bytes=24 * 2**20),
        cost_estimate=pl.CostEstimate(flops=10**9, bytes_accessed=10**7, transcendentals=0),
        name="combine",
    )(rows, ranks, base)


def local(
    queries,
    key_rows,
    value_rows,
    residual,
    out_weight,
    norm_gain,
    routes,
    route_weight,
    expert_gate,
    expert_up,
    expert_down,
    shared_gate,
    shared_up,
    shared_down,
):
    core = lax.axis_index("tp")
    offset = 128 * core + 16 * (lax.axis_index("sp") % 8)
    swap = [(0, 1), (1, 0)]
    cores = core[None].astype(jnp.int32)
    keep, send = pack(cores, queries, key_rows, value_rows)
    taken = lax.ppermute(send, "tp", swap)
    mine = lax.all_to_all(spread(cores, keep, taken), "sp", 0, 0, tiled=True)
    peer = lax.ppermute(mine, "tp", swap)
    mine, routes, route_weight = lax.optimization_barrier((mine, routes, route_weight))
    ranks = route(routes.T, route_weight.T, 64)
    peer, ranks, expert_gate_, expert_up_, expert_down_ = lax.optimization_barrier(
        (peer, ranks, expert_gate, expert_up, expert_down)
    )
    attended = attention(jnp.stack([core, offset]).astype(jnp.int32), mine, peer)
    gate_other = lax.ppermute(expert_gate_, "tp", swap)
    up_other = lax.ppermute(expert_up_, "tp", swap)
    down_other = lax.ppermute(expert_down_, "tp", swap)
    attended, gate_other, up_other, down_other = lax.optimization_barrier(
        (attended, gate_other, up_other, down_other)
    )
    attended = lax.all_to_all(attended, "sp", 0, 0, tiled=True)
    experts = lax.axis_size("sp")
    mixed, normed, outgoing = dispatch(
        attended, residual, out_weight, norm_gain[None, :], ranks, experts
    )
    incoming = lax.all_to_all(outgoing, "sp", 0, 0, tiled=True)
    result, base = expert(
        incoming,
        (
            expert_gate,
            expert_up,
            gate_other,
            up_other,
            expert_down,
            down_other,
            shared_gate,
            shared_up,
            shared_down,
        ),
        mixed,
        normed,
    )
    returned = lax.all_to_all(result, "sp", 0, 0, tiled=True)
    return combine(returned, ranks, base)


def solution(mesh):
    return jax.shard_map(
        local,
        mesh=mesh,
        in_specs=(
            P("sp", "tp"),
            P("sp", "tp"),
            P("sp", "tp"),
            P(("sp", "tp"), None),
            P(),
            P(),
            P(("sp", "tp"), None),
            P(("sp", "tp"), None),
            P("sp", None, "tp"),
            P("sp", None, "tp"),
            P("sp", "tp", None),
            P(),
            P(),
            P(),
        ),
        out_specs=P(("sp", "tp"), None),
        check_vma=False,
    )
```
